32 devices in a mesh: sp: 8 (over z, y), tp: 4 (over x, core).
Axes of the slice: x: 2, y: 2, z: 4, core: 2. Of those that a mesh axis runs over, the one named last changes fastest.
Arguments:
- queries: bfloat16 [8192, 1024], P('sp', 'tp'), may hold values from -6 to 6
- keys: bfloat16 [8192, 1024], P('sp', 'tp'), may hold values from -6 to 6
- values: bfloat16 [8192, 1024], P('sp', 'tp'), may hold values from -6 to 6
- gates: bfloat16 [8192, 1024], P('sp', 'tp'), may hold values from -6 to 6
- log_decay: float32 [8192, 8], P('sp', 'tp'), may hold values from -1.6 to 0, as said below
- norm_gain: float32 [8, 128], P('tp'), may hold values from 0.1 to 1.9
- out_weight: bfloat16 [1024, 2048], P('tp'), may hold values from -0.1875 to 0.1875
- resid: bfloat16 [8192, 2048], P(('sp', 'tp')), may hold values from -6 to 6
- post_mix_gain: float32 [2048], replicated, may hold values from 0.1 to 1.9
- pre_ffn_gain: float32 [2048], replicated, may hold values from 0.1 to 1.9
- w_gate: bfloat16 [2048, 5632], P('sp', 'tp'), may hold values from -0.125 to 0.125
- w_up: bfloat16 [2048, 5632], P('sp', 'tp'), may hold values from -0.125 to 0.125
- w_down: bfloat16 [5632, 2048], P('tp', 'sp'), may hold values from -0.078125 to 0.078125
- post_ffn_gain: float32 [2048], replicated, may hold values from 0.1 to 1.9
Outputs:
- updated: bfloat16 [8192, 2048], P(('sp', 'tp'))
The draws below stay inside these ranges and needn't reach their ends.
Inputs may be any that keep to these rules, and one draw needn't show every extreme that they name: `log_decay`: every entry is negative.
All inputs are finite; a program needn't handle non-finite values.
Results may differ from the reference program's by a relative error of at most 0.02.
Values may be sent and summed in bfloat16 or wider, within the bound.
A program may use at most 128 MiB of HBM per device.

```python
import math
import jax
import jax.numpy as jnp
from jax import lax

D = 2048
RETENTION_HEADS = 8
HEAD_DIM = 128
FF = 5632
TOK_DEV = 1024
RET_W = 1024
BLOCK = 512
SEQUENCE_TOKENS = 8192
N_TP = 4


def draw_log_decay(key, part):
    random_child_keys = jax.random.split(jax.random.fold_in(key, 17), 6)
    fast_share = 0.5
    is_fast = jax.random.uniform(random_child_keys[0], (RETENTION_HEADS,), jnp.float32) < fast_share
    fast_rate = jax.random.uniform(random_child_keys[1], (RETENTION_HEADS,), jnp.float32, 0.08, 0.15)
    baseline_decay_rate = jnp.where(is_fast, fast_rate, 0.6 / SEQUENCE_TOKENS)
    span_count = SEQUENCE_TOKENS // TOK_DEV
    factor = jnp.exp(jax.random.uniform(random_child_keys[2], (span_count, RETENTION_HEADS), jnp.float32, math.log(0.4), math.log(1.6)))
    row_values = jnp.repeat(factor, TOK_DEV, axis=0)
    random_noise = jax.random.uniform(random_child_keys[3], (SEQUENCE_TOKENS, RETENTION_HEADS), jnp.float32, 0.5, 1.5)
    spike_position = jax.random.randint(random_child_keys[4], (2, RETENTION_HEADS), 0, SEQUENCE_TOKENS)
    spike_length = jnp.log(jax.random.uniform(random_child_keys[5], (2, RETENTION_HEADS), jnp.float32, 0.55, 0.8))
    token_positions = lax.broadcasted_iota(jnp.int32, (SEQUENCE_TOKENS, RETENTION_HEADS), 0)
    spike_events = jnp.where(token_positions == spike_position[0][None, :], spike_length[0][None, :], 0.0)
    spike_events = spike_events + jnp.where(token_positions == spike_position[1][None, :], spike_length[1][None, :], 0.0)
    return (-baseline_decay_rate[None, :] * row_values * random_noise + spike_events).astype(jnp.float32)


def steps_of(own_key, extent, shards, low, largest):
    loudness, own = 1.0, jax.random.fold_in(own_key, 6)
    for axis_at, blocks in shards:
        draws = jnp.exp(jax.random.uniform(jax.random.fold_in(own, axis_at), (blocks,), jnp.float32, low / len(shards), largest / len(shards)))
        loudness = loudness * jnp.repeat(draws, extent[axis_at] // blocks).reshape([-1 if axis == axis_at else 1 for axis in range(len(extent))])
    return loudness


def normal_values(own_key, shape, spread, reach, cuts=(), dtype=jnp.bfloat16):
    result = spread * jax.random.normal(own_key, shape, jnp.float32)
    if cuts:
        result = result * steps_of(own_key, shape, cuts, -0.22, 0.18)
    return jnp.clip(result, -reach, reach).astype(dtype)


def setup_inputs(seed: int = 0) -> dict:
    streams_of = jax.random.split(jax.random.key(seed), 15)
    return {
        "queries": normal_values(streams_of[0], (SEQUENCE_TOKENS, RET_W), 1.0, 6.0, ((0, 8), (1, 4))),
        "keys": normal_values(streams_of[1], (SEQUENCE_TOKENS, RET_W), 1.0, 6.0, ((0, 8), (1, 4))),
        "values": normal_values(streams_of[2], (SEQUENCE_TOKENS, RET_W), 1.0, 6.0, ((0, 8), (1, 4))),
        "gates": normal_values(streams_of[3], (SEQUENCE_TOKENS, RET_W), 1.0, 6.0, ((0, 8), (1, 4))),
        "log_decay": draw_log_decay(jax.random.fold_in(streams_of[14], 71), 0),
        "norm_gain": jnp.clip(1.0 + 0.18 * jax.random.normal(streams_of[5], (RETENTION_HEADS, HEAD_DIM), jnp.float32), 0.1, 1.9),
        "out_weight": normal_values(streams_of[6], (RET_W, D), RET_W ** -0.5, 0.1875, ((0, 4),)),
        "resid": normal_values(streams_of[7], (SEQUENCE_TOKENS, D), 1.0, 6.0, ((0, 32),)),
        "post_mix_gain": jnp.clip(1.0 + 0.18 * jax.random.normal(streams_of[8], (D,), jnp.float32), 0.1, 1.9),
        "pre_ffn_gain": jnp.clip(1.0 + 0.18 * jax.random.normal(streams_of[9], (D,), jnp.float32), 0.1, 1.9),
        "w_gate": normal_values(streams_of[10], (D, FF), D ** -0.5, 0.125, ((0, 8), (1, 4))),
        "w_up": normal_values(streams_of[11], (D, FF), D ** -0.5, 0.125, ((0, 8), (1, 4))),
        "w_down": normal_values(streams_of[12], (FF, D), FF ** -0.5, 0.078125, ((0, 4), (1, 8))),
        "post_ffn_gain": jnp.clip(1.0 + 0.18 * jax.random.normal(streams_of[13], (D,), jnp.float32), 0.1, 1.9),
    }


EPSILON = 1e-06

def rms_norm(values_in, gain_vec):
    widened = values_in.astype(jnp.float32)
    return widened * lax.rsqrt(lax.optimization_barrier(jnp.mean(widened * widened, axis=-1, keepdims=True)) + EPSILON) * gain_vec.astype(jnp.float32)

def block_step(carried, pieces):
    query_blk, key_blk, value_blk, decay_blk = pieces
    length = query_blk.shape[1]
    key_scale = query_blk.shape[2] ** (-0.5)
    query_wide = query_blk.astype(jnp.float32)
    key_wide = key_blk.astype(jnp.float32)
    value_wide = value_blk.astype(jnp.float32)
    cumulative = jnp.cumsum(decay_blk, axis=1)
    log_gap = cumulative[:, :, None] - cumulative[:, None, :]
    causal = lax.broadcasted_iota(jnp.int32, (length, length), 0) >= lax.broadcasted_iota(jnp.int32, (length, length), 1)
    weight = jnp.where(causal[None], jnp.exp(jnp.minimum(log_gap, 0.0)), 0.0)
    products = jnp.einsum('htd,hsd->hts', query_wide, key_wide)
    scores = lax.optimization_barrier((products * key_scale * weight).astype(jnp.bfloat16))
    within = jnp.einsum('hts,hsd->htd', scores.astype(jnp.float32), value_wide)
    carried_term = jnp.einsum('htd,hde->hte', query_wide, carried, precision=lax.Precision.HIGHEST) * jnp.exp(cumulative)[:, :, None]
    to_end = jnp.exp(cumulative[:, -1:] - cumulative) * key_scale
    scaled_keys = lax.optimization_barrier((key_wide * to_end[:, :, None]).astype(jnp.bfloat16))
    added = jnp.einsum('hsd,hse->hde', scaled_keys.astype(jnp.float32), value_wide)
    carried = jnp.exp(cumulative[:, -1])[:, None, None] * carried + added
    return (carried, within + carried_term)

def to_blocks(matrix, block_len, head_count):
    row_count = matrix.shape[0]
    return matrix.reshape(row_count // block_len, block_len, head_count, -1).transpose(0, 2, 1, 3)

def finish_heads(retention, gates, norm_gain):
    centered = retention - lax.optimization_barrier(jnp.mean(retention, axis=-1, keepdims=True))
    variance = lax.optimization_barrier(jnp.mean(centered * centered, axis=-1, keepdims=True))
    normed = centered * lax.rsqrt(variance + EPSILON) * norm_gain.astype(jnp.float32)[None]
    gate_vals = gates.astype(jnp.float32).reshape(normed.shape)
    return (jax.nn.silu(gate_vals) * normed).reshape(normed.shape[0], -1).astype(jnp.bfloat16)

def grouped_product(left, right, group_count):
    inner = left.shape[1] // group_count
    total = jnp.zeros((left.shape[0], right.shape[1]), jnp.float32)
    for group in range(group_count):
        part = jnp.dot(left[:, group * inner:(group + 1) * inner], right[group * inner:(group + 1) * inner], preferred_element_type=jnp.float32)
        total = total + part.astype(jnp.bfloat16).astype(jnp.float32)
    return total.astype(jnp.bfloat16)

def reference(queries, keys, values, gates, log_decay, norm_gain, out_weight, resid, post_mix_gain, pre_ffn_gain, w_gate, w_up, w_down, post_ffn_gain):
    block_count = SEQUENCE_TOKENS // BLOCK
    query_blocks = to_blocks(queries, BLOCK, RETENTION_HEADS)
    key_blocks = to_blocks(keys, BLOCK, RETENTION_HEADS)
    value_blocks = to_blocks(values, BLOCK, RETENTION_HEADS)
    decay_blocks = log_decay.reshape(block_count, BLOCK, RETENTION_HEADS).transpose(0, 2, 1)
    start_state = jnp.zeros((RETENTION_HEADS, HEAD_DIM, HEAD_DIM), jnp.float32)
    _, outputs = lax.scan(block_step, start_state, (query_blocks, key_blocks, value_blocks, decay_blocks))
    retention = outputs.transpose(0, 2, 1, 3).reshape(SEQUENCE_TOKENS, RETENTION_HEADS, HEAD_DIM)
    retained = finish_heads(retention, gates, norm_gain)
    mixed = grouped_product(retained, out_weight, N_TP)
    middle = (resid.astype(jnp.float32) + rms_norm(mixed, post_mix_gain)).astype(jnp.bfloat16)
    ffn_input = rms_norm(middle, pre_ffn_gain).astype(jnp.bfloat16)

    def ffn_rows(row_block):
        gate_act = jnp.dot(row_block, w_gate, preferred_element_type=jnp.float32)
        up_act = jnp.dot(row_block, w_up, preferred_element_type=jnp.float32)
        hidden = (jax.nn.silu(gate_act) * up_act).astype(jnp.bfloat16)
        return grouped_product(hidden, w_down, N_TP)
    branch = lax.map(ffn_rows, ffn_input.reshape(SEQUENCE_TOKENS // TOK_DEV, TOK_DEV, D)).reshape(SEQUENCE_TOKENS, D)
    return (middle.astype(jnp.float32) + rms_norm(branch, post_ffn_gain)).astype(jnp.bfloat16)
```

```python
import jax
import jax.numpy as jnp
from jax import lax
from jax.experimental import pallas as pl
from jax.experimental.pallas import tpu as pltpu
from jax.sharding import PartitionSpec as P


BLOCK = 512


EPSILON = 1e-06
LONGEST_RING = 8


def entering(decay, state):
    place = lax.axis_index("sp")
    head_count, head_dim, _ = state.shape
    decay_rows = jnp.broadcast_to(decay[:, None, None], (head_count, 16, head_dim))
    packed = jnp.concatenate([state, decay_rows], axis=1).astype(jnp.bfloat16)
    gathered = lax.all_gather(packed, "sp")

    def one(step, running):
        piece = lax.dynamic_index_in_dim(gathered, step, 0, False).astype(jnp.float32)
        return piece[:, head_dim : head_dim + 1, :] * running + piece[:, :head_dim]

    return lax.fori_loop(0, place, one, jnp.zeros_like(state))


def from_earlier(packed, distance):
    count = lax.axis_size("sp")
    return lax.ppermute(packed, "sp", [(i, i + distance) for i in range(count - distance)])


def entering_by_hops(decay, state):
    count = lax.axis_size("sp")
    head_count, head_dim, _ = state.shape
    decay_rows = jnp.broadcast_to(decay[:, None, None], (head_count, 8, head_dim))
    packed = jnp.concatenate([state, decay_rows], axis=1)
    near = from_earlier(packed, 1)
    far = from_earlier(packed, 2)
    factor = near[:, head_dim:]
    pair = jnp.concatenate(
        [factor[:, :1] * far[:, :head_dim] + near[:, :head_dim], factor * far[:, head_dim:]],
        axis=1,
    )
    total, factor = pair[:, :head_dim], pair[:, head_dim : head_dim + 1]
    for piece in [from_earlier(pair, distance) for distance in range(2, count, 2)]:
        total = total + factor * piece[:, :head_dim]
        factor = factor * piece[:, head_dim : head_dim + 1]
    return total


def ring_order(count):
    return list(range(0, count, 2)) + list(range(1, count, 2))[::-1]


def ring_gather(block, forward_steps, backward_steps):
    count = lax.axis_size("sp")
    order = ring_order(count)
    ahead = [(order[i], order[(i + 1) % count]) for i in range(count)]
    behind = [(b, a) for a, b in ahead]
    arrived = [(0, block)]
    up, down = block, block
    for step in range(1, max(forward_steps, backward_steps) + 1):
        if step <= forward_steps:
            up = lax.ppermute(up, "sp", ahead)
            arrived.append((-step, up))
        if step <= backward_steps:
            down = lax.ppermute(down, "sp", behind)
            arrived.append((step, down))
    return arrived


def owner_of(offset):
    count = lax.axis_size("sp")
    me = lax.axis_index("sp")
    half = (count + 1) // 2
    position = jnp.where(me % 2 == 0, me // 2, count - 1 - me // 2)
    there = (position + offset + count) % count
    return jnp.where(there < half, 2 * there, 2 * (count - 1 - there) + 1)


def rms_norm(values_in, gain_vec):
    widened = values_in.astype(jnp.float32)
    return (
        widened
        * lax.rsqrt(jnp.mean(widened * widened, axis=-1, keepdims=True) + EPSILON)
        * gain_vec
    )


def block_step(carried, pieces):
    query_blk, key_blk, value_blk, decay_blk = pieces
    length = query_blk.shape[1]
    key_scale = query_blk.shape[2] ** (-0.5)
    cumulative = jnp.cumsum(decay_blk, axis=1)
    log_gap = cumulative[:, :, None] - cumulative[:, None, :]
    causal = lax.broadcasted_iota(jnp.int32, (length, length), 0) >= lax.broadcasted_iota(
        jnp.int32, (length, length), 1
    )
    weight = jnp.where(causal[None], jnp.exp(jnp.minimum(log_gap, 0.0)), 0.0)
    products = jnp.einsum("htd,hsd->hts", query_blk, key_blk, preferred_element_type=jnp.float32)
    scores = (products * key_scale * weight).astype(jnp.bfloat16)
    within = jnp.einsum("hts,hsd->htd", scores, value_blk, preferred_element_type=jnp.float32)
    carried_term = (
        jnp.einsum(
            "htd,hde->hte", query_blk.astype(jnp.float32), carried, precision=lax.Precision.HIGHEST
        )
        * jnp.exp(cumulative)[:, :, None]
    )
    to_end = jnp.exp(cumulative[:, -1:] - cumulative) * key_scale
    scaled_keys = (key_blk.astype(jnp.float32) * to_end[:, :, None]).astype(jnp.bfloat16)
    added = jnp.einsum("hsd,hse->hde", scaled_keys, value_blk, preferred_element_type=jnp.float32)
    carried = jnp.exp(cumulative[:, -1])[:, None, None] * carried + added
    return (carried, within + carried_term)


def to_blocks(matrix, block_len, head_count):
    row_count = matrix.shape[0]
    return matrix.reshape(row_count // block_len, block_len, head_count, -1).transpose(0, 2, 1, 3)


def finish_heads(retention, gates, norm_gain):
    centered = retention - jnp.mean(retention, axis=-1, keepdims=True)
    variance = jnp.mean(centered * centered, axis=-1, keepdims=True)
    normed = centered * lax.rsqrt(variance + EPSILON) * norm_gain[None]
    gate_vals = gates.astype(jnp.float32).reshape(normed.shape)
    return (jax.nn.silu(gate_vals) * normed).reshape(normed.shape[0], -1).astype(jnp.bfloat16)


def share_sum(part, row_count):
    count = lax.axis_size("tp")
    if count != 4:
        return lax.psum_scatter(part, "tp", scatter_dimension=0, tiled=True)
    me = lax.axis_index("tp")
    high, low = me // 2, me % 2
    shares = part.reshape(2, 2, row_count, -1)

    def swap(block, bit):
        return lax.ppermute(block, "tp", [(i, i ^ bit) for i in range(count)])

    def pick(block, index, dim):
        return lax.dynamic_index_in_dim(block, index, dim, False)

    nearer = swap(pick(shares, 1 - low, 1), 1).astype(jnp.float32)
    pair = pick(shares, low, 1).astype(jnp.float32) + nearer
    farther = swap(pick(pair, 1 - high, 0).astype(jnp.bfloat16), 2).astype(jnp.float32)
    return (pick(pair, high, 0) + farther).astype(jnp.bfloat16)


def ring_feed_forward(rows, gate_blocks, up_blocks, down_blocks, shape):
    depth = gate_blocks[0][1].shape[0]
    width = down_blocks[0][1].shape[1]
    half = (len(gate_blocks) + 1) // 2

    def project(blocks):
        total = None
        for some in (blocks[:half], blocks[half:]):
            if not some:
                continue
            columns = jnp.concatenate(
                [
                    lax.dynamic_slice_in_dim(rows, owner_of(offset) * depth, depth, 1)
                    for offset, _ in some
                ],
                axis=1,
            )
            weight = jnp.concatenate([block for _, block in some], axis=0)
            part = jnp.dot(columns, weight, preferred_element_type=jnp.float32)
            total = part if total is None else total + part
        return total

    gate_act = project(gate_blocks)
    up_act = project(up_blocks)
    hidden = (jax.nn.silu(gate_act) * up_act).astype(jnp.bfloat16)
    branch = jnp.zeros(shape, jnp.bfloat16)
    for some in (down_blocks[:half], down_blocks[half:]):
        if not some:
            continue
        wide = jnp.concatenate([block for _, block in some], axis=1)
        part = jnp.dot(hidden, wide, preferred_element_type=jnp.float32).astype(jnp.bfloat16)
        piece = share_sum(part, shape[0])
        for slot, (offset, _) in enumerate(some):
            branch = lax.dynamic_update_slice_in_dim(
                branch, piece[:, slot * width : (slot + 1) * width], owner_of(offset) * width, 1
            )
    return branch


def per_device(
    queries,
    keys,
    values,
    gates,
    log_decay,
    norm_gain,
    out_weight,
    resid,
    post_mix_gain,
    pre_ffn_gain,
    w_gate,
    w_up,
    w_down,
    post_ffn_gain,
):
    ring = lax.axis_size("sp")
    fewer = (ring - 1) // 2
    more = ring - 1 - fewer
    short = ring <= LONGEST_RING
    if short:
        gate_blocks = ring_gather(w_gate, more, fewer)
        up_blocks = ring_gather(w_up, fewer, more)
        down_blocks = ring_gather(w_down, more, fewer)
    row_count = queries.shape[0]
    head_count = log_decay.shape[1]
    head_dim = queries.shape[1] // head_count
    block_count = row_count // BLOCK
    query_blocks = to_blocks(queries, BLOCK, head_count)
    key_blocks = to_blocks(keys, BLOCK, head_count)
    value_blocks = to_blocks(values, BLOCK, head_count)
    decay_blocks = log_decay.reshape(block_count, BLOCK, head_count).transpose(0, 2, 1)
    start_state = jnp.zeros((head_count, head_dim, head_dim), jnp.float32)
    local_state, outputs = lax.scan(
        block_step, start_state, (query_blocks, key_blocks, value_blocks, decay_blocks)
    )
    retention = outputs.transpose(0, 2, 1, 3).reshape(row_count, head_count, head_dim)
    cumulative = jnp.cumsum(log_decay, axis=0)
    local_decay = jnp.exp(cumulative[-1])
    incoming = (entering_by_hops if short else entering)(local_decay, local_state)
    query_rows = queries.reshape(row_count, head_count, head_dim).astype(jnp.float32)
    retention = (
        retention
        + jnp.einsum("thd,hde->the", query_rows, incoming, precision=lax.Precision.HIGHEST)
        * jnp.exp(cumulative)[:, :, None]
    )
    retained = finish_heads(retention, gates, norm_gain)
    quarter = resid.shape[0]
    regrouped = lax.all_to_all(retained, "tp", split_axis=0, concat_axis=1, tiled=True)
    group_rows = out_weight.shape[0]
    empty_mix = jnp.zeros((quarter, out_weight.shape[1]), jnp.float32)
    running = empty_mix
    shard_piece = lax.all_gather(out_weight, "tp", axis=0, tiled=True)
    for offset in range(shard_piece.shape[0] // group_rows):
        columns = lax.dynamic_slice_in_dim(regrouped, offset * group_rows, group_rows, 1)
        part = jnp.dot(
            columns,
            shard_piece[offset * group_rows : (offset + 1) * group_rows],
            preferred_element_type=jnp.float32,
        )
        running = running + part.astype(jnp.bfloat16).astype(jnp.float32)
    mixed = running
    mixed = mixed.astype(jnp.bfloat16)
    middle = (resid.astype(jnp.float32) + rms_norm(mixed, post_mix_gain)).astype(jnp.bfloat16)
    ffn_input = rms_norm(middle, pre_ffn_gain).astype(jnp.bfloat16)
    gathered = lax.all_gather(ffn_input, "tp", axis=0, tiled=True)
    if not short:
        gate_act = jnp.dot(
            gathered,
            lax.all_gather(w_gate, "sp", axis=0, tiled=True),
            preferred_element_type=jnp.float32,
        )
        up_act = jnp.dot(
            gathered,
            lax.all_gather(w_up, "sp", axis=0, tiled=True),
            preferred_element_type=jnp.float32,
        )
        hidden = (jax.nn.silu(gate_act) * up_act).astype(jnp.bfloat16)
        down_full = lax.all_gather(w_down, "sp", axis=1, tiled=True)
        partial = jnp.dot(hidden, down_full, preferred_element_type=jnp.float32)
        branch = lax.psum_scatter(
            partial.astype(jnp.bfloat16), "tp", scatter_dimension=0, tiled=True
        )
    else:
        branch = ring_feed_forward(gathered, gate_blocks, up_blocks, down_blocks, resid.shape)
    return (middle.astype(jnp.float32) + rms_norm(branch, post_ffn_gain)).astype(jnp.bfloat16)


MESH = pl.DeviceIdType.MESH
HEADER_ROWS = 16
F32 = jnp.float32
BF16 = jnp.bfloat16


def silu_of(v):
    return v / (1.0 + jnp.exp(-v))


def layer_kernel(
    q_in,
    k_in,
    v_in,
    gates_in,
    decay_in,
    norm_gain,
    ow_in,
    resid_in,
    mix_gain,
    pre_gain,
    wg_in,
    wu_in,
    wd_in,
    post_gain,
    out,
    q_ref,
    k_ref,
    v_ref,
    gates_ref,
    resid_ref,
    wg,
    wu,
    wd,
    ow,
    cum_row,
    cum_col,
    local_state,
    start_state,
    state_out,
    state_pair,
    total_out,
    total_in,
    retention,
    retained_out,
    retained_in,
    mixed,
    middle,
    rows,
    hidden,
    part_out,
    part_in,
    sum_out,
    sum_in,
    branch,
    local_sem,
    own_sem,
    z_send,
    z_recv,
    y_send,
    y_recv,
    c_send,
    c_recv,
    ow_send,
    ow_recv,
    pair_send,
    pair_recv,
    total_send,
    total_recv,
    ret_send,
    ret_recv,
    rows_send,
    rows_recv,
    part_send,
    part_recv,
    sum_send,
    sum_recv,
):
    sp, tp = lax.axis_index("sp"), lax.axis_index("tp")
    planes = lax.axis_size("sp") // 2
    z, y = sp // 2, sp % 2
    x, core = tp // 2, tp % 2
    parity = z % 2
    pair = z + 1 - 2 * parity
    far = (z + 2) % planes
    far_pair = (pair + 2) % planes
    other_x, other_y, other_core = 1 - x, 1 - y, 1 - core
    is_main = core == parity
    is_helper = core != parity
    sp_y = z * 2 + other_y
    sp_pair = pair * 2 + y
    tp_x = other_x * 2 + core
    tp_core = x * 2 + other_core
    tp_both = other_x * 2 + other_core

    row_count, _ = q_ref.shape
    heads = norm_gain.shape[0]
    dim = norm_gain.shape[1]
    block_count = row_count // BLOCK
    quarter = resid_in.shape[0]
    model = resid_in.shape[1]
    units = wg_in.shape[1]
    tps = ow.shape[0]
    scale = dim ** (-0.5)

    inputs = [
        (k_in, k_ref),
        (v_in, v_ref),
        (q_in, q_ref),
        (gates_in, gates_ref),
        (resid_in, resid_ref),
        (ow_in, ow.at[tp]),
    ]

    def local_copy(i):
        return pltpu.make_async_copy(inputs[i][0], inputs[i][1], local_sem.at[i])

    weights_in = (wg_in, wu_in, wd_in)
    weights = (wg, wu, wd)

    def own_copy(m):
        return pltpu.make_async_copy(weights_in[m], weights[m].at[sp], own_sem.at[m])

    for i in range(len(inputs)):
        local_copy(i).start()

    @pl.when(is_main)
    def _():
        for m in range(3):
            own_copy(m).start()

    def remote(src, dst, send, recv, device):
        return pltpu.make_async_remote_copy(
            src_ref=src,
            dst_ref=dst,
            send_sem=send,
            recv_sem=recv,
            device_id=device,
            device_id_type=MESH,
        )

    barrier = pltpu.get_barrier_semaphore()
    peers = [(((z + i) % planes) * 2 + y, tp) for i in range(1, 4)]
    peers += [(sp_y, tp), (sp, tp_x), (sp, tp_core), (sp, tp_both), (sp_pair, tp_x)]
    for peer in peers:
        pl.semaphore_signal(barrier, inc=1, device_id=peer, device_id_type=MESH)
    pl.semaphore_wait(barrier, len(peers))

    far_target = lax.select(is_main, far, far_pair)

    def z_near(m):
        return remote(
            weights_in[m], weights[m].at[sp], z_send.at[m, 0], z_recv.at[m, z], (pair * 2 + y, tp)
        )

    def z_far(m):
        return remote(
            weights_in[m],
            weights[m].at[sp],
            z_send.at[m, 1],
            z_recv.at[m, z],
            (far_target * 2 + y, tp),
        )

    def start_z(m):
        @pl.when(is_helper)
        def _():
            z_near(m).start()

        z_far(m).start()

    def slot(m, source):
        return weights[m].at[source]

    def to_y(m, plane, src):
        place = plane * 2 + y
        return remote(
            src, slot(m, place), y_send.at[m, plane], y_recv.at[m, plane], (sp_y, tp)
        )

    def to_core(m, place, src):
        return remote(
            src, slot(m, place), c_send.at[m, place], c_recv.at[m, place], (sp, tp_core)
        )

    def z_arrival(m, plane):
        place = plane * 2 + y
        return remote(
            slot(m, place), slot(m, place), z_send.at[m, 1], z_recv.at[m, plane], (sp_y, tp)
        )

    def y_arrival(m, plane):
        place = plane * 2 + other_y
        return remote(
            slot(m, place), slot(m, place), y_send.at[m, plane], y_recv.at[m, plane], (sp_y, tp)
        )

    def start_own(m):
        @pl.when(is_main)
        def _():
            to_y(m, z, weights_in[m]).start()
            to_core(m, sp, weights_in[m]).start()

    def pass_z(m, planes_list):
        @pl.when(is_main)
        def _():
            for plane in planes_list:
                z_arrival(m, plane).wait_recv()
                place = plane * 2 + y
                to_y(m, plane, slot(m, place)).start()
                to_core(m, place, slot(m, place)).start()

    def pass_y(m, planes_list):
        @pl.when(is_main)
        def _():
            for plane in planes_list:
                y_arrival(m, plane).wait_recv()
                place = plane * 2 + other_y
                to_core(m, place, slot(m, place)).start()

    def core_wait(m, planes_list):
        @pl.when(is_helper)
        def _():
            for plane in planes_list:
                for place in (plane * 2 + y, plane * 2 + other_y):
                    to_core(m, place, slot(m, place)).wait_recv()

    def own_wait(m):
        @pl.when(is_main)
        def _():
            own_copy(m).wait()

    start_z(0)
    near_planes = [pair, far, far_pair]
    all_planes = [z] + near_planes

    ow_copies = [
        remote(ow_in, ow.at[tp], ow_send.at[0], ow_recv.at[tp], (sp, tp_x)),
        remote(ow_in, ow.at[tp], ow_send.at[1], ow_recv.at[tp], (sp, tp_core)),
        remote(ow.at[tp_x], ow.at[tp_x], ow_send.at[2], ow_recv.at[tp_x], (sp, tp_core)),
    ]
    ow_copies[0].start()
    ow_copies[1].start()

    for i in range(3):
        local_copy(i).wait()
    row_index = lax.broadcasted_iota(jnp.int32, (BLOCK, BLOCK), 0)
    col_index = lax.broadcasted_iota(jnp.int32, (BLOCK, BLOCK), 1)
    before = jnp.where(row_index <= col_index, 1.0, 0.0)
    until = jnp.where(row_index >= col_index, 1.0, 0.0)
    for b in range(block_count):
        decay = decay_in[:, b * BLOCK : (b + 1) * BLOCK]
        cum_row[b] = jnp.dot(
            decay, before, preferred_element_type=F32, precision=lax.Precision.HIGHEST
        )
        cum_col[b] = lax.dot_general(
            until,
            decay,
            (((1,), (1,)), ((), ())),
            preferred_element_type=F32,
            precision=lax.Precision.HIGHEST,
        )

    def block_decay(b, h):
        return jnp.exp(cum_row[b, h : h + 1, BLOCK - 1 : BLOCK])

    for h in range(heads):
        lanes = slice(h * dim, (h + 1) * dim)
        for b in range(block_count):
            span = slice(b * BLOCK, (b + 1) * BLOCK)
            last = cum_row[b, h : h + 1, BLOCK - 1 : BLOCK]
            to_end = jnp.exp(last - cum_col[b, :, h : h + 1]) * scale
            scaled = (k_ref[span, lanes].astype(F32) * to_end).astype(BF16)
            local_state[b, h] = lax.dot_general(
                scaled, v_ref[span, lanes], (((0,), (0,)), ((), ())), preferred_element_type=F32
            )

    def local_total(h):
        total, decay = local_state[0, h], block_decay(0, h)
        for b in range(1, block_count):
            total = block_decay(b, h) * total + local_state[b, h]
            decay = decay * block_decay(b, h)
        return total, decay

    header_row = lax.broadcasted_iota(jnp.int32, (HEADER_ROWS, dim), 0)

    def pack(ref, h, total, decay):
        ref[h, :dim] = total.astype(BF16)
        wide = jnp.broadcast_to(decay, (HEADER_ROWS, dim))
        high = wide.astype(BF16).astype(F32)
        ref[h, dim:] = jnp.where(header_row < 8, high, wide - high).astype(BF16)

    def unpack(packed, h):
        block = packed[h].astype(F32)
        return block[:dim], block[dim : dim + 1] + block[dim + 8 : dim + 9]

    for h in range(heads):
        total, decay = local_total(h)
        pack(state_out, h, total, decay)
    pair_copy = remote(state_out, state_pair, pair_send.at[0], pair_recv.at[0], (sp_y, tp))
    pair_copy.start()
    start_own(0)

    def scores_of(b):
        for h in range(heads):
            lanes = slice(h * dim, (h + 1) * dim)
            span = slice(b * BLOCK, (b + 1) * BLOCK)
            tile = 128
            keys, vals = k_ref[span, lanes], v_ref[span, lanes]
            row_sums = cum_row[b, h : h + 1, :]

            def one(i, _):
                at = pl.multiple_of(i * tile, tile)
                here = pl.ds(b * BLOCK + at, tile)
                products = lax.dot_general(
                    q_ref[here, lanes], keys, (((1,), (1,)), ((), ())), preferred_element_type=F32
                )
                gap = cum_col[b, pl.ds(at, tile), h : h + 1] - row_sums
                t_index = at + lax.broadcasted_iota(jnp.int32, (tile, BLOCK), 0)
                s_index = lax.broadcasted_iota(jnp.int32, (tile, BLOCK), 1)
                weight = jnp.where(s_index <= t_index, jnp.exp(jnp.minimum(gap, 0.0)), 0.0)
                scores = (products * scale * weight).astype(BF16)
                retention[here, lanes] = jnp.dot(scores, vals, preferred_element_type=F32)
                return 0

            lax.fori_loop(0, BLOCK // tile, one, 0)

    scores_of(0)

    pair_copy.wait_recv()
    for h in range(heads):
        total, decay = local_total(h)
        their_total, their_decay = unpack(state_pair, h)
        last_factor = jnp.where(y == 1, decay, their_decay)
        first = jnp.where(y == 1, their_total, total)
        second = jnp.where(y == 1, total, their_total)
        pack(total_out, h, last_factor * first + second, decay * their_decay)

    def total_copy(plane):
        return remote(
            total_out,
            total_in.at[z],
            total_send.at[plane],
            total_recv.at[z],
            (plane * 2 + y, tp),
        )

    for plane in range(1, 4):

        @pl.when(z < plane)
        def _():
            total_copy(plane).start()

    start_z(1)
    for b in range(1, block_count):
        scores_of(b)

    ow_arrival = [
        remote(ow.at[t], ow.at[t], ow_send.at[0], ow_recv.at[t], (sp, tp_x))
        for t in (tp_x, tp_core, tp_both)
    ]

    for h in range(heads):
        start_state[0, h] = jnp.zeros((dim, dim), F32)
    for plane in range(3):

        @pl.when(plane < z)
        def _():
            remote(
                total_out,
                total_in.at[plane],
                total_send.at[plane],
                total_recv.at[plane],
                (sp_y, tp),
            ).wait_recv()
            for h in range(heads):
                total, decay = unpack(total_in.at[plane], h)
                start_state[0, h] = decay * start_state[0, h] + total

    for h in range(heads):
        their_total, their_decay = unpack(state_pair, h)
        state = start_state[0, h]
        state = jnp.where(y == 1, their_decay * state + their_total, state)
        start_state[0, h] = state
        for b in range(1, block_count):
            state = block_decay(b - 1, h) * state + local_state[b - 1, h]
            start_state[b, h] = state

    local_copy(3).wait()

    def retained_copy(j):
        return remote(
            retained_out.at[j],
            retained_in.at[tp],
            ret_send.at[j],
            ret_recv.at[tp],
            (sp, j),
        )

    per_block = BLOCK // quarter

    def finish(j, target):
        b = j // per_block
        at = pl.multiple_of((j % per_block) * quarter, quarter)
        here = pl.ds(pl.multiple_of(j * quarter, quarter), quarter)
        for h in range(heads):
            lanes = slice(h * dim, (h + 1) * dim)
            state = start_state[b, h]
            high = state.astype(BF16)
            low = (state - high.astype(F32)).astype(BF16)
            query = q_ref[here, lanes]
            carried = jnp.dot(query, high, preferred_element_type=F32) + jnp.dot(
                query, low, preferred_element_type=F32
            )
            kept = retention[here, lanes] + carried * jnp.exp(
                cum_col[b, pl.ds(at, quarter), h : h + 1]
            )
            centered = kept - jnp.mean(kept, axis=-1, keepdims=True)
            variance = jnp.mean(centered * centered, axis=-1, keepdims=True)
            normed = centered * lax.rsqrt(variance + EPSILON) * norm_gain[h : h + 1, :]
            target[:, lanes] = (silu_of(gates_ref[here, lanes].astype(F32)) * normed).astype(BF16)

    others = [(tp + i) % tps for i in range(1, tps)]
    for j in others:
        finish(j, retained_out.at[j])
        retained_copy(j).start()
    finish(tp, retained_in.at[tp])

    pass_z(0, near_planes[:1])
    ow_arrival[0].wait_recv()
    ow_copies[2].start()
    for arrival in ow_arrival[1:]:
        arrival.wait_recv()
    local_copy(5).wait()
    local_copy(4).wait()
    for j in others:
        remote(
            retained_out.at[j],
            retained_in.at[j],
            ret_send.at[j],
            ret_recv.at[j],
            (sp, j),
        ).wait_recv()

    mix_tile = 512

    def mix(i, _):
        here = pl.ds(pl.multiple_of(i * mix_tile, mix_tile), mix_tile)
        total = jnp.zeros((quarter, mix_tile), F32)
        for g in range(tps):
            part = jnp.dot(retained_in[g], ow[g, :, here], preferred_element_type=F32)
            total = total + part.astype(BF16).astype(F32)
        mixed[:, here] = total.astype(BF16)
        return 0

    lax.fori_loop(0, model // mix_tile, mix, 0)

    def rms_of(v):
        return v * lax.rsqrt(jnp.mean(v * v, axis=-1, keepdims=True) + EPSILON)

    mine = x * 2 + parity
    norm_tile = 32

    def into_rows(i, _):
        here = pl.ds(pl.multiple_of(i * norm_tile, norm_tile), norm_tile)
        value = rms_of(mixed[here, :].astype(F32)) * mix_gain[...]
        value = (resid_ref[here, :].astype(F32) + value).astype(BF16)
        middle[here, :] = value
        rows[mine, here, :] = (rms_of(value.astype(F32)) * pre_gain[...]).astype(BF16)
        return 0

    lax.fori_loop(0, quarter // norm_tile, into_rows, 0)

    from_pair = x * 2 + 1 - parity
    from_x = other_x * 2 + parity
    from_both = other_x * 2 + 1 - parity

    def rows_copy(i, place, device):
        return remote(rows.at[place], rows.at[place], rows_send.at[i], rows_recv.at[place], device)

    rows_copy(0, mine, (sp_pair, tp)).start()
    rows_copy(1, mine, (sp, tp_x)).start()
    start_z(2)
    start_own(1)
    start_own(2)
    pass_z(0, near_planes[1:])
    pass_y(0, all_planes)
    pass_z(1, near_planes)
    rows_copy(0, from_pair, (sp_pair, tp)).wait_recv()
    rows_copy(2, from_pair, (sp, tp_x)).start()
    pass_y(1, all_planes)
    own_wait(0)
    own_wait(1)
    core_wait(0, all_planes)
    core_wait(1, all_planes)

    unit_tile = 128

    def gate_up(first):
        def one(i, _):
            here = pl.ds(pl.multiple_of(i * unit_tile, unit_tile), unit_tile)
            both = jnp.concatenate(
                [
                    wg[:, :, here].reshape(model, unit_tile),
                    wu[:, :, here].reshape(model, unit_tile),
                ],
                axis=1,
            )
            acts = jnp.dot(
                rows[pl.ds(first, 2)].reshape(2 * quarter, model), both, preferred_element_type=F32
            )
            value = silu_of(acts[:, :unit_tile]) * acts[:, unit_tile:]
            hidden[pl.ds(first, 2), :, here] = value.astype(BF16).reshape(2, quarter, unit_tile)
            return 0

        lax.fori_loop(0, units // unit_tile, one, 0)

    gate_up(x * 2)
    pass_z(2, near_planes)
    rows_copy(1, from_x, (sp, tp_x)).wait_recv()
    rows_copy(2, from_both, (sp, tp_x)).wait_recv()
    gate_up(other_x * 2)
    own_wait(2)

    columns = model // 8

    def down(plane, half, first):
        product = jnp.dot(
            hidden[pl.ds(first, 2)].reshape(2 * quarter, units),
            wd[plane * 2 + half],
            preferred_element_type=F32,
        )
        return product.reshape(2, quarter, columns)

    def part_copy(plane):
        return remote(
            part_out.at[plane],
            part_in.at[plane],
            part_send.at[plane],
            part_recv.at[plane],
            (sp, tp_x),
        )

    for plane in all_planes:
        pass_y(2, [plane])
        core_wait(2, [plane])
        for half in range(2):
            part_out[plane, :, :, half * columns : (half + 1) * columns] = down(
                plane, half, other_x * 2
            ).astype(BF16)
        part_copy(plane).start()

    def sum_copy(plane):
        return remote(
            sum_out.at[plane],
            sum_in.at[plane],
            sum_send.at[plane],
            sum_recv.at[plane],
            (sp_pair, tp),
        )

    for plane in all_planes:
        own_parts = [down(plane, half, x * 2) for half in range(2)]
        part_copy(plane).wait_recv()
        for half in range(2):
            lanes = slice(half * columns, (half + 1) * columns)
            mine_part = jnp.where(parity == 0, own_parts[half][0], own_parts[half][1])
            pair_part = jnp.where(parity == 0, own_parts[half][1], own_parts[half][0])
            sum_out[plane, :, lanes] = (
                pair_part.astype(BF16).astype(F32)
                + part_in[plane, 1 - parity, :, lanes].astype(F32)
            ).astype(BF16)
            branch[plane, :, lanes] = (
                mine_part.astype(BF16).astype(F32) + part_in[plane, parity, :, lanes].astype(F32)
            )
        sum_copy(plane).start()

    for plane in all_planes:
        sum_copy(plane).wait_recv()

    def final(i, _):
        here = pl.ds(pl.multiple_of(i * norm_tile, norm_tile), norm_tile)
        value = jnp.concatenate(
            [branch[n, here, :] + sum_in[n, here, :].astype(F32) for n in range(planes)], axis=1
        )
        value = rms_of(value.astype(BF16).astype(F32)) * post_gain[...]
        out[here, :] = (middle[here, :].astype(F32) + value).astype(BF16)
        return 0

    lax.fori_loop(0, quarter // norm_tile, final, 0)

    for m in range(3):
        z_far(m).wait_send()

        @pl.when(is_helper)
        def _():
            z_near(m).wait_send()

        @pl.when(is_main)
        def _():
            for plane in all_planes:
                src = weights_in[m] if plane is z else slot(m, plane * 2 + y)
                to_y(m, plane, src).wait_send()
                to_core(m, plane * 2 + y, src).wait_send()
                place = plane * 2 + other_y
                to_core(m, place, slot(m, place)).wait_send()

    for copy in ow_copies:
        copy.wait_send()
    pair_copy.wait_send()
    for plane in range(1, 4):

        @pl.when(z < plane)
        def _():
            total_copy(plane).wait_send()

    for j in others:
        retained_copy(j).wait_send()
    rows_copy(0, mine, (sp_pair, tp)).wait_send()
    rows_copy(1, mine, (sp, tp_x)).wait_send()
    rows_copy(2, from_pair, (sp, tp_x)).wait_send()
    for plane in range(4):
        part_copy(plane).wait_send()
        sum_copy(plane).wait_send()


def whole_layer(
    queries,
    keys,
    values,
    gates,
    log_decay,
    norm_gain,
    out_weight,
    resid,
    post_mix_gain,
    pre_ffn_gain,
    w_gate,
    w_up,
    w_down,
    post_ffn_gain,
):
    places, tps = lax.axis_size("sp"), lax.axis_size("tp")
    planes = places // 2
    row_count, width = queries.shape
    heads, dim = norm_gain.shape
    block_count = row_count // BLOCK
    quarter, model = resid.shape
    depth, units = w_gate.shape
    columns = w_down.shape[1]
    decay_rows = jnp.pad(log_decay.T, ((0, 8 - heads), (0, 0)))
    anywhere = pl.BlockSpec(memory_space=pl.ANY)
    onchip = pl.BlockSpec(memory_space=pltpu.VMEM)
    dma = pltpu.SemaphoreType.DMA
    packed = (heads, dim + HEADER_ROWS, dim)
    scratch = [
        pltpu.VMEM((row_count, width), BF16),
        pltpu.VMEM((row_count, width), BF16),
        pltpu.VMEM((row_count, width), BF16),
        pltpu.VMEM((row_count, width), BF16),
        pltpu.VMEM((quarter, model), BF16),
        pltpu.VMEM((places, depth, units), BF16),
        pltpu.VMEM((places, depth, units), BF16),
        pltpu.VMEM((places, units, columns), BF16),
        pltpu.VMEM((tps, width, model), BF16),
        pltpu.VMEM((block_count, 8, BLOCK), F32),
        pltpu.VMEM((block_count, BLOCK, 8), F32),
        pltpu.VMEM((block_count, heads, dim, dim), F32),
        pltpu.VMEM((block_count, heads, dim, dim), F32),
        pltpu.VMEM(packed, BF16),
        pltpu.VMEM(packed, BF16),
        pltpu.VMEM(packed, BF16),
        pltpu.VMEM((planes,) + packed, BF16),
        pltpu.VMEM((row_count, width), F32),
        pltpu.VMEM((tps, quarter, width), BF16),
        pltpu.VMEM((tps, quarter, width), BF16),
        pltpu.VMEM((quarter, model), BF16),
        pltpu.VMEM((quarter, model), BF16),
        pltpu.VMEM((4, quarter, model), BF16),
        pltpu.VMEM((4, quarter, units), BF16),
        pltpu.VMEM((planes, 2, quarter, 2 * columns), BF16),
        pltpu.VMEM((planes, 2, quarter, 2 * columns), BF16),
        pltpu.VMEM((planes, quarter, 2 * columns), BF16),
        pltpu.VMEM((planes, quarter, 2 * columns), BF16),
        pltpu.VMEM((planes, quarter, 2 * columns), F32),
        dma((6,)),
        dma((3,)),
        dma((3, 2)),
        dma((3, planes)),
        dma((3, planes)),
        dma((3, planes)),
        dma((3, places)),
        dma((3, places)),
        dma((3,)),
        dma((tps,)),
        dma((1,)),
        dma((1,)),
        dma((planes,)),
        dma((planes,)),
        dma((tps,)),
        dma((tps,)),
        dma((3,)),
        dma((4,)),
        dma((planes,)),
        dma((planes,)),
        dma((planes,)),
        dma((planes,)),
    ]
    return pl.pallas_call(
        layer_kernel,
        out_shape=jax.ShapeDtypeStruct((quarter, model), BF16),
        in_specs=[anywhere] * 4
        + [onchip, onchip, anywhere, anywhere, onchip, onchip]
        + [anywhere] * 3
        + [onchip],
        out_specs=onchip,
        scratch_shapes=scratch,
        compiler_params=pltpu.CompilerParams(
            collective_id=0, has_side_effects=True, vmem_limit_bytes=62 * 1024 * 1024
        ),
    )(
        queries,
        keys,
        values,
        gates,
        decay_rows,
        norm_gain,
        out_weight,
        resid,
        post_mix_gain[None],
        pre_ffn_gain[None],
        w_gate,
        w_up,
        w_down,
        post_ffn_gain[None],
    )


def solution(mesh):
    in_specs = (
        P("sp", "tp"),
        P("sp", "tp"),
        P("sp", "tp"),
        P("sp", "tp"),
        P("sp", "tp"),
        P("tp", None),
        P("tp", None),
        P(("sp", "tp"), None),
        P(),
        P(),
        P("sp", "tp"),
        P("sp", "tp"),
        P("tp", "sp"),
        P(),
    )
    out_specs = P(("sp", "tp"), None)
    if mesh.shape["sp"] == LONGEST_RING and mesh.shape["tp"] == 4:
        return jax.shard_map(
            whole_layer, mesh=mesh, in_specs=in_specs, out_specs=out_specs, check_vma=False
        )

    return jax.shard_map(
        per_device, mesh=mesh, in_specs=in_specs, out_specs=out_specs, check_vma=False
    )
```

```python
import jax
import jax.numpy as jnp
from jax import lax
from jax.experimental import pallas as pl
from jax.experimental.pallas import tpu as pltpu
from jax.sharding import PartitionSpec as P


BLOCK = 512


EPSILON = 1e-06
LONGEST_RING = 8


def entering(decay, state):
    place = lax.axis_index("sp")
    head_count, head_dim, _ = state.shape
    decay_rows = jnp.broadcast_to(decay[:, None, None], (head_count, 16, head_dim))
    packed = jnp.concatenate([state, decay_rows], axis=1).astype(jnp.bfloat16)
    gathered = lax.all_gather(packed, "sp")

    def one(step, running):
        piece = lax.dynamic_index_in_dim(gathered, step, 0, False).astype(jnp.float32)
        return piece[:, head_dim : head_dim + 1, :] * running + piece[:, :head_dim]

    return lax.fori_loop(0, place, one, jnp.zeros_like(state))


def from_earlier(packed, distance):
    count = lax.axis_size("sp")
    return lax.ppermute(packed, "sp", [(i, i + distance) for i in range(count - distance)])


def entering_by_hops(decay, state):
    count = lax.axis_size("sp")
    head_count, head_dim, _ = state.shape
    decay_rows = jnp.broadcast_to(decay[:, None, None], (head_count, 8, head_dim))
    packed = jnp.concatenate([state, decay_rows], axis=1)
    near = from_earlier(packed, 1)
    far = from_earlier(packed, 2)
    factor = near[:, head_dim:]
    pair = jnp.concatenate(
        [factor[:, :1] * far[:, :head_dim] + near[:, :head_dim], factor * far[:, head_dim:]],
        axis=1,
    )
    total, factor = pair[:, :head_dim], pair[:, head_dim : head_dim + 1]
    for piece in [from_earlier(pair, distance) for distance in range(2, count, 2)]:
        total = total + factor * piece[:, :head_dim]
        factor = factor * piece[:, head_dim : head_dim + 1]
    return total


def ring_order(count):
    return list(range(0, count, 2)) + list(range(1, count, 2))[::-1]


def ring_gather(block, forward_steps, backward_steps):
    count = lax.axis_size("sp")
    order = ring_order(count)
    ahead = [(order[i], order[(i + 1) % count]) for i in range(count)]
    behind = [(b, a) for a, b in ahead]
    arrived = [(0, block)]
    up, down = block, block
    for step in range(1, max(forward_steps, backward_steps) + 1):
        if step <= forward_steps:
            up = lax.ppermute(up, "sp", ahead)
            arrived.append((-step, up))
        if step <= backward_steps:
            down = lax.ppermute(down, "sp", behind)
            arrived.append((step, down))
    return arrived


def owner_of(offset):
    count = lax.axis_size("sp")
    me = lax.axis_index("sp")
    half = (count + 1) // 2
    position = jnp.where(me % 2 == 0, me // 2, count - 1 - me // 2)
    there = (position + offset + count) % count
    return jnp.where(there < half, 2 * there, 2 * (count - 1 - there) + 1)


def rms_norm(values_in, gain_vec):
    widened = values_in.astype(jnp.float32)
    return (
        widened
        * lax.rsqrt(jnp.mean(widened * widened, axis=-1, keepdims=True) + EPSILON)
        * gain_vec
    )


def block_step(carried, pieces):
    query_blk, key_blk, value_blk, decay_blk = pieces
    length = query_blk.shape[1]
    key_scale = query_blk.shape[2] ** (-0.5)
    cumulative = jnp.cumsum(decay_blk, axis=1)
    log_gap = cumulative[:, :, None] - cumulative[:, None, :]
    causal = lax.broadcasted_iota(jnp.int32, (length, length), 0) >= lax.broadcasted_iota(
        jnp.int32, (length, length), 1
    )
    weight = jnp.where(causal[None], jnp.exp(jnp.minimum(log_gap, 0.0)), 0.0)
    products = jnp.einsum("htd,hsd->hts", query_blk, key_blk, preferred_element_type=jnp.float32)
    scores = (products * key_scale * weight).astype(jnp.bfloat16)
    within = jnp.einsum("hts,hsd->htd", scores, value_blk, preferred_element_type=jnp.float32)
    carried_term = (
        jnp.einsum(
            "htd,hde->hte", query_blk.astype(jnp.float32), carried, precision=lax.Precision.HIGHEST
        )
        * jnp.exp(cumulative)[:, :, None]
    )
    to_end = jnp.exp(cumulative[:, -1:] - cumulative) * key_scale
    scaled_keys = (key_blk.astype(jnp.float32) * to_end[:, :, None]).astype(jnp.bfloat16)
    added = jnp.einsum("hsd,hse->hde", scaled_keys, value_blk, preferred_element_type=jnp.float32)
    carried = jnp.exp(cumulative[:, -1])[:, None, None] * carried + added
    return (carried, within + carried_term)


def to_blocks(matrix, block_len, head_count):
    row_count = matrix.shape[0]
    return matrix.reshape(row_count // block_len, block_len, head_count, -1).transpose(0, 2, 1, 3)


def finish_heads(retention, gates, norm_gain):
    centered = retention - jnp.mean(retention, axis=-1, keepdims=True)
    variance = jnp.mean(centered * centered, axis=-1, keepdims=True)
    normed = centered * lax.rsqrt(variance + EPSILON) * norm_gain[None]
    gate_vals = gates.astype(jnp.float32).reshape(normed.shape)
    return (jax.nn.silu(gate_vals) * normed).reshape(normed.shape[0], -1).astype(jnp.bfloat16)


def share_sum(part, row_count):
    count = lax.axis_size("tp")
    if count != 4:
        return lax.psum_scatter(part, "tp", scatter_dimension=0, tiled=True)
    me = lax.axis_index("tp")
    high, low = me // 2, me % 2
    shares = part.reshape(2, 2, row_count, -1)

    def swap(block, bit):
        return lax.ppermute(block, "tp", [(i, i ^ bit) for i in range(count)])

    def pick(block, index, dim):
        return lax.dynamic_index_in_dim(block, index, dim, False)

    nearer = swap(pick(shares, 1 - low, 1), 1).astype(jnp.float32)
    pair = pick(shares, low, 1).astype(jnp.float32) + nearer
    farther = swap(pick(pair, 1 - high, 0).astype(jnp.bfloat16), 2).astype(jnp.float32)
    return (pick(pair, high, 0) + farther).astype(jnp.bfloat16)


def ring_feed_forward(rows, gate_blocks, up_blocks, down_blocks, shape):
    depth = gate_blocks[0][1].shape[0]
    width = down_blocks[0][1].shape[1]
    half = (len(gate_blocks) + 1) // 2

    def project(blocks):
        total = None
        for some in (blocks[:half], blocks[half:]):
            if not some:
                continue
            columns = jnp.concatenate(
                [
                    lax.dynamic_slice_in_dim(rows, owner_of(offset) * depth, depth, 1)
                    for offset, _ in some
                ],
                axis=1,
            )
            weight = jnp.concatenate([block for _, block in some], axis=0)
            part = jnp.dot(columns, weight, preferred_element_type=jnp.float32)
            total = part if total is None else total + part
        return total

    gate_act = project(gate_blocks)
    up_act = project(up_blocks)
    hidden = (jax.nn.silu(gate_act) * up_act).astype(jnp.bfloat16)
    branch = jnp.zeros(shape, jnp.bfloat16)
    for some in (down_blocks[:half], down_blocks[half:]):
        if not some:
            continue
        wide = jnp.concatenate([block for _, block in some], axis=1)
        part = jnp.dot(hidden, wide, preferred_element_type=jnp.float32).astype(jnp.bfloat16)
        piece = share_sum(part, shape[0])
        for slot, (offset, _) in enumerate(some):
            branch = lax.dynamic_update_slice_in_dim(
                branch, piece[:, slot * width : (slot + 1) * width], owner_of(offset) * width, 1
            )
    return branch


def per_device(
    queries,
    keys,
    values,
    gates,
    log_decay,
    norm_gain,
    out_weight,
    resid,
    post_mix_gain,
    pre_ffn_gain,
    w_gate,
    w_up,
    w_down,
    post_ffn_gain,
):
    ring = lax.axis_size("sp")
    fewer = (ring - 1) // 2
    more = ring - 1 - fewer
    short = ring <= LONGEST_RING
    if short:
        gate_blocks = ring_gather(w_gate, more, fewer)
        up_blocks = ring_gather(w_up, fewer, more)
        down_blocks = ring_gather(w_down, more, fewer)
    row_count = queries.shape[0]
    head_count = log_decay.shape[1]
    head_dim = queries.shape[1] // head_count
    block_count = row_count // BLOCK
    query_blocks = to_blocks(queries, BLOCK, head_count)
    key_blocks = to_blocks(keys, BLOCK, head_count)
    value_blocks = to_blocks(values, BLOCK, head_count)
    decay_blocks = log_decay.reshape(block_count, BLOCK, head_count).transpose(0, 2, 1)
    start_state = jnp.zeros((head_count, head_dim, head_dim), jnp.float32)
    local_state, outputs = lax.scan(
        block_step, start_state, (query_blocks, key_blocks, value_blocks, decay_blocks)
    )
    retention = outputs.transpose(0, 2, 1, 3).reshape(row_count, head_count, head_dim)
    cumulative = jnp.cumsum(log_decay, axis=0)
    local_decay = jnp.exp(cumulative[-1])
    incoming = (entering_by_hops if short else entering)(local_decay, local_state)
    query_rows = queries.reshape(row_count, head_count, head_dim).astype(jnp.float32)
    retention = (
        retention
        + jnp.einsum("thd,hde->the", query_rows, incoming, precision=lax.Precision.HIGHEST)
        * jnp.exp(cumulative)[:, :, None]
    )
    retained = finish_heads(retention, gates, norm_gain)
    quarter = resid.shape[0]
    regrouped = lax.all_to_all(retained, "tp", split_axis=0, concat_axis=1, tiled=True)
    group_rows = out_weight.shape[0]
    empty_mix = jnp.zeros((quarter, out_weight.shape[1]), jnp.float32)
    running = empty_mix
    shard_piece = lax.all_gather(out_weight, "tp", axis=0, tiled=True)
    for offset in range(shard_piece.shape[0] // group_rows):
        columns = lax.dynamic_slice_in_dim(regrouped, offset * group_rows, group_rows, 1)
        part = jnp.dot(
            columns,
            shard_piece[offset * group_rows : (offset + 1) * group_rows],
            preferred_element_type=jnp.float32,
        )
        running = running + part.astype(jnp.bfloat16).astype(jnp.float32)
    mixed = running
    mixed = mixed.astype(jnp.bfloat16)
    middle = (resid.astype(jnp.float32) + rms_norm(mixed, post_mix_gain)).astype(jnp.bfloat16)
    ffn_input = rms_norm(middle, pre_ffn_gain).astype(jnp.bfloat16)
    gathered = lax.all_gather(ffn_input, "tp", axis=0, tiled=True)
    if not short:
        gate_act = jnp.dot(
            gathered,
            lax.all_gather(w_gate, "sp", axis=0, tiled=True),
            preferred_element_type=jnp.float32,
        )
        up_act = jnp.dot(
            gathered,
            lax.all_gather(w_up, "sp", axis=0, tiled=True),
            preferred_element_type=jnp.float32,
        )
        hidden = (jax.nn.silu(gate_act) * up_act).astype(jnp.bfloat16)
        down_full = lax.all_gather(w_down, "sp", axis=1, tiled=True)
        partial = jnp.dot(hidden, down_full, preferred_element_type=jnp.float32)
        branch = lax.psum_scatter(
            partial.astype(jnp.bfloat16), "tp", scatter_dimension=0, tiled=True
        )
    else:
        branch = ring_feed_forward(gathered, gate_blocks, up_blocks, down_blocks, resid.shape)
    return (middle.astype(jnp.float32) + rms_norm(branch, post_ffn_gain)).astype(jnp.bfloat16)


MESH = pl.DeviceIdType.MESH
HEADER_ROWS = 16
F32 = jnp.float32
BF16 = jnp.bfloat16


def silu_of(v):
    return v / (1.0 + jnp.exp(-v))


def layer_kernel(
    q_in,
    k_in,
    v_in,
    gates_in,
    decay_in,
    norm_gain,
    ow_in,
    resid_in,
    mix_gain,
    pre_gain,
    wg_in,
    wu_in,
    wd_in,
    post_gain,
    out,
    q_ref,
    k_ref,
    v_ref,
    gates_ref,
    resid_ref,
    wg,
    wu,
    wd,
    ow,
    cum_row,
    cum_col,
    local_state,
    start_state,
    state_out,
    state_pair,
    total_out,
    total_in,
    retention,
    retained_out,
    retained_in,
    mixed,
    middle,
    rows,
    gate_acts,
    hidden,
    part_out,
    part_in,
    sum_out,
    sum_in,
    branch,
    local_sem,
    own_sem,
    z_send,
    z_recv,
    y_send,
    y_recv,
    c_send,
    c_recv,
    ow_send,
    ow_recv,
    pair_send,
    pair_recv,
    total_send,
    total_recv,
    ret_send,
    ret_recv,
    rows_send,
    rows_recv,
    part_send,
    part_recv,
    sum_send,
    sum_recv,
):
    sp, tp = lax.axis_index("sp"), lax.axis_index("tp")
    planes = lax.axis_size("sp") // 2
    z, y = sp // 2, sp % 2
    x, core = tp // 2, tp % 2
    parity = z % 2
    pair = z + 1 - 2 * parity
    far = (z + 2) % planes
    far_pair = (pair + 2) % planes
    other_x, other_y, other_core = 1 - x, 1 - y, 1 - core
    is_main = core == parity
    is_helper = core != parity
    sp_y = z * 2 + other_y
    sp_pair = pair * 2 + y
    tp_x = other_x * 2 + core
    tp_core = x * 2 + other_core
    tp_both = other_x * 2 + other_core

    row_count, _ = q_ref.shape
    heads = norm_gain.shape[0]
    dim = norm_gain.shape[1]
    block_count = row_count // BLOCK
    quarter = resid_in.shape[0]
    model = resid_in.shape[1]
    units = wg_in.shape[1]
    tps = ow.shape[0]
    scale = dim ** (-0.5)

    inputs = [
        (k_in, k_ref),
        (v_in, v_ref),
        (q_in, q_ref),
        (gates_in, gates_ref),
        (resid_in, resid_ref),
        (ow_in, ow.at[tp]),
    ]

    def local_copy(i):
        return pltpu.make_async_copy(inputs[i][0], inputs[i][1], local_sem.at[i])

    weights_in = (wg_in, wu_in, wd_in)
    weights = (wg, wu, wd)

    def own_copy(m):
        return pltpu.make_async_copy(weights_in[m], weights[m].at[sp], own_sem.at[m])

    for i in range(len(inputs)):
        local_copy(i).start()

    @pl.when(is_main)
    def _():
        for m in range(3):
            own_copy(m).start()

    def remote(src, dst, send, recv, device):
        return pltpu.make_async_remote_copy(
            src_ref=src,
            dst_ref=dst,
            send_sem=send,
            recv_sem=recv,
            device_id=device,
            device_id_type=MESH,
        )

    barrier = pltpu.get_barrier_semaphore()
    peers = [(((z + i) % planes) * 2 + y, tp) for i in range(1, 4)]
    peers += [(sp_y, tp), (sp, tp_x), (sp, tp_core), (sp, tp_both), (sp_pair, tp_x)]
    for peer in peers:
        pl.semaphore_signal(barrier, inc=1, device_id=peer, device_id_type=MESH)
    pl.semaphore_wait(barrier, len(peers))

    far_target = lax.select(is_main, far, far_pair)
    in_middle = jnp.logical_and(z > 0, z < planes - 1)
    at_end = jnp.logical_or(z == 0, z == planes - 1)

    def cut(ref, half):
        size = ref.shape[0] // 2
        return ref.at[half * size : (half + 1) * size]

    def source(m, half):
        return cut(weights_in[m], half)

    def slot(m, half, place):
        size = weights[m].shape[1] // 2
        return weights[m].at[place, half * size : (half + 1) * size]

    def z_near(m, half):
        piece = 2 * m + half
        return remote(
            source(m, half),
            slot(m, half, sp),
            z_send.at[piece, 0],
            z_recv.at[piece, z],
            (pair * 2 + y, tp),
        )

    def z_far(m, half):
        piece = 2 * m + half
        return remote(
            source(m, half),
            slot(m, half, sp),
            z_send.at[piece, 1],
            z_recv.at[piece, z],
            (far_target * 2 + y, tp),
        )

    def to_y(m, half, plane, src):
        piece, place = 2 * m + half, plane * 2 + y
        return remote(
            src,
            slot(m, half, place),
            y_send.at[piece, plane],
            y_recv.at[piece, plane],
            (sp_y, tp),
        )

    def to_core(m, half, place, src):
        piece = 2 * m + half
        return remote(
            src,
            slot(m, half, place),
            c_send.at[piece, place],
            c_recv.at[piece, place],
            (sp, tp_core),
        )

    def z_arrival(m, half, plane):
        piece, here = 2 * m + half, slot(m, half, plane * 2 + y)
        return remote(here, here, z_send.at[piece, 1], z_recv.at[piece, plane], (sp_y, tp))

    def y_arrival(m, half, plane):
        piece, here = 2 * m + half, slot(m, half, plane * 2 + other_y)
        return remote(here, here, y_send.at[piece, plane], y_recv.at[piece, plane], (sp_y, tp))

    def start_own(m):
        @pl.when(is_main)
        def _():
            for half in range(2):
                to_y(m, half, z, source(m, half)).start()
                to_core(m, half, sp, source(m, half)).start()

    def pass_plane(m, half, plane):
        z_arrival(m, half, plane).wait_recv()
        here = slot(m, half, plane * 2 + y)
        to_y(m, half, plane, here).start()
        to_core(m, half, plane * 2 + y, here).start()

    def pass_z(m, half, planes_list):
        @pl.when(is_main)
        def _():
            for plane in planes_list:
                pass_plane(m, half, plane)

    def pass_if(condition, m, half, plane):
        @pl.when(jnp.logical_and(condition, is_main))
        def _():
            pass_plane(m, half, plane)

    def pass_y(m, half, planes_list):
        @pl.when(is_main)
        def _():
            for plane in planes_list:
                y_arrival(m, half, plane).wait_recv()
                place = plane * 2 + other_y
                to_core(m, half, place, slot(m, half, place)).start()

    def core_wait(m, planes_list):
        @pl.when(is_helper)
        def _():
            for plane in planes_list:
                for half in range(2):
                    for place in (plane * 2 + y, plane * 2 + other_y):
                        here = slot(m, half, place)
                        to_core(m, half, place, here).wait_recv()

    def own_wait(m):
        @pl.when(is_main)
        def _():
            own_copy(m).wait()

    near_up = parity == 0
    far_up = z < planes // 2
    near_down, far_down = parity == 1, z >= planes // 2
    one_hop = jnp.logical_and(in_middle, is_helper)
    more_hops = jnp.logical_or(at_end, is_main)
    both = jnp.logical_and

    def when_do(condition, do):
        @pl.when(condition)
        def _():
            do()

    def start_far(m, half, condition):
        when_do(condition, lambda: z_far(m, half).start())

    def start_near(m, half, condition):
        when_do(both(is_helper, condition), lambda: z_near(m, half).start())

    when_do(is_helper, lambda: z_near(0, 0).start())
    start_far(0, 0, jnp.logical_or(far_down, one_hop))
    start_near(0, 1, near_down)
    start_far(0, 1, far_down)
    near_planes = [pair, far, far_pair]
    all_planes = [z] + near_planes

    ow_copies = [
        remote(ow_in, ow.at[tp], ow_send.at[0], ow_recv.at[tp], (sp, tp_x)),
        remote(ow_in, ow.at[tp], ow_send.at[1], ow_recv.at[tp], (sp, tp_core)),
        remote(ow.at[tp_x], ow.at[tp_x], ow_send.at[2], ow_recv.at[tp_x], (sp, tp_core)),
    ]
    ow_copies[0].start()
    ow_copies[1].start()

    for i in range(3):
        local_copy(i).wait()

    row_index = lax.broadcasted_iota(jnp.int32, (BLOCK, BLOCK), 0)
    col_index = lax.broadcasted_iota(jnp.int32, (BLOCK, BLOCK), 1)
    before = jnp.where(row_index <= col_index, 1.0, 0.0)
    until = jnp.where(row_index >= col_index, 1.0, 0.0)
    for b in range(block_count):
        decay = decay_in[:, b * BLOCK : (b + 1) * BLOCK]
        cum_row[b] = jnp.dot(
            decay, before, preferred_element_type=F32, precision=lax.Precision.HIGHEST
        )
        cum_col[b] = lax.dot_general(
            until,
            decay,
            (((1,), (1,)), ((), ())),
            preferred_element_type=F32,
            precision=lax.Precision.HIGHEST,
        )

    def block_decay(b, h):
        return jnp.exp(cum_row[b, h : h + 1, BLOCK - 1 : BLOCK])

    for h in range(heads):
        lanes = slice(h * dim, (h + 1) * dim)
        for b in range(block_count):
            span = slice(b * BLOCK, (b + 1) * BLOCK)
            last = cum_row[b, h : h + 1, BLOCK - 1 : BLOCK]
            to_end = jnp.exp(last - cum_col[b, :, h : h + 1]) * scale
            scaled = (k_ref[span, lanes].astype(F32) * to_end).astype(BF16)
            local_state[b, h] = lax.dot_general(
                scaled, v_ref[span, lanes], (((0,), (0,)), ((), ())), preferred_element_type=F32
            )

    def local_total(h):
        total, decay = local_state[0, h], block_decay(0, h)
        for b in range(1, block_count):
            total = block_decay(b, h) * total + local_state[b, h]
            decay = decay * block_decay(b, h)
        return total, decay

    header_row = lax.broadcasted_iota(jnp.int32, (HEADER_ROWS, dim), 0)

    def pack(ref, h, total, decay):
        ref[h, :dim] = total.astype(BF16)
        wide = jnp.broadcast_to(decay, (HEADER_ROWS, dim))
        high = wide.astype(BF16).astype(F32)
        ref[h, dim:] = jnp.where(header_row < 8, high, wide - high).astype(BF16)

    def unpack(packed, h):
        block = packed[h].astype(F32)
        return block[:dim], block[dim : dim + 1] + block[dim + 8 : dim + 9]

    for h in range(heads):
        total, decay = local_total(h)
        pack(state_out, h, total, decay)
    pair_copy = remote(state_out, state_pair, pair_send.at[0], pair_recv.at[0], (sp_y, tp))
    pair_copy.start()
    start_own(0)

    def scores_of(b):
        for h in range(heads):
            lanes = slice(h * dim, (h + 1) * dim)
            span = slice(b * BLOCK, (b + 1) * BLOCK)
            tile = 128
            keys, vals = k_ref[span, lanes], v_ref[span, lanes]
            row_sums = cum_row[b, h : h + 1, :]

            def one(i, _):
                at = pl.multiple_of(i * tile, tile)
                here = pl.ds(b * BLOCK + at, tile)
                products = lax.dot_general(
                    q_ref[here, lanes], keys, (((1,), (1,)), ((), ())), preferred_element_type=F32
                )
                gap = cum_col[b, pl.ds(at, tile), h : h + 1] - row_sums
                t_index = at + lax.broadcasted_iota(jnp.int32, (tile, BLOCK), 0)
                s_index = lax.broadcasted_iota(jnp.int32, (tile, BLOCK), 1)
                weight = jnp.where(s_index <= t_index, jnp.exp(jnp.minimum(gap, 0.0)), 0.0)
                scores = (products * scale * weight).astype(BF16)
                retention[here, lanes] = jnp.dot(scores, vals, preferred_element_type=F32)
                return 0

            lax.fori_loop(0, BLOCK // tile, one, 0)

    scores_of(0)

    pair_copy.wait_recv()
    for h in range(heads):
        total, decay = local_total(h)
        their_total, their_decay = unpack(state_pair, h)
        last_factor = jnp.where(y == 1, decay, their_decay)
        first = jnp.where(y == 1, their_total, total)
        second = jnp.where(y == 1, total, their_total)
        pack(total_out, h, last_factor * first + second, decay * their_decay)

    def total_copy(plane):
        return remote(
            total_out,
            total_in.at[z],
            total_send.at[plane],
            total_recv.at[z],
            (plane * 2 + y, tp),
        )

    for plane in range(1, 4):

        @pl.when(z < plane)
        def _():
            total_copy(plane).start()


    for half in range(2):
        start_far(1, half, both(far_down, in_middle))
        start_near(1, half, near_down)
    for b in range(1, block_count):
        scores_of(b)

    ow_arrival = [
        remote(ow.at[t], ow.at[t], ow_send.at[0], ow_recv.at[t], (sp, tp_x))
        for t in (tp_x, tp_core, tp_both)
    ]

    for h in range(heads):
        start_state[0, h] = jnp.zeros((dim, dim), F32)
    for plane in range(3):

        @pl.when(plane < z)
        def _():
            remote(
                total_out,
                total_in.at[plane],
                total_send.at[plane],
                total_recv.at[plane],
                (sp_y, tp),
            ).wait_recv()
            for h in range(heads):
                total, decay = unpack(total_in.at[plane], h)
                start_state[0, h] = decay * start_state[0, h] + total

    for h in range(heads):
        their_total, their_decay = unpack(state_pair, h)
        state = start_state[0, h]
        state = jnp.where(y == 1, their_decay * state + their_total, state)
        start_state[0, h] = state
        for b in range(1, block_count):
            state = block_decay(b - 1, h) * state + local_state[b - 1, h]
            start_state[b, h] = state

    local_copy(3).wait()

    def retained_copy(j):
        return remote(
            retained_out.at[j],
            retained_in.at[tp],
            ret_send.at[j],
            ret_recv.at[tp],
            (sp, j),
        )

    per_block = BLOCK // quarter

    def finish(j, target):
        b = j // per_block
        at = pl.multiple_of((j % per_block) * quarter, quarter)
        here = pl.ds(pl.multiple_of(j * quarter, quarter), quarter)
        for h in range(heads):
            lanes = slice(h * dim, (h + 1) * dim)
            state = start_state[b, h]
            high = state.astype(BF16)
            low = (state - high.astype(F32)).astype(BF16)
            query = q_ref[here, lanes]
            carried = jnp.dot(query, high, preferred_element_type=F32) + jnp.dot(
                query, low, preferred_element_type=F32
            )
            kept = retention[here, lanes] + carried * jnp.exp(
                cum_col[b, pl.ds(at, quarter), h : h + 1]
            )
            centered = kept - jnp.mean(kept, axis=-1, keepdims=True)
            variance = jnp.mean(centered * centered, axis=-1, keepdims=True)
            normed = centered * lax.rsqrt(variance + EPSILON) * norm_gain[h : h + 1, :]
            target[:, lanes] = (silu_of(gates_ref[here, lanes].astype(F32)) * normed).astype(BF16)

    others = [(tp + i) % tps for i in range(1, tps)]
    start_near(0, 1, near_up)
    start_far(0, 0, both(far_up, more_hops))
    start_far(0, 1, far_up)
    for half in range(2):
        start_far(1, half, both(far_up, in_middle))
        start_near(1, half, near_up)

    for j in others:
        finish(j, retained_out.at[j])
        retained_copy(j).start()
    finish(tp, retained_in.at[tp])

    pass_z(0, 0, near_planes[:1])
    start_own(1)
    ow_arrival[0].wait_recv()
    ow_copies[2].start()
    for arrival in ow_arrival[1:]:
        arrival.wait_recv()
    local_copy(5).wait()
    local_copy(4).wait()
    for j in others:
        remote(
            retained_out.at[j],
            retained_in.at[j],
            ret_send.at[j],
            ret_recv.at[j],
            (sp, j),
        ).wait_recv()

    mix_tile = 512

    def mix(i, _):
        here = pl.ds(pl.multiple_of(i * mix_tile, mix_tile), mix_tile)
        total = jnp.zeros((quarter, mix_tile), F32)
        for g in range(tps):
            part = jnp.dot(retained_in[g], ow[g, :, here], preferred_element_type=F32)
            total = total + part.astype(BF16).astype(F32)
        mixed[:, here] = total.astype(BF16)
        return 0

    lax.fori_loop(0, model // mix_tile, mix, 0)

    def rms_of(v):
        return v * lax.rsqrt(jnp.mean(v * v, axis=-1, keepdims=True) + EPSILON)

    mine = x * 2 + parity
    norm_tile = 32

    def into_rows(i, _):
        here = pl.ds(pl.multiple_of(i * norm_tile, norm_tile), norm_tile)
        value = rms_of(mixed[here, :].astype(F32)) * mix_gain[...]
        value = (resid_ref[here, :].astype(F32) + value).astype(BF16)
        middle[here, :] = value
        rows[mine, here, :] = (rms_of(value.astype(F32)) * pre_gain[...]).astype(BF16)
        return 0

    from_pair = x * 2 + 1 - parity
    from_x = other_x * 2 + parity
    from_both = other_x * 2 + 1 - parity
    half_rows = quarter // 2

    def rows_copy(i, half, place, device):
        here = rows.at[place, half * half_rows : (half + 1) * half_rows]
        return remote(here, here, rows_send.at[i, half], rows_recv.at[place, half], device)

    for half in range(2):
        steps = half_rows // norm_tile
        lax.fori_loop(half * steps, (half + 1) * steps, into_rows, 0)
        rows_copy(0, half, mine, (sp_pair, tp)).start()
        rows_copy(1, half, mine, (sp, tp_x)).start()

    for half in range(2):
        start_far(2, half, one_hop)
    pass_z(0, 1, near_planes[:1])
    pass_z(0, 0, near_planes[1:])
    pass_z(0, 1, near_planes[1:])
    for half in range(2):
        pass_z(1, half, near_planes[:1])
    rows_copy(0, 0, from_pair, (sp_pair, tp)).wait_recv()
    rows_copy(2, 0, from_pair, (sp, tp_x)).start()
    for half in range(2):
        start_far(1, half, at_end)
    start_own(2)
    for half in range(2):
        pass_if(at_end, 1, half, far)
        pass_if(in_middle, 1, half, far_pair)
    rows_copy(0, 1, from_pair, (sp_pair, tp)).wait_recv()
    rows_copy(2, 1, from_pair, (sp, tp_x)).start()
    for half in range(2):
        when_do(is_helper, lambda: z_near(2, half).start())
        start_far(2, half, more_hops)
    for half in range(2):
        pass_y(0, half, all_planes)
    own_wait(0)
    core_wait(0, all_planes)

    unit_tile = 256
    unit_steps = units // unit_tile

    def acts_of(weight, first, at, size):
        here = pl.ds(at, size)
        return jnp.dot(
            rows[pl.ds(first, 2)].reshape(2 * quarter, model),
            weight[:, :, here].reshape(model, size),
            preferred_element_type=F32,
        ).reshape(2, quarter, size)

    def over_units(one):
        def step(i, _):
            one(pl.multiple_of(i * unit_tile, unit_tile), unit_tile)
            return 0

        lax.fori_loop(0, unit_steps, step, 0)
        if units % unit_tile:
            one(unit_steps * unit_tile, units % unit_tile)

    def gate_of(first):
        def one(at, size):
            gate_acts[pl.ds(first, 2), :, pl.ds(at, size)] = acts_of(wg, first, at, size)

        over_units(one)

    def up_of(first):
        def one(at, size):
            here = pl.ds(at, size)
            gate = gate_acts[pl.ds(first, 2), :, here]
            value = silu_of(gate) * acts_of(wu, first, at, size)
            hidden[pl.ds(first, 2), :, here] = value.astype(BF16)

        over_units(one)

    gate_of(x * 2)
    pass_if(at_end, 1, 0, far_pair)
    pass_if(in_middle, 1, 0, far)
    pass_if(at_end, 1, 1, far_pair)
    pass_if(in_middle, 1, 1, far)
    for half in range(2):
        rows_copy(1, half, from_x, (sp, tp_x)).wait_recv()
        rows_copy(2, half, from_both, (sp, tp_x)).wait_recv()
    gate_of(other_x * 2)
    pass_z(2, 0, near_planes[:1])
    pass_y(1, 0, all_planes)
    for half in range(2):
        pass_if(in_middle, 2, half, far_pair)
    pass_y(1, 1, all_planes)
    pass_if(at_end, 2, 0, far)
    pass_if(at_end, 2, 0, far_pair)
    pass_if(in_middle, 2, 0, far)
    own_wait(1)
    core_wait(1, all_planes)

    columns = model // 8

    def down(plane, half, first):
        product = jnp.dot(
            hidden[pl.ds(first, 2)].reshape(2 * quarter, units),
            wd[plane * 2 + half],
            preferred_element_type=F32,
        )
        return product.reshape(2, quarter, columns)

    def part_copy(plane):
        return remote(
            part_out.at[plane],
            part_in.at[plane],
            part_send.at[plane],
            part_recv.at[plane],
            (sp, tp_x),
        )

    def part_of(plane):
        for half in range(2):
            pass_y(2, half, [plane])
        core_wait(2, [plane])
        for half in range(2):
            part_out[plane, :, :, half * columns : (half + 1) * columns] = down(
                plane, half, other_x * 2
            ).astype(BF16)
        part_copy(plane).start()

    up_of(other_x * 2)
    own_wait(2)
    part_of(z)
    pass_z(2, 1, near_planes[:1])
    pass_if(at_end, 2, 1, far)
    pass_if(at_end, 2, 1, far_pair)
    pass_if(in_middle, 2, 1, far)
    part_of(near_planes[0])
    up_of(x * 2)
    for plane in near_planes[1:]:
        part_of(plane)

    def sum_copy(plane):
        return remote(
            sum_out.at[plane],
            sum_in.at[plane],
            sum_send.at[plane],
            sum_recv.at[plane],
            (sp_pair, tp),
        )

    for plane in all_planes:
        own_parts = [down(plane, half, x * 2) for half in range(2)]
        part_copy(plane).wait_recv()
        for half in range(2):
            lanes = slice(half * columns, (half + 1) * columns)
            mine_part = jnp.where(parity == 0, own_parts[half][0], own_parts[half][1])
            pair_part = jnp.where(parity == 0, own_parts[half][1], own_parts[half][0])
            sum_out[plane, :, lanes] = (
                pair_part.astype(BF16).astype(F32)
                + part_in[plane, 1 - parity, :, lanes].astype(F32)
            ).astype(BF16)
            branch[plane, :, lanes] = (
                mine_part.astype(BF16).astype(F32) + part_in[plane, parity, :, lanes].astype(F32)
            )
        sum_copy(plane).start()

    for plane in all_planes:
        sum_copy(plane).wait_recv()

    def final(i, _):
        here = pl.ds(pl.multiple_of(i * norm_tile, norm_tile), norm_tile)
        value = jnp.concatenate(
            [branch[n, here, :] + sum_in[n, here, :].astype(F32) for n in range(planes)], axis=1
        )
        value = rms_of(value.astype(BF16).astype(F32)) * post_gain[...]
        out[here, :] = (middle[here, :].astype(F32) + value).astype(BF16)
        return 0

    lax.fori_loop(0, quarter // norm_tile, final, 0)

    for m in range(3):
        for half in range(2):
            z_far(m, half).wait_send()
            when_do(is_helper, lambda: z_near(m, half).wait_send())

            @pl.when(is_main)
            def _():
                for plane in all_planes:
                    place = plane * 2 + y
                    src = source(m, half) if plane is z else slot(m, half, place)
                    to_y(m, half, plane, src).wait_send()
                    to_core(m, half, place, src).wait_send()
                    place = plane * 2 + other_y
                    to_core(m, half, place, slot(m, half, place)).wait_send()

    for copy in ow_copies:
        copy.wait_send()
    pair_copy.wait_send()
    for plane in range(1, 4):

        @pl.when(z < plane)
        def _():
            total_copy(plane).wait_send()

    for j in others:
        retained_copy(j).wait_send()
    for half in range(2):
        rows_copy(0, half, mine, (sp_pair, tp)).wait_send()
        rows_copy(1, half, mine, (sp, tp_x)).wait_send()
        rows_copy(2, half, from_pair, (sp, tp_x)).wait_send()
    for plane in range(4):
        part_copy(plane).wait_send()
        sum_copy(plane).wait_send()


def whole_layer(
    queries,
    keys,
    values,
    gates,
    log_decay,
    norm_gain,
    out_weight,
    resid,
    post_mix_gain,
    pre_ffn_gain,
    w_gate,
    w_up,
    w_down,
    post_ffn_gain,
):
    places, tps = lax.axis_size("sp"), lax.axis_size("tp")
    planes = places // 2
    row_count, width = queries.shape
    heads, dim = norm_gain.shape
    block_count = row_count // BLOCK
    quarter, model = resid.shape
    depth, units = w_gate.shape
    columns = w_down.shape[1]
    decay_rows = jnp.pad(log_decay.T, ((0, 8 - heads), (0, 0)))
    anywhere = pl.BlockSpec(memory_space=pl.ANY)
    onchip = pl.BlockSpec(memory_space=pltpu.VMEM)
    dma = pltpu.SemaphoreType.DMA
    packed = (heads, dim + HEADER_ROWS, dim)
    scratch = [
        pltpu.VMEM((row_count, width), BF16),
        pltpu.VMEM((row_count, width), BF16),
        pltpu.VMEM((row_count, width), BF16),
        pltpu.VMEM((row_count, width), BF16),
        pltpu.VMEM((quarter, model), BF16),
        pltpu.VMEM((places, depth, units), BF16),
        pltpu.VMEM((places, depth, units), BF16),
        pltpu.VMEM((places, units, columns), BF16),
        pltpu.VMEM((tps, width, model), BF16),
        pltpu.VMEM((block_count, 8, BLOCK), F32),
        pltpu.VMEM((block_count, BLOCK, 8), F32),
        pltpu.VMEM((block_count, heads, dim, dim), F32),
        pltpu.VMEM((block_count, heads, dim, dim), F32),
        pltpu.VMEM(packed, BF16),
        pltpu.VMEM(packed, BF16),
        pltpu.VMEM(packed, BF16),
        pltpu.VMEM((planes,) + packed, BF16),
        pltpu.VMEM((row_count, width), F32),
        pltpu.VMEM((tps, quarter, width), BF16),
        pltpu.VMEM((tps, quarter, width), BF16),
        pltpu.VMEM((quarter, model), BF16),
        pltpu.VMEM((quarter, model), BF16),
        pltpu.VMEM((4, quarter, model), BF16),
        pltpu.VMEM((4, quarter, units), F32),
        pltpu.VMEM((4, quarter, units), BF16),
        pltpu.VMEM((planes, 2, quarter, 2 * columns), BF16),
        pltpu.VMEM((planes, 2, quarter, 2 * columns), BF16),
        pltpu.VMEM((planes, quarter, 2 * columns), BF16),
        pltpu.VMEM((planes, quarter, 2 * columns), BF16),
        pltpu.VMEM((planes, quarter, 2 * columns), F32),
        dma((6,)),
        dma((3,)),
        dma((6, 2)),
        dma((6, planes)),
        dma((6, planes)),
        dma((6, planes)),
        dma((6, places)),
        dma((6, places)),
        dma((3,)),
        dma((tps,)),
        dma((1,)),
        dma((1,)),
        dma((planes,)),
        dma((planes,)),
        dma((tps,)),
        dma((tps,)),
        dma((3, 2)),
        dma((4, 2)),
        dma((planes,)),
        dma((planes,)),
        dma((planes,)),
        dma((planes,)),
    ]
    return pl.pallas_call(
        layer_kernel,
        out_shape=jax.ShapeDtypeStruct((quarter, model), BF16),
        in_specs=[anywhere] * 4
        + [onchip, onchip, anywhere, anywhere, onchip, onchip]
        + [anywhere] * 3
        + [onchip],
        out_specs=onchip,
        scratch_shapes=scratch,
        compiler_params=pltpu.CompilerParams(
            collective_id=0, has_side_effects=True, vmem_limit_bytes=62 * 1024 * 1024
        ),
    )(
        queries,
        keys,
        values,
        gates,
        decay_rows,
        norm_gain,
        out_weight,
        resid,
        post_mix_gain[None],
        pre_ffn_gain[None],
        w_gate,
        w_up,
        w_down,
        post_ffn_gain[None],
    )


def solution(mesh):
    in_specs = (
        P("sp", "tp"),
        P("sp", "tp"),
        P("sp", "tp"),
        P("sp", "tp"),
        P("sp", "tp"),
        P("tp", None),
        P("tp", None),
        P(("sp", "tp"), None),
        P(),
        P(),
        P("sp", "tp"),
        P("sp", "tp"),
        P("tp", "sp"),
        P(),
    )
    out_specs = P(("sp", "tp"), None)
    if mesh.shape["sp"] == LONGEST_RING and mesh.shape["tp"] == 4:
        return jax.shard_map(
            whole_layer, mesh=mesh, in_specs=in_specs, out_specs=out_specs, check_vma=False
        )

    return jax.shard_map(
        per_device, mesh=mesh, in_specs=in_specs, out_specs=out_specs, check_vma=False
    )
```

```python
import jax
import jax.numpy as jnp
from jax import lax
from jax.experimental import pallas as pl
from jax.experimental.pallas import tpu as pltpu
from jax.sharding import PartitionSpec as P


BLOCK = 512


EPSILON = 1e-06
LONGEST_RING = 8


def entering(decay, state):
    place = lax.axis_index("sp")
    head_count, head_dim, _ = state.shape
    decay_rows = jnp.broadcast_to(decay[:, None, None], (head_count, 16, head_dim))
    packed = jnp.concatenate([state, decay_rows], axis=1).astype(jnp.bfloat16)
    gathered = lax.all_gather(packed, "sp")

    def one(step, running):
        piece = lax.dynamic_index_in_dim(gathered, step, 0, False).astype(jnp.float32)
        return piece[:, head_dim : head_dim + 1, :] * running + piece[:, :head_dim]

    return lax.fori_loop(0, place, one, jnp.zeros_like(state))


def from_earlier(packed, distance):
    count = lax.axis_size("sp")
    return lax.ppermute(packed, "sp", [(i, i + distance) for i in range(count - distance)])


def entering_by_hops(decay, state):
    count = lax.axis_size("sp")
    head_count, head_dim, _ = state.shape
    decay_rows = jnp.broadcast_to(decay[:, None, None], (head_count, 8, head_dim))
    packed = jnp.concatenate([state, decay_rows], axis=1)
    near = from_earlier(packed, 1)
    far = from_earlier(packed, 2)
    factor = near[:, head_dim:]
    pair = jnp.concatenate(
        [factor[:, :1] * far[:, :head_dim] + near[:, :head_dim], factor * far[:, head_dim:]],
        axis=1,
    )
    total, factor = pair[:, :head_dim], pair[:, head_dim : head_dim + 1]
    for piece in [from_earlier(pair, distance) for distance in range(2, count, 2)]:
        total = total + factor * piece[:, :head_dim]
        factor = factor * piece[:, head_dim : head_dim + 1]
    return total


def ring_order(count):
    return list(range(0, count, 2)) + list(range(1, count, 2))[::-1]


def ring_gather(block, forward_steps, backward_steps):
    count = lax.axis_size("sp")
    order = ring_order(count)
    ahead = [(order[i], order[(i + 1) % count]) for i in range(count)]
    behind = [(b, a) for a, b in ahead]
    arrived = [(0, block)]
    up, down = block, block
    for step in range(1, max(forward_steps, backward_steps) + 1):
        if step <= forward_steps:
            up = lax.ppermute(up, "sp", ahead)
            arrived.append((-step, up))
        if step <= backward_steps:
            down = lax.ppermute(down, "sp", behind)
            arrived.append((step, down))
    return arrived


def owner_of(offset):
    count = lax.axis_size("sp")
    me = lax.axis_index("sp")
    half = (count + 1) // 2
    position = jnp.where(me % 2 == 0, me // 2, count - 1 - me // 2)
    there = (position + offset + count) % count
    return jnp.where(there < half, 2 * there, 2 * (count - 1 - there) + 1)


def rms_norm(values_in, gain_vec):
    widened = values_in.astype(jnp.float32)
    return (
        widened
        * lax.rsqrt(jnp.mean(widened * widened, axis=-1, keepdims=True) + EPSILON)
        * gain_vec
    )


def block_step(carried, pieces):
    query_blk, key_blk, value_blk, decay_blk = pieces
    length = query_blk.shape[1]
    key_scale = query_blk.shape[2] ** (-0.5)
    cumulative = jnp.cumsum(decay_blk, axis=1)
    log_gap = cumulative[:, :, None] - cumulative[:, None, :]
    causal = lax.broadcasted_iota(jnp.int32, (length, length), 0) >= lax.broadcasted_iota(
        jnp.int32, (length, length), 1
    )
    weight = jnp.where(causal[None], jnp.exp(jnp.minimum(log_gap, 0.0)), 0.0)
    products = jnp.einsum("htd,hsd->hts", query_blk, key_blk, preferred_element_type=jnp.float32)
    scores = (products * key_scale * weight).astype(jnp.bfloat16)
    within = jnp.einsum("hts,hsd->htd", scores, value_blk, preferred_element_type=jnp.float32)
    carried_term = (
        jnp.einsum(
            "htd,hde->hte", query_blk.astype(jnp.float32), carried, precision=lax.Precision.HIGHEST
        )
        * jnp.exp(cumulative)[:, :, None]
    )
    to_end = jnp.exp(cumulative[:, -1:] - cumulative) * key_scale
    scaled_keys = (key_blk.astype(jnp.float32) * to_end[:, :, None]).astype(jnp.bfloat16)
    added = jnp.einsum("hsd,hse->hde", scaled_keys, value_blk, preferred_element_type=jnp.float32)
    carried = jnp.exp(cumulative[:, -1])[:, None, None] * carried + added
    return (carried, within + carried_term)


def to_blocks(matrix, block_len, head_count):
    row_count = matrix.shape[0]
    return matrix.reshape(row_count // block_len, block_len, head_count, -1).transpose(0, 2, 1, 3)


def finish_heads(retention, gates, norm_gain):
    centered = retention - jnp.mean(retention, axis=-1, keepdims=True)
    variance = jnp.mean(centered * centered, axis=-1, keepdims=True)
    normed = centered * lax.rsqrt(variance + EPSILON) * norm_gain[None]
    gate_vals = gates.astype(jnp.float32).reshape(normed.shape)
    return (jax.nn.silu(gate_vals) * normed).reshape(normed.shape[0], -1).astype(jnp.bfloat16)


def share_sum(part, row_count):
    count = lax.axis_size("tp")
    if count != 4:
        return lax.psum_scatter(part, "tp", scatter_dimension=0, tiled=True)
    me = lax.axis_index("tp")
    high, low = me // 2, me % 2
    shares = part.reshape(2, 2, row_count, -1)

    def swap(block, bit):
        return lax.ppermute(block, "tp", [(i, i ^ bit) for i in range(count)])

    def pick(block, index, dim):
        return lax.dynamic_index_in_dim(block, index, dim, False)

    nearer = swap(pick(shares, 1 - low, 1), 1).astype(jnp.float32)
    pair = pick(shares, low, 1).astype(jnp.float32) + nearer
    farther = swap(pick(pair, 1 - high, 0).astype(jnp.bfloat16), 2).astype(jnp.float32)
    return (pick(pair, high, 0) + farther).astype(jnp.bfloat16)


def ring_feed_forward(rows, gate_blocks, up_blocks, down_blocks, shape):
    depth = gate_blocks[0][1].shape[0]
    width = down_blocks[0][1].shape[1]
    half = (len(gate_blocks) + 1) // 2

    def project(blocks):
        total = None
        for some in (blocks[:half], blocks[half:]):
            if not some:
                continue
            columns = jnp.concatenate(
                [
                    lax.dynamic_slice_in_dim(rows, owner_of(offset) * depth, depth, 1)
                    for offset, _ in some
                ],
                axis=1,
            )
            weight = jnp.concatenate([block for _, block in some], axis=0)
            part = jnp.dot(columns, weight, preferred_element_type=jnp.float32)
            total = part if total is None else total + part
        return total

    gate_act = project(gate_blocks)
    up_act = project(up_blocks)
    hidden = (jax.nn.silu(gate_act) * up_act).astype(jnp.bfloat16)
    branch = jnp.zeros(shape, jnp.bfloat16)
    for some in (down_blocks[:half], down_blocks[half:]):
        if not some:
            continue
        wide = jnp.concatenate([block for _, block in some], axis=1)
        part = jnp.dot(hidden, wide, preferred_element_type=jnp.float32).astype(jnp.bfloat16)
        piece = share_sum(part, shape[0])
        for slot, (offset, _) in enumerate(some):
            branch = lax.dynamic_update_slice_in_dim(
                branch, piece[:, slot * width : (slot + 1) * width], owner_of(offset) * width, 1
            )
    return branch


def per_device(
    queries,
    keys,
    values,
    gates,
    log_decay,
    norm_gain,
    out_weight,
    resid,
    post_mix_gain,
    pre_ffn_gain,
    w_gate,
    w_up,
    w_down,
    post_ffn_gain,
):
    ring = lax.axis_size("sp")
    fewer = (ring - 1) // 2
    more = ring - 1 - fewer
    short = ring <= LONGEST_RING
    if short:
        gate_blocks = ring_gather(w_gate, more, fewer)
        up_blocks = ring_gather(w_up, fewer, more)
        down_blocks = ring_gather(w_down, more, fewer)
    row_count = queries.shape[0]
    head_count = log_decay.shape[1]
    head_dim = queries.shape[1] // head_count
    block_count = row_count // BLOCK
    query_blocks = to_blocks(queries, BLOCK, head_count)
    key_blocks = to_blocks(keys, BLOCK, head_count)
    value_blocks = to_blocks(values, BLOCK, head_count)
    decay_blocks = log_decay.reshape(block_count, BLOCK, head_count).transpose(0, 2, 1)
    start_state = jnp.zeros((head_count, head_dim, head_dim), jnp.float32)
    local_state, outputs = lax.scan(
        block_step, start_state, (query_blocks, key_blocks, value_blocks, decay_blocks)
    )
    retention = outputs.transpose(0, 2, 1, 3).reshape(row_count, head_count, head_dim)
    cumulative = jnp.cumsum(log_decay, axis=0)
    local_decay = jnp.exp(cumulative[-1])
    incoming = (entering_by_hops if short else entering)(local_decay, local_state)
    query_rows = queries.reshape(row_count, head_count, head_dim).astype(jnp.float32)
    retention = (
        retention
        + jnp.einsum("thd,hde->the", query_rows, incoming, precision=lax.Precision.HIGHEST)
        * jnp.exp(cumulative)[:, :, None]
    )
    retained = finish_heads(retention, gates, norm_gain)
    quarter = resid.shape[0]
    regrouped = lax.all_to_all(retained, "tp", split_axis=0, concat_axis=1, tiled=True)
    group_rows = out_weight.shape[0]
    empty_mix = jnp.zeros((quarter, out_weight.shape[1]), jnp.float32)
    running = empty_mix
    shard_piece = lax.all_gather(out_weight, "tp", axis=0, tiled=True)
    for offset in range(shard_piece.shape[0] // group_rows):
        columns = lax.dynamic_slice_in_dim(regrouped, offset * group_rows, group_rows, 1)
        part = jnp.dot(
            columns,
            shard_piece[offset * group_rows : (offset + 1) * group_rows],
            preferred_element_type=jnp.float32,
        )
        running = running + part.astype(jnp.bfloat16).astype(jnp.float32)
    mixed = running
    mixed = mixed.astype(jnp.bfloat16)
    middle = (resid.astype(jnp.float32) + rms_norm(mixed, post_mix_gain)).astype(jnp.bfloat16)
    ffn_input = rms_norm(middle, pre_ffn_gain).astype(jnp.bfloat16)
    gathered = lax.all_gather(ffn_input, "tp", axis=0, tiled=True)
    if not short:
        gate_act = jnp.dot(
            gathered,
            lax.all_gather(w_gate, "sp", axis=0, tiled=True),
            preferred_element_type=jnp.float32,
        )
        up_act = jnp.dot(
            gathered,
            lax.all_gather(w_up, "sp", axis=0, tiled=True),
            preferred_element_type=jnp.float32,
        )
        hidden = (jax.nn.silu(gate_act) * up_act).astype(jnp.bfloat16)
        down_full = lax.all_gather(w_down, "sp", axis=1, tiled=True)
        partial = jnp.dot(hidden, down_full, preferred_element_type=jnp.float32)
        branch = lax.psum_scatter(
            partial.astype(jnp.bfloat16), "tp", scatter_dimension=0, tiled=True
        )
    else:
        branch = ring_feed_forward(gathered, gate_blocks, up_blocks, down_blocks, resid.shape)
    return (middle.astype(jnp.float32) + rms_norm(branch, post_ffn_gain)).astype(jnp.bfloat16)


MESH = pl.DeviceIdType.MESH
HEADER_ROWS = 16
F32 = jnp.float32
BF16 = jnp.bfloat16


def silu_of(v):
    return v / (1.0 + jnp.exp(-v))


def layer_kernel(
    q_in,
    k_in,
    v_in,
    gates_in,
    decay_in,
    norm_gain,
    ow_in,
    resid_in,
    mix_gain,
    pre_gain,
    wg_in,
    wu_in,
    wd_in,
    post_gain,
    out,
    q_ref,
    k_ref,
    v_ref,
    gates_ref,
    resid_ref,
    wg,
    wu,
    wd,
    ow,
    cum_row,
    cum_col,
    local_state,
    start_state,
    state_out,
    state_pair,
    total_out,
    total_in,
    retention,
    retained_out,
    retained_in,
    mixed,
    middle,
    rows,
    gate_acts,
    hidden,
    part_out,
    part_in,
    sum_out,
    sum_in,
    branch,
    local_sem,
    own_sem,
    z_send,
    z_recv,
    y_send,
    y_recv,
    c_send,
    c_recv,
    ow_send,
    ow_recv,
    pair_send,
    pair_recv,
    total_send,
    total_recv,
    ret_send,
    ret_recv,
    rows_send,
    rows_recv,
    part_send,
    part_recv,
    sum_send,
    sum_recv,
):
    sp, tp = lax.axis_index("sp"), lax.axis_index("tp")
    planes = lax.axis_size("sp") // 2
    z, y = sp // 2, sp % 2
    x, core = tp // 2, tp % 2
    parity = z % 2
    pair = z + 1 - 2 * parity
    far = (z + 2) % planes
    far_pair = (pair + 2) % planes
    other_x, other_y, other_core = 1 - x, 1 - y, 1 - core
    is_main = core == parity
    is_helper = core != parity
    sp_y = z * 2 + other_y
    sp_pair = pair * 2 + y
    tp_x = other_x * 2 + core
    tp_core = x * 2 + other_core
    tp_both = other_x * 2 + other_core

    row_count, _ = q_ref.shape
    heads = norm_gain.shape[0]
    dim = norm_gain.shape[1]
    block_count = row_count // BLOCK
    quarter = resid_in.shape[0]
    model = resid_in.shape[1]
    units = wg_in.shape[1]
    tps = ow.shape[0]
    scale = dim ** (-0.5)

    inputs = [
        (k_in, k_ref),
        (v_in, v_ref),
        (q_in, q_ref),
        (gates_in, gates_ref),
        (resid_in, resid_ref),
        (ow_in, ow.at[tp]),
    ]

    def local_copy(i):
        return pltpu.make_async_copy(inputs[i][0], inputs[i][1], local_sem.at[i])

    weights_in = (wg_in, wu_in, wd_in)
    weights = (wg, wu, wd)

    def own_copy(m):
        return pltpu.make_async_copy(weights_in[m], weights[m].at[sp], own_sem.at[m])

    for i in range(len(inputs)):
        local_copy(i).start()

    @pl.when(is_main)
    def _():
        for m in range(3):
            own_copy(m).start()

    def remote(src, dst, send, recv, device):
        return pltpu.make_async_remote_copy(
            src_ref=src,
            dst_ref=dst,
            send_sem=send,
            recv_sem=recv,
            device_id=device,
            device_id_type=MESH,
        )

    barrier = pltpu.get_barrier_semaphore()
    peers = [(((z + i) % planes) * 2 + y, tp) for i in range(1, 4)]
    peers += [(sp_y, tp), (sp, tp_x), (sp, tp_core), (sp, tp_both), (sp_pair, tp_x)]
    for peer in peers:
        pl.semaphore_signal(barrier, inc=1, device_id=peer, device_id_type=MESH)
    pl.semaphore_wait(barrier, len(peers))

    far_target = lax.select(is_main, far, far_pair)
    in_middle = jnp.logical_and(z > 0, z < planes - 1)
    at_end = jnp.logical_or(z == 0, z == planes - 1)

    def cut(ref, half):
        size = ref.shape[0] // 2
        return ref.at[half * size : (half + 1) * size]

    def source(m, half):
        return cut(weights_in[m], half)

    def slot(m, half, place):
        size = weights[m].shape[1] // 2
        return weights[m].at[place, half * size : (half + 1) * size]

    def z_near(m, half):
        piece = 2 * m + half
        return remote(
            source(m, half),
            slot(m, half, sp),
            z_send.at[piece, 0],
            z_recv.at[piece, z],
            (pair * 2 + y, tp),
        )

    def z_far(m, half):
        piece = 2 * m + half
        return remote(
            source(m, half),
            slot(m, half, sp),
            z_send.at[piece, 1],
            z_recv.at[piece, z],
            (far_target * 2 + y, tp),
        )

    def to_y(m, half, plane, src):
        piece, place = 2 * m + half, plane * 2 + y
        return remote(
            src,
            slot(m, half, place),
            y_send.at[piece, plane],
            y_recv.at[piece, plane],
            (sp_y, tp),
        )

    def to_core(m, half, place, src):
        piece = 2 * m + half
        return remote(
            src,
            slot(m, half, place),
            c_send.at[piece, place],
            c_recv.at[piece, place],
            (sp, tp_core),
        )

    def z_arrival(m, half, plane):
        piece, here = 2 * m + half, slot(m, half, plane * 2 + y)
        return remote(here, here, z_send.at[piece, 1], z_recv.at[piece, plane], (sp_y, tp))

    def y_arrival(m, half, plane):
        piece, here = 2 * m + half, slot(m, half, plane * 2 + other_y)
        return remote(here, here, y_send.at[piece, plane], y_recv.at[piece, plane], (sp_y, tp))

    def start_own(m):
        @pl.when(is_main)
        def _():
            for half in range(2):
                to_y(m, half, z, source(m, half)).start()
                to_core(m, half, sp, source(m, half)).start()

    def pass_plane(m, half, plane):
        z_arrival(m, half, plane).wait_recv()
        here = slot(m, half, plane * 2 + y)
        to_y(m, half, plane, here).start()
        to_core(m, half, plane * 2 + y, here).start()

    def pass_z(m, half, planes_list):
        @pl.when(is_main)
        def _():
            for plane in planes_list:
                pass_plane(m, half, plane)

    def pass_if(condition, m, half, plane):
        @pl.when(jnp.logical_and(condition, is_main))
        def _():
            pass_plane(m, half, plane)

    def pass_y(m, half, planes_list, condition=True):
        @pl.when(jnp.logical_and(condition, is_main))
        def _():
            for plane in planes_list:
                y_arrival(m, half, plane).wait_recv()
                place = plane * 2 + other_y
                to_core(m, half, place, slot(m, half, place)).start()

    def core_wait(m, planes_list):
        @pl.when(is_helper)
        def _():
            for plane in planes_list:
                for half in range(2):
                    for place in (plane * 2 + y, plane * 2 + other_y):
                        here = slot(m, half, place)
                        to_core(m, half, place, here).wait_recv()

    def own_wait(m):
        @pl.when(is_main)
        def _():
            own_copy(m).wait()

    near_up = parity == 0
    far_up = z < planes // 2
    near_down, far_down = parity == 1, z >= planes // 2
    one_hop = jnp.logical_and(in_middle, is_helper)
    more_hops = jnp.logical_or(at_end, is_main)
    both = jnp.logical_and

    def when_do(condition, do):
        @pl.when(condition)
        def _():
            do()

    def start_far(m, half, condition):
        when_do(condition, lambda: z_far(m, half).start())

    def start_near(m, half, condition):
        when_do(both(is_helper, condition), lambda: z_near(m, half).start())

    when_do(is_helper, lambda: z_near(0, 0).start())
    start_far(0, 0, jnp.logical_or(far_down, one_hop))
    when_do(is_helper, lambda: z_near(0, 1).start())
    start_far(0, 1, far_down)
    near_planes = [pair, far, far_pair]
    all_planes = [z] + near_planes

    ow_copies = [
        remote(ow_in, ow.at[tp], ow_send.at[0], ow_recv.at[tp], (sp, tp_x)),
        remote(ow_in, ow.at[tp], ow_send.at[1], ow_recv.at[tp], (sp, tp_core)),
        remote(ow.at[tp_x], ow.at[tp_x], ow_send.at[2], ow_recv.at[tp_x], (sp, tp_core)),
    ]
    ow_copies[0].start()
    ow_copies[1].start()

    for i in range(3):
        local_copy(i).wait()

    row_index = lax.broadcasted_iota(jnp.int32, (BLOCK, BLOCK), 0)
    col_index = lax.broadcasted_iota(jnp.int32, (BLOCK, BLOCK), 1)
    before = jnp.where(row_index <= col_index, 1.0, 0.0).astype(BF16)
    until = jnp.where(row_index >= col_index, 1.0, 0.0).astype(BF16)
    for b in range(block_count):
        decay = decay_in[:, b * BLOCK : (b + 1) * BLOCK]
        high = decay.astype(BF16)
        rest = decay - high.astype(F32)
        middle_term = rest.astype(BF16)
        low = (rest - middle_term.astype(F32)).astype(BF16)
        by_row, by_col = 0.0, 0.0
        for term in (low, middle_term, high):
            by_row = by_row + jnp.dot(term, before, preferred_element_type=F32)
            by_col = by_col + lax.dot_general(
                until, term, (((1,), (1,)), ((), ())), preferred_element_type=F32
            )
        cum_row[b] = by_row
        cum_col[b] = by_col

    def block_decay(b, h):
        return jnp.exp(cum_row[b, h : h + 1, BLOCK - 1 : BLOCK])

    for h in range(heads):
        lanes = slice(h * dim, (h + 1) * dim)
        for b in range(block_count):
            span = slice(b * BLOCK, (b + 1) * BLOCK)
            last = cum_row[b, h : h + 1, BLOCK - 1 : BLOCK]
            to_end = jnp.exp(last - cum_col[b, :, h : h + 1]) * scale
            scaled = (k_ref[span, lanes].astype(F32) * to_end).astype(BF16)
            local_state[b, h] = lax.dot_general(
                scaled, v_ref[span, lanes], (((0,), (0,)), ((), ())), preferred_element_type=F32
            )

    def local_total(h):
        total, decay = local_state[0, h], block_decay(0, h)
        for b in range(1, block_count):
            total = block_decay(b, h) * total + local_state[b, h]
            decay = decay * block_decay(b, h)
        return total, decay

    header_row = lax.broadcasted_iota(jnp.int32, (HEADER_ROWS, dim), 0)

    def pack(ref, h, total, decay):
        ref[h, :dim] = total.astype(BF16)
        wide = jnp.broadcast_to(decay, (HEADER_ROWS, dim))
        high = wide.astype(BF16).astype(F32)
        ref[h, dim:] = jnp.where(header_row < 8, high, wide - high).astype(BF16)

    def unpack(packed, h):
        block = packed[h].astype(F32)
        return block[:dim], block[dim : dim + 1] + block[dim + 8 : dim + 9]

    for h in range(heads):
        total, decay = local_total(h)
        pack(state_out, h, total, decay)
    pair_copy = remote(state_out, state_pair, pair_send.at[0], pair_recv.at[0], (sp_y, tp))
    pair_copy.start()
    start_own(0)

    def scores_of(b):
        for h in range(heads):
            lanes = slice(h * dim, (h + 1) * dim)
            span = slice(b * BLOCK, (b + 1) * BLOCK)
            tile = 128
            keys, vals = k_ref[span, lanes], v_ref[span, lanes]
            row_sums = cum_row[b, h : h + 1, :]

            def one(i, _):
                at = pl.multiple_of(i * tile, tile)
                here = pl.ds(b * BLOCK + at, tile)
                products = lax.dot_general(
                    q_ref[here, lanes], keys, (((1,), (1,)), ((), ())), preferred_element_type=F32
                )
                gap = cum_col[b, pl.ds(at, tile), h : h + 1] - row_sums
                t_index = at + lax.broadcasted_iota(jnp.int32, (tile, BLOCK), 0)
                s_index = lax.broadcasted_iota(jnp.int32, (tile, BLOCK), 1)
                weight = jnp.where(s_index <= t_index, jnp.exp(jnp.minimum(gap, 0.0)), 0.0)
                scores = (products * scale * weight).astype(BF16)
                retention[here, lanes] = jnp.dot(scores, vals, preferred_element_type=F32)
                return 0

            lax.fori_loop(0, BLOCK // tile, one, 0)

    scores_of(0)

    pair_copy.wait_recv()
    for h in range(heads):
        total, decay = local_total(h)
        their_total, their_decay = unpack(state_pair, h)
        last_factor = jnp.where(y == 1, decay, their_decay)
        first = jnp.where(y == 1, their_total, total)
        second = jnp.where(y == 1, total, their_total)
        pack(total_out, h, last_factor * first + second, decay * their_decay)

    def total_copy(plane):
        return remote(
            total_out,
            total_in.at[z],
            total_send.at[plane],
            total_recv.at[z],
            (plane * 2 + y, tp),
        )

    for plane in range(1, 4):

        @pl.when(z < plane)
        def _():
            total_copy(plane).start()


    for half in range(2):
        start_far(1, half, both(far_down, in_middle))
        start_near(1, half, near_down)
    for b in range(1, block_count):
        scores_of(b)

    ow_arrival = [
        remote(ow.at[t], ow.at[t], ow_send.at[0], ow_recv.at[t], (sp, tp_x))
        for t in (tp_x, tp_core, tp_both)
    ]

    for h in range(heads):
        start_state[0, h] = jnp.zeros((dim, dim), F32)
    for plane in range(3):

        @pl.when(plane < z)
        def _():
            remote(
                total_out,
                total_in.at[plane],
                total_send.at[plane],
                total_recv.at[plane],
                (sp_y, tp),
            ).wait_recv()
            for h in range(heads):
                total, decay = unpack(total_in.at[plane], h)
                start_state[0, h] = decay * start_state[0, h] + total

    for h in range(heads):
        their_total, their_decay = unpack(state_pair, h)
        state = start_state[0, h]
        state = jnp.where(y == 1, their_decay * state + their_total, state)
        start_state[0, h] = state
        for b in range(1, block_count):
            state = block_decay(b - 1, h) * state + local_state[b - 1, h]
            start_state[b, h] = state

    local_copy(3).wait()

    def retained_copy(j):
        return remote(
            retained_out.at[j],
            retained_in.at[tp],
            ret_send.at[j],
            ret_recv.at[tp],
            (sp, j),
        )

    per_block = BLOCK // quarter

    def finish(j, target):
        b = j // per_block
        at = pl.multiple_of((j % per_block) * quarter, quarter)
        here = pl.ds(pl.multiple_of(j * quarter, quarter), quarter)
        for h in range(heads):
            lanes = slice(h * dim, (h + 1) * dim)
            state = start_state[b, h]
            high = state.astype(BF16)
            low = (state - high.astype(F32)).astype(BF16)
            query = q_ref[here, lanes]
            carried = jnp.dot(query, high, preferred_element_type=F32) + jnp.dot(
                query, low, preferred_element_type=F32
            )
            kept = retention[here, lanes] + carried * jnp.exp(
                cum_col[b, pl.ds(at, quarter), h : h + 1]
            )
            centered = kept - jnp.mean(kept, axis=-1, keepdims=True)
            variance = jnp.mean(centered * centered, axis=-1, keepdims=True)
            normed = centered * lax.rsqrt(variance + EPSILON) * norm_gain[h : h + 1, :]
            target[:, lanes] = (silu_of(gates_ref[here, lanes].astype(F32)) * normed).astype(BF16)

    others = [(tp + i) % tps for i in range(1, tps)]
    start_far(0, 0, both(far_up, more_hops))
    start_far(0, 1, far_up)
    for half in range(2):
        start_far(1, half, both(far_up, in_middle))
        start_near(1, half, near_up)

    for j in others:
        finish(j, retained_out.at[j])
        retained_copy(j).start()
    finish(tp, retained_in.at[tp])

    pass_z(0, 0, near_planes[:1])
    start_own(1)
    ow_arrival[0].wait_recv()
    ow_copies[2].start()
    for arrival in ow_arrival[1:]:
        arrival.wait_recv()
    local_copy(5).wait()
    local_copy(4).wait()
    for j in others:
        remote(
            retained_out.at[j],
            retained_in.at[j],
            ret_send.at[j],
            ret_recv.at[j],
            (sp, j),
        ).wait_recv()

    mix_tile = 512

    def mix(i, _):
        here = pl.ds(pl.multiple_of(i * mix_tile, mix_tile), mix_tile)
        total = jnp.zeros((quarter, mix_tile), F32)
        for g in range(tps):
            part = jnp.dot(retained_in[g], ow[g, :, here], preferred_element_type=F32)
            total = total + part.astype(BF16).astype(F32)
        mixed[:, here] = total.astype(BF16)
        return 0

    lax.fori_loop(0, model // mix_tile, mix, 0)

    def rms_of(v):
        return v * lax.rsqrt(jnp.mean(v * v, axis=-1, keepdims=True) + EPSILON)

    mine = x * 2 + parity
    norm_tile = 32

    def into_rows(i, _):
        here = pl.ds(pl.multiple_of(i * norm_tile, norm_tile), norm_tile)
        value = rms_of(mixed[here, :].astype(F32)) * mix_gain[...]
        value = (resid_ref[here, :].astype(F32) + value).astype(BF16)
        middle[here, :] = value
        rows[mine, here, :] = (rms_of(value.astype(F32)) * pre_gain[...]).astype(BF16)
        return 0

    from_pair = x * 2 + 1 - parity
    from_x = other_x * 2 + parity
    from_both = other_x * 2 + 1 - parity
    row_parts = 4
    part_rows = quarter // row_parts

    def rows_copy(i, half, place, device):
        here = rows.at[place, half * part_rows : (half + 1) * part_rows]
        return remote(here, here, rows_send.at[i, half], rows_recv.at[place, half], device)

    for half in range(row_parts):
        steps = part_rows // norm_tile
        lax.fori_loop(half * steps, (half + 1) * steps, into_rows, 0)
        rows_copy(0, half, mine, (sp_pair, tp)).start()
        rows_copy(1, half, mine, (sp, tp_x)).start()

    pass_z(0, 1, near_planes[:1])
    pass_z(0, 0, near_planes[1:])
    pass_z(0, 1, near_planes[1:])
    for half in range(2):
        pass_z(1, half, near_planes[:1])
    for half in range(row_parts // 2):
        rows_copy(0, half, from_pair, (sp_pair, tp)).wait_recv()
        rows_copy(2, half, from_pair, (sp, tp_x)).start()
    for half in range(2):
        start_far(1, half, at_end)
    start_own(2)
    for half in range(2):
        pass_if(at_end, 1, half, far)
        pass_if(in_middle, 1, half, far_pair)
    for half in range(row_parts // 2, row_parts):
        rows_copy(0, half, from_pair, (sp_pair, tp)).wait_recv()
        rows_copy(2, half, from_pair, (sp, tp_x)).start()
    for half in range(2):
        when_do(is_helper, lambda: z_near(2, half).start())
        start_far(2, half, in_middle)
    for half in range(2):
        pass_y(0, half, all_planes)
    own_wait(0)
    core_wait(0, all_planes)

    unit_tile = 256
    unit_steps = units // unit_tile

    def acts_of(weight, first, at, size):
        here = pl.ds(at, size)
        return jnp.dot(
            rows[pl.ds(first, 2)].reshape(2 * quarter, model),
            weight[:, :, here].reshape(model, size),
            preferred_element_type=F32,
        ).reshape(2, quarter, size)

    def over_units(one, begin=0, end=unit_steps + 1):
        def step(i, _):
            one(pl.multiple_of(i * unit_tile, unit_tile), unit_tile)
            return 0

        lax.fori_loop(begin, min(end, unit_steps), step, 0)
        if end > unit_steps and units % unit_tile:
            one(unit_steps * unit_tile, units % unit_tile)

    def gate_of(first):
        def one(at, size):
            gate_acts[pl.ds(first, 2), :, pl.ds(at, size)] = acts_of(wg, first, at, size)

        over_units(one)

    def up_of(first, begin=0, end=unit_steps + 1):
        def one(at, size):
            here = pl.ds(at, size)
            gate = gate_acts[pl.ds(first, 2), :, here]
            value = silu_of(gate) * acts_of(wu, first, at, size)
            hidden[pl.ds(first, 2), :, here] = value.astype(BF16)

        over_units(one, begin, end)

    gate_of(x * 2)
    for half in range(2):
        start_far(2, half, at_end)
    pass_if(at_end, 1, 0, far_pair)
    pass_if(in_middle, 1, 0, far)
    pass_if(at_end, 1, 1, far_pair)
    pass_if(in_middle, 1, 1, far)
    for half in range(2):
        pass_y(1, half, [z, pair])
        pass_y(1, half, [far], at_end)
        pass_y(1, half, [far_pair], in_middle)
    pass_z(2, 0, near_planes[:1])
    for half in range(row_parts):
        rows_copy(1, half, from_x, (sp, tp_x)).wait_recv()
        rows_copy(2, half, from_both, (sp, tp_x)).wait_recv()
    gate_of(other_x * 2)
    for half in range(2):
        pass_y(1, half, [far_pair], at_end)
        pass_y(1, half, [far], in_middle)
    for half in range(2):
        pass_y(2, half, [z])
    pass_z(2, 1, near_planes[:1])
    own_wait(1)
    core_wait(1, all_planes)

    columns = wd_in.shape[1]

    def down(place, first, second):
        left = jnp.concatenate([hidden[first], hidden[second]], axis=0)
        product = jnp.dot(left, wd[place], preferred_element_type=F32)
        return product.astype(BF16).reshape(2, quarter, columns)

    def part_copy(place, over_x):
        device = (sp, tp_x) if over_x else (sp_pair, tp)
        return remote(
            part_out.at[place], part_in.at[place], part_send.at[place], part_recv.at[place], device
        )

    def sum_copy(place, over_x):
        device = (sp_pair, tp) if over_x else (sp, tp_x)
        return remote(
            sum_out.at[place], sum_in.at[place], sum_send.at[place], sum_recv.at[place], device
        )

    def place_wait(place):
        @pl.when(is_helper)
        def _():
            for half in range(2):
                to_core(2, half, place, slot(2, half, place)).wait_recv()

    def send_part(plane, over_x):
        place = plane * 2 + (y if over_x else other_y)
        if not over_x and plane is not z:
            for half in range(2):
                pass_y(2, half, [plane])
        place_wait(place)
        if over_x:
            part_out[place] = down(place, other_x * 2, other_x * 2 + 1)
        else:
            part_out[place] = down(place, 1 - parity, 3 - parity)
        part_copy(place, over_x).start()

    def own_product(plane):
        for over_x in (True, False):
            place = plane * 2 + (y if over_x else other_y)
            product = down(place, mine, from_pair if over_x else from_x)
            branch[place] = product[0].astype(F32)
            sum_out[place] = product[1]

    def own_part(plane, over_x):
        place = plane * 2 + (y if over_x else other_y)
        mine_at, other_at = (parity, 1 - parity) if over_x else (x, other_x)
        part_copy(place, over_x).wait_recv()
        sum_out[place] = (
            sum_out[place].astype(F32) + part_in[place, other_at].astype(F32)
        ).astype(BF16)
        sum_copy(place, over_x).start()
        branch[place] = branch[place] + part_in[place, mine_at].astype(F32)

    def pass_late(half):
        pass_if(at_end, 2, half, far)
        pass_if(at_end, 2, half, far_pair)
        pass_if(in_middle, 2, half, far_pair)
        pass_if(in_middle, 2, half, far)

    up_of(other_x * 2)
    own_wait(2)
    send_part(z, True)
    up_of(x * 2, 0, unit_steps // 2)
    pass_late(0)
    up_of(x * 2, unit_steps // 2)
    send_part(z, False)
    pass_late(1)
    send_part(pair, True)
    own_product(z)
    own_part(z, True)
    send_part(pair, False)
    send_part(far, True)
    own_product(pair)
    own_part(pair, False)
    send_part(far, False)
    send_part(far_pair, True)
    own_part(pair, True)
    send_part(far_pair, False)
    own_product(far)
    own_product(far_pair)
    own_part(z, False)
    own_part(far, True)
    own_part(far_pair, False)
    own_part(far_pair, True)
    own_part(far, False)

    for plane in all_planes:
        sum_copy(plane * 2 + y, True).wait_recv()
        sum_copy(plane * 2 + other_y, False).wait_recv()

    def final(i, _):
        here = pl.ds(pl.multiple_of(i * norm_tile, norm_tile), norm_tile)
        value = jnp.concatenate(
            [branch[n, here, :] + sum_in[n, here, :].astype(F32) for n in range(2 * planes)],
            axis=1,
        )
        value = rms_of(value.astype(BF16).astype(F32)) * post_gain[...]
        out[here, :] = (middle[here, :].astype(F32) + value).astype(BF16)
        return 0

    lax.fori_loop(0, quarter // norm_tile, final, 0)

    for m in range(3):
        for half in range(2):
            z_far(m, half).wait_send()
            when_do(is_helper, lambda: z_near(m, half).wait_send())

            @pl.when(is_main)
            def _():
                for plane in all_planes:
                    place = plane * 2 + y
                    src = source(m, half) if plane is z else slot(m, half, place)
                    to_y(m, half, plane, src).wait_send()
                    to_core(m, half, place, src).wait_send()
                    place = plane * 2 + other_y
                    to_core(m, half, place, slot(m, half, place)).wait_send()

    for copy in ow_copies:
        copy.wait_send()
    pair_copy.wait_send()
    for plane in range(1, 4):

        @pl.when(z < plane)
        def _():
            total_copy(plane).wait_send()

    for j in others:
        retained_copy(j).wait_send()
    for half in range(row_parts):
        rows_copy(0, half, mine, (sp_pair, tp)).wait_send()
        rows_copy(1, half, mine, (sp, tp_x)).wait_send()
        rows_copy(2, half, from_pair, (sp, tp_x)).wait_send()
    for plane in range(planes):
        for over_x in (True, False):
            place = plane * 2 + (y if over_x else other_y)
            part_copy(place, over_x).wait_send()
            sum_copy(place, over_x).wait_send()


def whole_layer(
    queries,
    keys,
    values,
    gates,
    log_decay,
    norm_gain,
    out_weight,
    resid,
    post_mix_gain,
    pre_ffn_gain,
    w_gate,
    w_up,
    w_down,
    post_ffn_gain,
):
    places, tps = lax.axis_size("sp"), lax.axis_size("tp")
    planes = places // 2
    row_count, width = queries.shape
    heads, dim = norm_gain.shape
    block_count = row_count // BLOCK
    quarter, model = resid.shape
    depth, units = w_gate.shape
    columns = w_down.shape[1]
    decay_rows = log_decay.T
    anywhere = pl.BlockSpec(memory_space=pl.ANY)
    onchip = pl.BlockSpec(memory_space=pltpu.VMEM)
    dma = pltpu.SemaphoreType.DMA
    packed = (heads, dim + HEADER_ROWS, dim)
    scratch = [
        pltpu.VMEM((row_count, width), BF16),
        pltpu.VMEM((row_count, width), BF16),
        pltpu.VMEM((row_count, width), BF16),
        pltpu.VMEM((row_count, width), BF16),
        pltpu.VMEM((quarter, model), BF16),
        pltpu.VMEM((places, depth, units), BF16),
        pltpu.VMEM((places, depth, units), BF16),
        pltpu.VMEM((places, units, columns), BF16),
        pltpu.VMEM((tps, width, model), BF16),
        pltpu.VMEM((block_count, heads, BLOCK), F32),
        pltpu.VMEM((block_count, BLOCK, heads), F32),
        pltpu.VMEM((block_count, heads, dim, dim), F32),
        pltpu.VMEM((block_count, heads, dim, dim), F32),
        pltpu.VMEM(packed, BF16),
        pltpu.VMEM(packed, BF16),
        pltpu.VMEM(packed, BF16),
        pltpu.VMEM((planes,) + packed, BF16),
        pltpu.VMEM((row_count, width), F32),
        pltpu.VMEM((tps, quarter, width), BF16),
        pltpu.VMEM((tps, quarter, width), BF16),
        pltpu.VMEM((quarter, model), BF16),
        pltpu.VMEM((quarter, model), BF16),
        pltpu.VMEM((4, quarter, model), BF16),
        pltpu.VMEM((4, quarter, units), F32),
        pltpu.VMEM((4, quarter, units), BF16),
        pltpu.VMEM((places, 2, quarter, columns), BF16),
        pltpu.VMEM((places, 2, quarter, columns), BF16),
        pltpu.VMEM((places, quarter, columns), BF16),
        pltpu.VMEM((places, quarter, columns), BF16),
        pltpu.VMEM((places, quarter, columns), F32),
        dma((6,)),
        dma((3,)),
        dma((6, 2)),
        dma((6, planes)),
        dma((6, planes)),
        dma((6, planes)),
        dma((6, places)),
        dma((6, places)),
        dma((3,)),
        dma((tps,)),
        dma((1,)),
        dma((1,)),
        dma((planes,)),
        dma((planes,)),
        dma((tps,)),
        dma((tps,)),
        dma((3, 4)),
        dma((4, 4)),
        dma((places,)),
        dma((places,)),
        dma((places,)),
        dma((places,)),
    ]
    return pl.pallas_call(
        layer_kernel,
        out_shape=jax.ShapeDtypeStruct((quarter, model), BF16),
        in_specs=[anywhere] * 4
        + [onchip, onchip, anywhere, anywhere, onchip, onchip]
        + [anywhere] * 3
        + [onchip],
        out_specs=onchip,
        scratch_shapes=scratch,
        compiler_params=pltpu.CompilerParams(
            collective_id=0, has_side_effects=True, vmem_limit_bytes=62 * 1024 * 1024
        ),
    )(
        queries,
        keys,
        values,
        gates,
        decay_rows,
        norm_gain,
        out_weight,
        resid,
        post_mix_gain[None],
        pre_ffn_gain[None],
        w_gate,
        w_up,
        w_down,
        post_ffn_gain[None],
    )


def solution(mesh):
    in_specs = (
        P("sp", "tp"),
        P("sp", "tp"),
        P("sp", "tp"),
        P("sp", "tp"),
        P("sp", "tp"),
        P("tp", None),
        P("tp", None),
        P(("sp", "tp"), None),
        P(),
        P(),
        P("sp", "tp"),
        P("sp", "tp"),
        P("tp", "sp"),
        P(),
    )
    out_specs = P(("sp", "tp"), None)
    if mesh.shape["sp"] == LONGEST_RING and mesh.shape["tp"] == 4:
        return jax.shard_map(
            whole_layer, mesh=mesh, in_specs=in_specs, out_specs=out_specs, check_vma=False
        )

    return jax.shard_map(
        per_device, mesh=mesh, in_specs=in_specs, out_specs=out_specs, check_vma=False
    )
```

```python
import jax
import jax.numpy as jnp
from jax import lax
from jax.experimental import pallas as pl
from jax.experimental.pallas import tpu as pltpu
from jax.sharding import PartitionSpec as P


BLOCK = 512


EPSILON = 1e-06
LONGEST_RING = 8


def entering(decay, state):
    place = lax.axis_index("sp")
    head_count, head_dim, _ = state.shape
    decay_rows = jnp.broadcast_to(decay[:, None, None], (head_count, 16, head_dim))
    packed = jnp.concatenate([state, decay_rows], axis=1).astype(jnp.bfloat16)
    gathered = lax.all_gather(packed, "sp")

    def one(step, running):
        piece = lax.dynamic_index_in_dim(gathered, step, 0, False).astype(jnp.float32)
        return piece[:, head_dim : head_dim + 1, :] * running + piece[:, :head_dim]

    return lax.fori_loop(0, place, one, jnp.zeros_like(state))


def from_earlier(packed, distance):
    count = lax.axis_size("sp")
    return lax.ppermute(packed, "sp", [(i, i + distance) for i in range(count - distance)])


def entering_by_hops(decay, state):
    count = lax.axis_size("sp")
    head_count, head_dim, _ = state.shape
    decay_rows = jnp.broadcast_to(decay[:, None, None], (head_count, 8, head_dim))
    packed = jnp.concatenate([state, decay_rows], axis=1)
    near = from_earlier(packed, 1)
    far = from_earlier(packed, 2)
    factor = near[:, head_dim:]
    pair = jnp.concatenate(
        [factor[:, :1] * far[:, :head_dim] + near[:, :head_dim], factor * far[:, head_dim:]],
        axis=1,
    )
    total, factor = pair[:, :head_dim], pair[:, head_dim : head_dim + 1]
    for piece in [from_earlier(pair, distance) for distance in range(2, count, 2)]:
        total = total + factor * piece[:, :head_dim]
        factor = factor * piece[:, head_dim : head_dim + 1]
    return total


def ring_order(count):
    return list(range(0, count, 2)) + list(range(1, count, 2))[::-1]


def ring_gather(block, forward_steps, backward_steps):
    count = lax.axis_size("sp")
    order = ring_order(count)
    ahead = [(order[i], order[(i + 1) % count]) for i in range(count)]
    behind = [(b, a) for a, b in ahead]
    arrived = [(0, block)]
    up, down = block, block
    for step in range(1, max(forward_steps, backward_steps) + 1):
        if step <= forward_steps:
            up = lax.ppermute(up, "sp", ahead)
            arrived.append((-step, up))
        if step <= backward_steps:
            down = lax.ppermute(down, "sp", behind)
            arrived.append((step, down))
    return arrived


def owner_of(offset):
    count = lax.axis_size("sp")
    me = lax.axis_index("sp")
    half = (count + 1) // 2
    position = jnp.where(me % 2 == 0, me // 2, count - 1 - me // 2)
    there = (position + offset + count) % count
    return jnp.where(there < half, 2 * there, 2 * (count - 1 - there) + 1)


def rms_norm(values_in, gain_vec):
    widened = values_in.astype(jnp.float32)
    return (
        widened
        * lax.rsqrt(jnp.mean(widened * widened, axis=-1, keepdims=True) + EPSILON)
        * gain_vec
    )


def block_step(carried, pieces):
    query_blk, key_blk, value_blk, decay_blk = pieces
    length = query_blk.shape[1]
    key_scale = query_blk.shape[2] ** (-0.5)
    cumulative = jnp.cumsum(decay_blk, axis=1)
    log_gap = cumulative[:, :, None] - cumulative[:, None, :]
    causal = lax.broadcasted_iota(jnp.int32, (length, length), 0) >= lax.broadcasted_iota(
        jnp.int32, (length, length), 1
    )
    weight = jnp.where(causal[None], jnp.exp(jnp.minimum(log_gap, 0.0)), 0.0)
    products = jnp.einsum("htd,hsd->hts", query_blk, key_blk, preferred_element_type=jnp.float32)
    scores = (products * key_scale * weight).astype(jnp.bfloat16)
    within = jnp.einsum("hts,hsd->htd", scores, value_blk, preferred_element_type=jnp.float32)
    carried_term = (
        jnp.einsum(
            "htd,hde->hte", query_blk.astype(jnp.float32), carried, precision=lax.Precision.HIGHEST
        )
        * jnp.exp(cumulative)[:, :, None]
    )
    to_end = jnp.exp(cumulative[:, -1:] - cumulative) * key_scale
    scaled_keys = (key_blk.astype(jnp.float32) * to_end[:, :, None]).astype(jnp.bfloat16)
    added = jnp.einsum("hsd,hse->hde", scaled_keys, value_blk, preferred_element_type=jnp.float32)
    carried = jnp.exp(cumulative[:, -1])[:, None, None] * carried + added
    return (carried, within + carried_term)


def to_blocks(matrix, block_len, head_count):
    row_count = matrix.shape[0]
    return matrix.reshape(row_count // block_len, block_len, head_count, -1).transpose(0, 2, 1, 3)


def finish_heads(retention, gates, norm_gain):
    centered = retention - jnp.mean(retention, axis=-1, keepdims=True)
    variance = jnp.mean(centered * centered, axis=-1, keepdims=True)
    normed = centered * lax.rsqrt(variance + EPSILON) * norm_gain[None]
    gate_vals = gates.astype(jnp.float32).reshape(normed.shape)
    return (jax.nn.silu(gate_vals) * normed).reshape(normed.shape[0], -1).astype(jnp.bfloat16)


def share_sum(part, row_count):
    count = lax.axis_size("tp")
    if count != 4:
        return lax.psum_scatter(part, "tp", scatter_dimension=0, tiled=True)
    me = lax.axis_index("tp")
    high, low = me // 2, me % 2
    shares = part.reshape(2, 2, row_count, -1)

    def swap(block, bit):
        return lax.ppermute(block, "tp", [(i, i ^ bit) for i in range(count)])

    def pick(block, index, dim):
        return lax.dynamic_index_in_dim(block, index, dim, False)

    nearer = swap(pick(shares, 1 - low, 1), 1).astype(jnp.float32)
    pair = pick(shares, low, 1).astype(jnp.float32) + nearer
    farther = swap(pick(pair, 1 - high, 0).astype(jnp.bfloat16), 2).astype(jnp.float32)
    return (pick(pair, high, 0) + farther).astype(jnp.bfloat16)


def ring_feed_forward(rows, gate_blocks, up_blocks, down_blocks, shape):
    depth = gate_blocks[0][1].shape[0]
    width = down_blocks[0][1].shape[1]
    half = (len(gate_blocks) + 1) // 2

    def project(blocks):
        total = None
        for some in (blocks[:half], blocks[half:]):
            if not some:
                continue
            columns = jnp.concatenate(
                [
                    lax.dynamic_slice_in_dim(rows, owner_of(offset) * depth, depth, 1)
                    for offset, _ in some
                ],
                axis=1,
            )
            weight = jnp.concatenate([block for _, block in some], axis=0)
            part = jnp.dot(columns, weight, preferred_element_type=jnp.float32)
            total = part if total is None else total + part
        return total

    gate_act = project(gate_blocks)
    up_act = project(up_blocks)
    hidden = (jax.nn.silu(gate_act) * up_act).astype(jnp.bfloat16)
    branch = jnp.zeros(shape, jnp.bfloat16)
    for some in (down_blocks[:half], down_blocks[half:]):
        if not some:
            continue
        wide = jnp.concatenate([block for _, block in some], axis=1)
        part = jnp.dot(hidden, wide, preferred_element_type=jnp.float32).astype(jnp.bfloat16)
        piece = share_sum(part, shape[0])
        for slot, (offset, _) in enumerate(some):
            branch = lax.dynamic_update_slice_in_dim(
                branch, piece[:, slot * width : (slot + 1) * width], owner_of(offset) * width, 1
            )
    return branch


def per_device(
    queries,
    keys,
    values,
    gates,
    log_decay,
    norm_gain,
    out_weight,
    resid,
    post_mix_gain,
    pre_ffn_gain,
    w_gate,
    w_up,
    w_down,
    post_ffn_gain,
):
    ring = lax.axis_size("sp")
    fewer = (ring - 1) // 2
    more = ring - 1 - fewer
    short = ring <= LONGEST_RING
    if short:
        gate_blocks = ring_gather(w_gate, more, fewer)
        up_blocks = ring_gather(w_up, fewer, more)
        down_blocks = ring_gather(w_down, more, fewer)
    row_count = queries.shape[0]
    head_count = log_decay.shape[1]
    head_dim = queries.shape[1] // head_count
    block_count = row_count // BLOCK
    query_blocks = to_blocks(queries, BLOCK, head_count)
    key_blocks = to_blocks(keys, BLOCK, head_count)
    value_blocks = to_blocks(values, BLOCK, head_count)
    decay_blocks = log_decay.reshape(block_count, BLOCK, head_count).transpose(0, 2, 1)
    start_state = jnp.zeros((head_count, head_dim, head_dim), jnp.float32)
    local_state, outputs = lax.scan(
        block_step, start_state, (query_blocks, key_blocks, value_blocks, decay_blocks)
    )
    retention = outputs.transpose(0, 2, 1, 3).reshape(row_count, head_count, head_dim)
    cumulative = jnp.cumsum(log_decay, axis=0)
    local_decay = jnp.exp(cumulative[-1])
    incoming = (entering_by_hops if short else entering)(local_decay, local_state)
    query_rows = queries.reshape(row_count, head_count, head_dim).astype(jnp.float32)
    retention = (
        retention
        + jnp.einsum("thd,hde->the", query_rows, incoming, precision=lax.Precision.HIGHEST)
        * jnp.exp(cumulative)[:, :, None]
    )
    retained = finish_heads(retention, gates, norm_gain)
    quarter = resid.shape[0]
    regrouped = lax.all_to_all(retained, "tp", split_axis=0, concat_axis=1, tiled=True)
    group_rows = out_weight.shape[0]
    empty_mix = jnp.zeros((quarter, out_weight.shape[1]), jnp.float32)
    running = empty_mix
    shard_piece = lax.all_gather(out_weight, "tp", axis=0, tiled=True)
    for offset in range(shard_piece.shape[0] // group_rows):
        columns = lax.dynamic_slice_in_dim(regrouped, offset * group_rows, group_rows, 1)
        part = jnp.dot(
            columns,
            shard_piece[offset * group_rows : (offset + 1) * group_rows],
            preferred_element_type=jnp.float32,
        )
        running = running + part.astype(jnp.bfloat16).astype(jnp.float32)
    mixed = running
    mixed = mixed.astype(jnp.bfloat16)
    middle = (resid.astype(jnp.float32) + rms_norm(mixed, post_mix_gain)).astype(jnp.bfloat16)
    ffn_input = rms_norm(middle, pre_ffn_gain).astype(jnp.bfloat16)
    gathered = lax.all_gather(ffn_input, "tp", axis=0, tiled=True)
    if not short:
        gate_act = jnp.dot(
            gathered,
            lax.all_gather(w_gate, "sp", axis=0, tiled=True),
            preferred_element_type=jnp.float32,
        )
        up_act = jnp.dot(
            gathered,
            lax.all_gather(w_up, "sp", axis=0, tiled=True),
            preferred_element_type=jnp.float32,
        )
        hidden = (jax.nn.silu(gate_act) * up_act).astype(jnp.bfloat16)
        down_full = lax.all_gather(w_down, "sp", axis=1, tiled=True)
        partial = jnp.dot(hidden, down_full, preferred_element_type=jnp.float32)
        branch = lax.psum_scatter(
            partial.astype(jnp.bfloat16), "tp", scatter_dimension=0, tiled=True
        )
    else:
        branch = ring_feed_forward(gathered, gate_blocks, up_blocks, down_blocks, resid.shape)
    return (middle.astype(jnp.float32) + rms_norm(branch, post_ffn_gain)).astype(jnp.bfloat16)


MESH = pl.DeviceIdType.MESH
HEADER_ROWS = 16
F32 = jnp.float32
BF16 = jnp.bfloat16


def silu_of(v):
    return v / (1.0 + jnp.exp(-v))


def layer_kernel(
    q_in,
    k_in,
    v_in,
    gates_in,
    decay_in,
    norm_gain,
    ow_in,
    resid_in,
    mix_gain,
    pre_gain,
    wg_in,
    wu_in,
    wd_in,
    post_gain,
    out,
    q_ref,
    k_ref,
    v_ref,
    gates_ref,
    resid_ref,
    wg,
    wu,
    wd,
    ow,
    cum_row,
    cum_col,
    local_state,
    start_state,
    state_out,
    state_pair,
    total_out,
    total_in,
    retention,
    retained_out,
    retained_in,
    mixed,
    middle,
    rows,
    gate_acts,
    hidden,
    part_out,
    part_in,
    sum_out,
    sum_in,
    branch,
    local_sem,
    own_sem,
    z_send,
    z_recv,
    y_send,
    y_recv,
    c_send,
    c_recv,
    ow_send,
    ow_recv,
    pair_send,
    pair_recv,
    total_send,
    total_recv,
    ret_send,
    ret_recv,
    rows_send,
    rows_recv,
    part_send,
    part_recv,
    sum_send,
    sum_recv,
):
    sp, tp = lax.axis_index("sp"), lax.axis_index("tp")
    planes = lax.axis_size("sp") // 2
    z, y = sp // 2, sp % 2
    x, core = tp // 2, tp % 2
    parity = z % 2
    pair = z + 1 - 2 * parity
    far = (z + 2) % planes
    far_pair = (pair + 2) % planes
    other_x, other_y, other_core = 1 - x, 1 - y, 1 - core
    is_main = core == parity
    is_helper = core != parity
    sp_y = z * 2 + other_y
    sp_pair = pair * 2 + y
    tp_x = other_x * 2 + core
    tp_core = x * 2 + other_core
    tp_both = other_x * 2 + other_core

    row_count, _ = q_ref.shape
    heads = norm_gain.shape[0]
    dim = norm_gain.shape[1]
    block_count = row_count // BLOCK
    quarter = resid_in.shape[0]
    model = resid_in.shape[1]
    units = wg_in.shape[1]
    tps = ow.shape[0]
    scale = dim ** (-0.5)

    inputs = [
        (k_in, k_ref),
        (v_in, v_ref),
        (q_in, q_ref),
        (gates_in, gates_ref),
        (resid_in, resid_ref),
        (ow_in, ow.at[tp]),
    ]

    def local_copy(i):
        return pltpu.make_async_copy(inputs[i][0], inputs[i][1], local_sem.at[i])

    weights_in = (wg_in, wu_in, wd_in)
    weights = (wg, wu, wd)

    def own_copy(m):
        return pltpu.make_async_copy(weights_in[m], weights[m].at[sp], own_sem.at[m])

    for i in range(len(inputs)):
        local_copy(i).start()

    @pl.when(is_main)
    def _():
        for m in range(3):
            own_copy(m).start()

    def remote(src, dst, send, recv, device):
        return pltpu.make_async_remote_copy(
            src_ref=src,
            dst_ref=dst,
            send_sem=send,
            recv_sem=recv,
            device_id=device,
            device_id_type=MESH,
        )

    barrier = pltpu.get_barrier_semaphore()
    peers = [(((z + i) % planes) * 2 + y, tp) for i in range(1, 4)]
    peers += [(sp_y, tp), (sp, tp_x), (sp, tp_core), (sp, tp_both), (sp_pair, tp_x)]
    for peer in peers:
        pl.semaphore_signal(barrier, inc=1, device_id=peer, device_id_type=MESH)
    pl.semaphore_wait(barrier, len(peers))

    far_target = lax.select(is_main, far, far_pair)
    in_middle = jnp.logical_and(z > 0, z < planes - 1)
    at_end = jnp.logical_or(z == 0, z == planes - 1)

    def cut(ref, half):
        size = ref.shape[0] // 2
        return ref.at[half * size : (half + 1) * size]

    def source(m, half):
        return cut(weights_in[m], half)

    def slot(m, half, place):
        size = weights[m].shape[1] // 2
        return weights[m].at[place, half * size : (half + 1) * size]

    def z_near(m, half):
        piece = 2 * m + half
        return remote(
            source(m, half),
            slot(m, half, sp),
            z_send.at[piece, 0],
            z_recv.at[piece, z],
            (pair * 2 + y, tp),
        )

    def z_far(m, half):
        piece = 2 * m + half
        return remote(
            source(m, half),
            slot(m, half, sp),
            z_send.at[piece, 1],
            z_recv.at[piece, z],
            (far_target * 2 + y, tp),
        )

    def to_y(m, half, plane, src):
        piece, place = 2 * m + half, plane * 2 + y
        return remote(
            src,
            slot(m, half, place),
            y_send.at[piece, plane],
            y_recv.at[piece, plane],
            (sp_y, tp),
        )

    def to_core(m, half, place, src):
        piece = 2 * m + half
        return remote(
            src,
            slot(m, half, place),
            c_send.at[piece, place],
            c_recv.at[piece, place],
            (sp, tp_core),
        )

    def z_arrival(m, half, plane):
        piece, here = 2 * m + half, slot(m, half, plane * 2 + y)
        return remote(here, here, z_send.at[piece, 1], z_recv.at[piece, plane], (sp_y, tp))

    def y_arrival(m, half, plane):
        piece, here = 2 * m + half, slot(m, half, plane * 2 + other_y)
        return remote(here, here, y_send.at[piece, plane], y_recv.at[piece, plane], (sp_y, tp))

    def start_own(m):
        @pl.when(is_main)
        def _():
            for half in range(2):
                to_y(m, half, z, source(m, half)).start()
                to_core(m, half, sp, source(m, half)).start()

    def pass_plane(m, half, plane):
        z_arrival(m, half, plane).wait_recv()
        here = slot(m, half, plane * 2 + y)
        to_y(m, half, plane, here).start()
        to_core(m, half, plane * 2 + y, here).start()

    def pass_z(m, half, planes_list):
        @pl.when(is_main)
        def _():
            for plane in planes_list:
                pass_plane(m, half, plane)

    def pass_if(condition, m, half, plane):
        @pl.when(jnp.logical_and(condition, is_main))
        def _():
            pass_plane(m, half, plane)

    def pass_y(m, half, planes_list, condition=True):
        @pl.when(jnp.logical_and(condition, is_main))
        def _():
            for plane in planes_list:
                y_arrival(m, half, plane).wait_recv()
                place = plane * 2 + other_y
                to_core(m, half, place, slot(m, half, place)).start()

    def core_wait(m, planes_list):
        @pl.when(is_helper)
        def _():
            for plane in planes_list:
                for half in range(2):
                    for place in (plane * 2 + y, plane * 2 + other_y):
                        here = slot(m, half, place)
                        to_core(m, half, place, here).wait_recv()

    def own_wait(m):
        @pl.when(is_main)
        def _():
            own_copy(m).wait()

    near_up = parity == 0
    far_up = z < planes // 2
    near_down, far_down = parity == 1, z >= planes // 2
    one_hop = jnp.logical_and(in_middle, is_helper)
    more_hops = jnp.logical_or(at_end, is_main)
    both = jnp.logical_and

    def when_do(condition, do):
        @pl.when(condition)
        def _():
            do()

    def start_far(m, half, condition):
        when_do(condition, lambda: z_far(m, half).start())

    def start_near(m, half, condition):
        when_do(both(is_helper, condition), lambda: z_near(m, half).start())

    when_do(is_helper, lambda: z_near(0, 0).start())
    start_far(0, 0, jnp.logical_or(far_down, one_hop))
    when_do(is_helper, lambda: z_near(0, 1).start())
    start_far(0, 1, far_down)
    near_planes = [pair, far, far_pair]
    all_planes = [z] + near_planes

    ow_copies = [
        remote(ow_in, ow.at[tp], ow_send.at[0], ow_recv.at[tp], (sp, tp_x)),
        remote(ow_in, ow.at[tp], ow_send.at[1], ow_recv.at[tp], (sp, tp_core)),
        remote(ow.at[tp_x], ow.at[tp_x], ow_send.at[2], ow_recv.at[tp_x], (sp, tp_core)),
    ]
    ow_copies[0].start()
    ow_copies[1].start()

    for i in range(3):
        local_copy(i).wait()

    row_index = lax.broadcasted_iota(jnp.int32, (BLOCK, BLOCK), 0)
    col_index = lax.broadcasted_iota(jnp.int32, (BLOCK, BLOCK), 1)
    before = jnp.where(row_index <= col_index, 1.0, 0.0).astype(BF16)
    until = jnp.where(row_index >= col_index, 1.0, 0.0).astype(BF16)
    for b in range(block_count):
        decay = decay_in[:, b * BLOCK : (b + 1) * BLOCK]
        high = decay.astype(BF16)
        rest = decay - high.astype(F32)
        middle_term = rest.astype(BF16)
        low = (rest - middle_term.astype(F32)).astype(BF16)
        by_row, by_col = 0.0, 0.0
        for term in (low, middle_term, high):
            by_row = by_row + jnp.dot(term, before, preferred_element_type=F32)
            by_col = by_col + lax.dot_general(
                until, term, (((1,), (1,)), ((), ())), preferred_element_type=F32
            )
        cum_row[b] = by_row
        cum_col[b] = by_col

    def block_decay(b, h):
        return jnp.exp(cum_row[b, h : h + 1, BLOCK - 1 : BLOCK])

    for h in range(heads):
        lanes = slice(h * dim, (h + 1) * dim)
        for b in range(block_count):
            span = slice(b * BLOCK, (b + 1) * BLOCK)
            last = cum_row[b, h : h + 1, BLOCK - 1 : BLOCK]
            to_end = jnp.exp(last - cum_col[b, :, h : h + 1]) * scale
            scaled = (k_ref[span, lanes].astype(F32) * to_end).astype(BF16)
            local_state[b, h] = lax.dot_general(
                scaled, v_ref[span, lanes], (((0,), (0,)), ((), ())), preferred_element_type=F32
            )

    def local_total(h):
        total, decay = local_state[0, h], block_decay(0, h)
        for b in range(1, block_count):
            total = block_decay(b, h) * total + local_state[b, h]
            decay = decay * block_decay(b, h)
        return total, decay

    header_row = lax.broadcasted_iota(jnp.int32, (HEADER_ROWS, dim), 0)

    def pack(ref, h, total, decay):
        ref[h, :dim] = total.astype(BF16)
        wide = jnp.broadcast_to(decay, (HEADER_ROWS, dim))
        high = wide.astype(BF16).astype(F32)
        ref[h, dim:] = jnp.where(header_row < 8, high, wide - high).astype(BF16)

    def unpack(packed, h):
        block = packed[h].astype(F32)
        return block[:dim], block[dim : dim + 1] + block[dim + 8 : dim + 9]

    for h in range(heads):
        total, decay = local_total(h)
        pack(state_out, h, total, decay)
    pair_copy = remote(state_out, state_pair, pair_send.at[0], pair_recv.at[0], (sp_y, tp))
    pair_copy.start()
    start_own(0)

    def scores_of(b):
        for h in range(heads):
            lanes = slice(h * dim, (h + 1) * dim)
            span = slice(b * BLOCK, (b + 1) * BLOCK)
            tile = 128
            keys, vals = k_ref[span, lanes], v_ref[span, lanes]
            row_sums = cum_row[b, h : h + 1, :]

            def one(i, _):
                at = pl.multiple_of(i * tile, tile)
                here = pl.ds(b * BLOCK + at, tile)
                products = lax.dot_general(
                    q_ref[here, lanes], keys, (((1,), (1,)), ((), ())), preferred_element_type=F32
                )
                gap = cum_col[b, pl.ds(at, tile), h : h + 1] - row_sums
                t_index = at + lax.broadcasted_iota(jnp.int32, (tile, BLOCK), 0)
                s_index = lax.broadcasted_iota(jnp.int32, (tile, BLOCK), 1)
                weight = jnp.where(s_index <= t_index, jnp.exp(jnp.minimum(gap, 0.0)), 0.0)
                scores = (products * scale * weight).astype(BF16)
                retention[here, lanes] = jnp.dot(scores, vals, preferred_element_type=F32)
                return 0

            lax.fori_loop(0, BLOCK // tile, one, 0)

    scores_of(0)

    pair_copy.wait_recv()
    for h in range(heads):
        total, decay = local_total(h)
        their_total, their_decay = unpack(state_pair, h)
        last_factor = jnp.where(y == 1, decay, their_decay)
        first = jnp.where(y == 1, their_total, total)
        second = jnp.where(y == 1, total, their_total)
        pack(total_out, h, last_factor * first + second, decay * their_decay)

    def total_copy(plane):
        return remote(
            total_out,
            total_in.at[z],
            total_send.at[plane],
            total_recv.at[z],
            (plane * 2 + y, tp),
        )

    for plane in range(1, 4):

        @pl.when(z < plane)
        def _():
            total_copy(plane).start()


    for half in range(2):
        start_far(1, half, both(far_down, in_middle))
        start_near(1, half, near_down)
    for b in range(1, block_count):
        scores_of(b)

    ow_arrival = [
        remote(ow.at[t], ow.at[t], ow_send.at[0], ow_recv.at[t], (sp, tp_x))
        for t in (tp_x, tp_core, tp_both)
    ]

    for h in range(heads):
        start_state[0, h] = jnp.zeros((dim, dim), F32)
    for plane in range(3):

        @pl.when(plane < z)
        def _():
            remote(
                total_out,
                total_in.at[plane],
                total_send.at[plane],
                total_recv.at[plane],
                (sp_y, tp),
            ).wait_recv()
            for h in range(heads):
                total, decay = unpack(total_in.at[plane], h)
                start_state[0, h] = decay * start_state[0, h] + total

    for h in range(heads):
        their_total, their_decay = unpack(state_pair, h)
        state = start_state[0, h]
        state = jnp.where(y == 1, their_decay * state + their_total, state)
        start_state[0, h] = state
        for b in range(1, block_count):
            state = block_decay(b - 1, h) * state + local_state[b - 1, h]
            start_state[b, h] = state

    local_copy(3).wait()

    def retained_copy(j):
        return remote(
            retained_out.at[j],
            retained_in.at[tp],
            ret_send.at[j],
            ret_recv.at[tp],
            (sp, j),
        )

    per_block = BLOCK // quarter

    def finish(j, target):
        b = j // per_block
        at = pl.multiple_of((j % per_block) * quarter, quarter)
        here = pl.ds(pl.multiple_of(j * quarter, quarter), quarter)
        for h in range(heads):
            lanes = slice(h * dim, (h + 1) * dim)
            state = start_state[b, h]
            high = state.astype(BF16)
            low = (state - high.astype(F32)).astype(BF16)
            query = q_ref[here, lanes]
            carried = jnp.dot(query, high, preferred_element_type=F32) + jnp.dot(
                query, low, preferred_element_type=F32
            )
            kept = retention[here, lanes] + carried * jnp.exp(
                cum_col[b, pl.ds(at, quarter), h : h + 1]
            )
            centered = kept - jnp.mean(kept, axis=-1, keepdims=True)
            variance = jnp.mean(centered * centered, axis=-1, keepdims=True)
            normed = centered * lax.rsqrt(variance + EPSILON) * norm_gain[h : h + 1, :]
            target[:, lanes] = (silu_of(gates_ref[here, lanes].astype(F32)) * normed).astype(BF16)

    others = [(tp + i) % tps for i in range(1, tps)]
    start_far(0, 0, both(far_up, more_hops))
    start_far(0, 1, far_up)
    for half in range(2):
        start_far(1, half, both(far_up, in_middle))
        start_near(1, half, near_up)

    for j in others:
        finish(j, retained_out.at[j])
        retained_copy(j).start()
    finish(tp, retained_in.at[tp])

    pass_z(0, 0, near_planes[:1])
    start_own(1)
    ow_arrival[0].wait_recv()
    ow_copies[2].start()
    for arrival in ow_arrival[1:]:
        arrival.wait_recv()
    local_copy(5).wait()
    local_copy(4).wait()
    for j in others:
        remote(
            retained_out.at[j],
            retained_in.at[j],
            ret_send.at[j],
            ret_recv.at[j],
            (sp, j),
        ).wait_recv()

    mix_tile = 512

    def mix(i, _):
        here = pl.ds(pl.multiple_of(i * mix_tile, mix_tile), mix_tile)
        total = jnp.zeros((quarter, mix_tile), F32)
        for g in range(tps):
            part = jnp.dot(retained_in[g], ow[g, :, here], preferred_element_type=F32)
            total = total + part.astype(BF16).astype(F32)
        mixed[:, here] = total.astype(BF16)
        return 0

    lax.fori_loop(0, model // mix_tile, mix, 0)

    def rms_of(v):
        return v * lax.rsqrt(jnp.mean(v * v, axis=-1, keepdims=True) + EPSILON)

    mine = x * 2 + parity
    norm_tile = 32

    def into_rows(i, _):
        here = pl.ds(pl.multiple_of(i * norm_tile, norm_tile), norm_tile)
        value = rms_of(mixed[here, :].astype(F32)) * mix_gain[...]
        value = (resid_ref[here, :].astype(F32) + value).astype(BF16)
        middle[here, :] = value
        rows[mine, here, :] = (rms_of(value.astype(F32)) * pre_gain[...]).astype(BF16)
        return 0

    from_pair = x * 2 + 1 - parity
    from_x = other_x * 2 + parity
    from_both = other_x * 2 + 1 - parity
    row_parts = 4
    part_rows = quarter // row_parts

    def rows_copy(i, half, place, device):
        here = rows.at[place, half * part_rows : (half + 1) * part_rows]
        return remote(here, here, rows_send.at[i, half], rows_recv.at[place, half], device)

    for half in range(row_parts):
        steps = part_rows // norm_tile
        lax.fori_loop(half * steps, (half + 1) * steps, into_rows, 0)
        rows_copy(0, half, mine, (sp_pair, tp)).start()
        rows_copy(1, half, mine, (sp, tp_x)).start()

    pass_z(0, 1, near_planes[:1])
    pass_z(0, 0, near_planes[1:])
    pass_z(0, 1, near_planes[1:])
    for half in range(2):
        pass_z(1, half, near_planes[:1])
    for half in range(row_parts // 2):
        rows_copy(0, half, from_pair, (sp_pair, tp)).wait_recv()
        rows_copy(2, half, from_pair, (sp, tp_x)).start()
    for half in range(2):
        start_far(1, half, at_end)
    start_own(2)
    for half in range(2):
        pass_if(at_end, 1, half, far)
        pass_if(in_middle, 1, half, far_pair)
    for half in range(row_parts // 2, row_parts):
        rows_copy(0, half, from_pair, (sp_pair, tp)).wait_recv()
        rows_copy(2, half, from_pair, (sp, tp_x)).start()
    for half in range(2):
        when_do(is_helper, lambda: z_near(2, half).start())
        start_far(2, half, in_middle)
    for half in range(2):
        pass_y(0, half, all_planes)
    own_wait(0)
    core_wait(0, all_planes)

    unit_tile = 256
    unit_steps = units // unit_tile

    def acts_of(weight, first, at, size):
        here = pl.ds(at, size)
        return jnp.dot(
            rows[pl.ds(first, 2)].reshape(2 * quarter, model),
            weight[:, :, here].reshape(model, size),
            preferred_element_type=F32,
        ).reshape(2, quarter, size)

    def over_units(one, begin=0, end=unit_steps + 1):
        def step(i, _):
            one(pl.multiple_of(i * unit_tile, unit_tile), unit_tile)
            return 0

        lax.fori_loop(begin, min(end, unit_steps), step, 0)
        if end > unit_steps and units % unit_tile:
            one(unit_steps * unit_tile, units % unit_tile)

    def gate_of(first):
        def one(at, size):
            gate_acts[pl.ds(first, 2), :, pl.ds(at, size)] = acts_of(wg, first, at, size)

        over_units(one)

    def up_of(first, begin=0, end=unit_steps + 1):
        def one(at, size):
            here = pl.ds(at, size)
            gate = gate_acts[pl.ds(first, 2), :, here]
            value = silu_of(gate) * acts_of(wu, first, at, size)
            hidden[pl.ds(first, 2), :, here] = value.astype(BF16)

        over_units(one, begin, end)

    gate_of(x * 2)
    for half in range(2):
        start_far(2, half, at_end)
    pass_if(at_end, 1, 0, far_pair)
    pass_if(in_middle, 1, 0, far)
    pass_if(at_end, 1, 1, far_pair)
    pass_if(in_middle, 1, 1, far)
    for half in range(2):
        pass_y(1, half, [z, pair])
        pass_y(1, half, [far], at_end)
        pass_y(1, half, [far_pair], in_middle)
    pass_z(2, 0, near_planes[:1])
    for half in range(row_parts):
        rows_copy(1, half, from_x, (sp, tp_x)).wait_recv()
        rows_copy(2, half, from_both, (sp, tp_x)).wait_recv()
    gate_of(other_x * 2)
    for half in range(2):
        pass_y(1, half, [far_pair], at_end)
        pass_y(1, half, [far], in_middle)
    for half in range(2):
        pass_y(2, half, [z])
    pass_z(2, 1, near_planes[:1])
    own_wait(1)
    core_wait(1, all_planes)

    columns = wd_in.shape[1]

    def down(place, first, second):
        left = jnp.concatenate([hidden[first], hidden[second]], axis=0)
        product = jnp.dot(left, wd[place], preferred_element_type=F32)
        return product.astype(BF16).reshape(2, quarter, columns)

    def place_of(plane, over_x):
        even = plane % 2 == 0
        return plane * 2 + (lax.select(even, y, other_y) if over_x else lax.select(even, other_y, y))

    def block_of(plane, own):
        place = plane * 2 + (y if own else other_y)
        return place, (plane % 2 == 0) if own else (plane % 2 == 1)

    def part_copy(place, over_x):
        if isinstance(over_x, bool):
            device = (sp, tp_x) if over_x else (sp_pair, tp)
        else:
            device = (lax.select(over_x, sp, sp_pair), lax.select(over_x, tp_x, tp))
        return remote(
            part_out.at[place], part_in.at[place], part_send.at[place], part_recv.at[place], device
        )

    def sum_copy(place, over_x):
        device = (sp_pair, tp) if over_x else (sp, tp_x)
        return remote(
            sum_out.at[place], sum_in.at[place], sum_send.at[place], sum_recv.at[place], device
        )

    def place_wait(place):
        @pl.when(is_helper)
        def _():
            for half in range(2):
                to_core(2, half, place, slot(2, half, place)).wait_recv()

    def send_part(plane, own):
        place, over_x = block_of(plane, own)
        if not own and plane is not z:
            for half in range(2):
                pass_y(2, half, [plane])
        place_wait(place)
        part_out[place] = down(
            place,
            lax.select(over_x, other_x * 2, 1 - parity),
            lax.select(over_x, other_x * 2 + 1, 3 - parity),
        )
        part_copy(place, over_x).start()

    def own_product(plane, over_x):
        place = place_of(plane, over_x)
        product = down(place, mine, from_pair if over_x else from_x)
        branch[place] = product[0].astype(F32)
        sum_out[place] = product[1]

    def own_part(plane, over_x):
        place = place_of(plane, over_x)
        mine_at, other_at = (parity, 1 - parity) if over_x else (x, other_x)
        part_copy(place, over_x).wait_recv()
        sum_out[place] = (
            sum_out[place].astype(F32) + part_in[place, other_at].astype(F32)
        ).astype(BF16)
        sum_copy(place, over_x).start()
        branch[place] = branch[place] + part_in[place, mine_at].astype(F32)

    def pass_late(half):
        pass_if(at_end, 2, half, far)
        pass_if(at_end, 2, half, far_pair)
        pass_if(in_middle, 2, half, far_pair)
        pass_if(in_middle, 2, half, far)

    up_of(other_x * 2)
    own_wait(2)
    when_do(parity == 0, lambda: send_part(z, True))
    when_do(parity == 1, lambda: send_part(z, False))
    up_of(x * 2, 0, unit_steps // 2)
    pass_late(0)
    up_of(x * 2, unit_steps // 2)
    when_do(parity == 0, lambda: send_part(z, False))
    when_do(parity == 1, lambda: send_part(z, True))
    pass_late(1)
    send_part(pair, True)
    own_product(z, True)
    own_product(z, False)
    own_part(z, True)
    send_part(pair, False)
    send_part(far, True)
    own_product(pair, True)
    own_product(pair, False)
    own_part(pair, False)
    send_part(far, False)
    send_part(far_pair, True)
    send_part(far_pair, False)
    own_part(z, False)
    own_part(pair, True)
    own_product(far, True)
    own_part(far, True)
    own_product(far_pair, False)
    own_part(far_pair, False)
    own_product(far_pair, True)
    own_part(far_pair, True)
    own_product(far, False)
    own_part(far, False)

    for plane in all_planes:
        for over_x in (True, False):
            sum_copy(place_of(plane, over_x), over_x).wait_recv()

    def final(i, _):
        here = pl.ds(pl.multiple_of(i * norm_tile, norm_tile), norm_tile)
        value = jnp.concatenate(
            [branch[n, here, :] + sum_in[n, here, :].astype(F32) for n in range(2 * planes)],
            axis=1,
        )
        value = rms_of(value.astype(BF16).astype(F32)) * post_gain[...]
        out[here, :] = (middle[here, :].astype(F32) + value).astype(BF16)
        return 0

    lax.fori_loop(0, quarter // norm_tile, final, 0)

    for m in range(3):
        for half in range(2):
            z_far(m, half).wait_send()
            when_do(is_helper, lambda: z_near(m, half).wait_send())

            @pl.when(is_main)
            def _():
                for plane in all_planes:
                    place = plane * 2 + y
                    src = source(m, half) if plane is z else slot(m, half, place)
                    to_y(m, half, plane, src).wait_send()
                    to_core(m, half, place, src).wait_send()
                    place = plane * 2 + other_y
                    to_core(m, half, place, slot(m, half, place)).wait_send()

    for copy in ow_copies:
        copy.wait_send()
    pair_copy.wait_send()
    for plane in range(1, 4):

        @pl.when(z < plane)
        def _():
            total_copy(plane).wait_send()

    for j in others:
        retained_copy(j).wait_send()
    for half in range(row_parts):
        rows_copy(0, half, mine, (sp_pair, tp)).wait_send()
        rows_copy(1, half, mine, (sp, tp_x)).wait_send()
        rows_copy(2, half, from_pair, (sp, tp_x)).wait_send()
    for plane in range(planes):
        for over_x in (True, False):
            place = plane * 2 + int(over_x)
            part_copy(place, over_x).wait_send()
            sum_copy(place, over_x).wait_send()


def whole_layer(
    queries,
    keys,
    values,
    gates,
    log_decay,
    norm_gain,
    out_weight,
    resid,
    post_mix_gain,
    pre_ffn_gain,
    w_gate,
    w_up,
    w_down,
    post_ffn_gain,
):
    places, tps = lax.axis_size("sp"), lax.axis_size("tp")
    planes = places // 2
    row_count, width = queries.shape
    heads, dim = norm_gain.shape
    block_count = row_count // BLOCK
    quarter, model = resid.shape
    depth, units = w_gate.shape
    columns = w_down.shape[1]
    decay_rows = log_decay.T
    anywhere = pl.BlockSpec(memory_space=pl.ANY)
    onchip = pl.BlockSpec(memory_space=pltpu.VMEM)
    dma = pltpu.SemaphoreType.DMA
    packed = (heads, dim + HEADER_ROWS, dim)
    scratch = [
        pltpu.VMEM((row_count, width), BF16),
        pltpu.VMEM((row_count, width), BF16),
        pltpu.VMEM((row_count, width), BF16),
        pltpu.VMEM((row_count, width), BF16),
        pltpu.VMEM((quarter, model), BF16),
        pltpu.VMEM((places, depth, units), BF16),
        pltpu.VMEM((places, depth, units), BF16),
        pltpu.VMEM((places, units, columns), BF16),
        pltpu.VMEM((tps, width, model), BF16),
        pltpu.VMEM((block_count, heads, BLOCK), F32),
        pltpu.VMEM((block_count, BLOCK, heads), F32),
        pltpu.VMEM((block_count, heads, dim, dim), F32),
        pltpu.VMEM((block_count, heads, dim, dim), F32),
        pltpu.VMEM(packed, BF16),
        pltpu.VMEM(packed, BF16),
        pltpu.VMEM(packed, BF16),
        pltpu.VMEM((planes,) + packed, BF16),
        pltpu.VMEM((row_count, width), F32),
        pltpu.VMEM((tps, quarter, width), BF16),
        pltpu.VMEM((tps, quarter, width), BF16),
        pltpu.VMEM((quarter, model), BF16),
        pltpu.VMEM((quarter, model), BF16),
        pltpu.VMEM((4, quarter, model), BF16),
        pltpu.VMEM((4, quarter, units), F32),
        pltpu.VMEM((4, quarter, units), BF16),
        pltpu.VMEM((places, 2, quarter, columns), BF16),
        pltpu.VMEM((places, 2, quarter, columns), BF16),
        pltpu.VMEM((places, quarter, columns), BF16),
        pltpu.VMEM((places, quarter, columns), BF16),
        pltpu.VMEM((places, quarter, columns), F32),
        dma((6,)),
        dma((3,)),
        dma((6, 2)),
        dma((6, planes)),
        dma((6, planes)),
        dma((6, planes)),
        dma((6, places)),
        dma((6, places)),
        dma((3,)),
        dma((tps,)),
        dma((1,)),
        dma((1,)),
        dma((planes,)),
        dma((planes,)),
        dma((tps,)),
        dma((tps,)),
        dma((3, 4)),
        dma((4, 4)),
        dma((places,)),
        dma((places,)),
        dma((places,)),
        dma((places,)),
    ]
    return pl.pallas_call(
        layer_kernel,
        out_shape=jax.ShapeDtypeStruct((quarter, model), BF16),
        in_specs=[anywhere] * 4
        + [onchip, onchip, anywhere, anywhere, onchip, onchip]
        + [anywhere] * 3
        + [onchip],
        out_specs=onchip,
        scratch_shapes=scratch,
        compiler_params=pltpu.CompilerParams(
            collective_id=0, has_side_effects=True, vmem_limit_bytes=62 * 1024 * 1024
        ),
    )(
        queries,
        keys,
        values,
        gates,
        decay_rows,
        norm_gain,
        out_weight,
        resid,
        post_mix_gain[None],
        pre_ffn_gain[None],
        w_gate,
        w_up,
        w_down,
        post_ffn_gain[None],
    )


def solution(mesh):
    in_specs = (
        P("sp", "tp"),
        P("sp", "tp"),
        P("sp", "tp"),
        P("sp", "tp"),
        P("sp", "tp"),
        P("tp", None),
        P("tp", None),
        P(("sp", "tp"), None),
        P(),
        P(),
        P("sp", "tp"),
        P("sp", "tp"),
        P("tp", "sp"),
        P(),
    )
    out_specs = P(("sp", "tp"), None)
    if mesh.shape["sp"] == LONGEST_RING and mesh.shape["tp"] == 4:
        return jax.shard_map(
            whole_layer, mesh=mesh, in_specs=in_specs, out_specs=out_specs, check_vma=False
        )

    return jax.shard_map(
        per_device, mesh=mesh, in_specs=in_specs, out_specs=out_specs, check_vma=False
    )
```

```python
import jax
import jax.numpy as jnp
from jax import lax
from jax.experimental import pallas as pl
from jax.experimental.pallas import tpu as pltpu
from jax.sharding import PartitionSpec as P


BLOCK = 512


EPSILON = 1e-06
LONGEST_RING = 8


def entering(decay, state):
    place = lax.axis_index("sp")
    head_count, head_dim, _ = state.shape
    decay_rows = jnp.broadcast_to(decay[:, None, None], (head_count, 16, head_dim))
    packed = jnp.concatenate([state, decay_rows], axis=1).astype(jnp.bfloat16)
    gathered = lax.all_gather(packed, "sp")

    def one(step, running):
        piece = lax.dynamic_index_in_dim(gathered, step, 0, False).astype(jnp.float32)
        return piece[:, head_dim : head_dim + 1, :] * running + piece[:, :head_dim]

    return lax.fori_loop(0, place, one, jnp.zeros_like(state))


def from_earlier(packed, distance):
    count = lax.axis_size("sp")
    return lax.ppermute(packed, "sp", [(i, i + distance) for i in range(count - distance)])


def entering_by_hops(decay, state):
    count = lax.axis_size("sp")
    head_count, head_dim, _ = state.shape
    decay_rows = jnp.broadcast_to(decay[:, None, None], (head_count, 8, head_dim))
    packed = jnp.concatenate([state, decay_rows], axis=1)
    near = from_earlier(packed, 1)
    far = from_earlier(packed, 2)
    factor = near[:, head_dim:]
    pair = jnp.concatenate(
        [factor[:, :1] * far[:, :head_dim] + near[:, :head_dim], factor * far[:, head_dim:]],
        axis=1,
    )
    total, factor = pair[:, :head_dim], pair[:, head_dim : head_dim + 1]
    for piece in [from_earlier(pair, distance) for distance in range(2, count, 2)]:
        total = total + factor * piece[:, :head_dim]
        factor = factor * piece[:, head_dim : head_dim + 1]
    return total


def ring_order(count):
    return list(range(0, count, 2)) + list(range(1, count, 2))[::-1]


def ring_gather(block, forward_steps, backward_steps):
    count = lax.axis_size("sp")
    order = ring_order(count)
    ahead = [(order[i], order[(i + 1) % count]) for i in range(count)]
    behind = [(b, a) for a, b in ahead]
    arrived = [(0, block)]
    up, down = block, block
    for step in range(1, max(forward_steps, backward_steps) + 1):
        if step <= forward_steps:
            up = lax.ppermute(up, "sp", ahead)
            arrived.append((-step, up))
        if step <= backward_steps:
            down = lax.ppermute(down, "sp", behind)
            arrived.append((step, down))
    return arrived


def owner_of(offset):
    count = lax.axis_size("sp")
    me = lax.axis_index("sp")
    half = (count + 1) // 2
    position = jnp.where(me % 2 == 0, me // 2, count - 1 - me // 2)
    there = (position + offset + count) % count
    return jnp.where(there < half, 2 * there, 2 * (count - 1 - there) + 1)


def rms_norm(values_in, gain_vec):
    widened = values_in.astype(jnp.float32)
    return (
        widened
        * lax.rsqrt(jnp.mean(widened * widened, axis=-1, keepdims=True) + EPSILON)
        * gain_vec
    )


def block_step(carried, pieces):
    query_blk, key_blk, value_blk, decay_blk = pieces
    length = query_blk.shape[1]
    key_scale = query_blk.shape[2] ** (-0.5)
    cumulative = jnp.cumsum(decay_blk, axis=1)
    log_gap = cumulative[:, :, None] - cumulative[:, None, :]
    causal = lax.broadcasted_iota(jnp.int32, (length, length), 0) >= lax.broadcasted_iota(
        jnp.int32, (length, length), 1
    )
    weight = jnp.where(causal[None], jnp.exp(jnp.minimum(log_gap, 0.0)), 0.0)
    products = jnp.einsum("htd,hsd->hts", query_blk, key_blk, preferred_element_type=jnp.float32)
    scores = (products * key_scale * weight).astype(jnp.bfloat16)
    within = jnp.einsum("hts,hsd->htd", scores, value_blk, preferred_element_type=jnp.float32)
    carried_term = (
        jnp.einsum(
            "htd,hde->hte", query_blk.astype(jnp.float32), carried, precision=lax.Precision.HIGHEST
        )
        * jnp.exp(cumulative)[:, :, None]
    )
    to_end = jnp.exp(cumulative[:, -1:] - cumulative) * key_scale
    scaled_keys = (key_blk.astype(jnp.float32) * to_end[:, :, None]).astype(jnp.bfloat16)
    added = jnp.einsum("hsd,hse->hde", scaled_keys, value_blk, preferred_element_type=jnp.float32)
    carried = jnp.exp(cumulative[:, -1])[:, None, None] * carried + added
    return (carried, within + carried_term)


def to_blocks(matrix, block_len, head_count):
    row_count = matrix.shape[0]
    return matrix.reshape(row_count // block_len, block_len, head_count, -1).transpose(0, 2, 1, 3)


def finish_heads(retention, gates, norm_gain):
    centered = retention - jnp.mean(retention, axis=-1, keepdims=True)
    variance = jnp.mean(centered * centered, axis=-1, keepdims=True)
    normed = centered * lax.rsqrt(variance + EPSILON) * norm_gain[None]
    gate_vals = gates.astype(jnp.float32).reshape(normed.shape)
    return (jax.nn.silu(gate_vals) * normed).reshape(normed.shape[0], -1).astype(jnp.bfloat16)


def share_sum(part, row_count):
    count = lax.axis_size("tp")
    if count != 4:
        return lax.psum_scatter(part, "tp", scatter_dimension=0, tiled=True)
    me = lax.axis_index("tp")
    high, low = me // 2, me % 2
    shares = part.reshape(2, 2, row_count, -1)

    def swap(block, bit):
        return lax.ppermute(block, "tp", [(i, i ^ bit) for i in range(count)])

    def pick(block, index, dim):
        return lax.dynamic_index_in_dim(block, index, dim, False)

    nearer = swap(pick(shares, 1 - low, 1), 1).astype(jnp.float32)
    pair = pick(shares, low, 1).astype(jnp.float32) + nearer
    farther = swap(pick(pair, 1 - high, 0).astype(jnp.bfloat16), 2).astype(jnp.float32)
    return (pick(pair, high, 0) + farther).astype(jnp.bfloat16)


def ring_feed_forward(rows, gate_blocks, up_blocks, down_blocks, shape):
    depth = gate_blocks[0][1].shape[0]
    width = down_blocks[0][1].shape[1]
    half = (len(gate_blocks) + 1) // 2

    def project(blocks):
        total = None
        for some in (blocks[:half], blocks[half:]):
            if not some:
                continue
            columns = jnp.concatenate(
                [
                    lax.dynamic_slice_in_dim(rows, owner_of(offset) * depth, depth, 1)
                    for offset, _ in some
                ],
                axis=1,
            )
            weight = jnp.concatenate([block for _, block in some], axis=0)
            part = jnp.dot(columns, weight, preferred_element_type=jnp.float32)
            total = part if total is None else total + part
        return total

    gate_act = project(gate_blocks)
    up_act = project(up_blocks)
    hidden = (jax.nn.silu(gate_act) * up_act).astype(jnp.bfloat16)
    branch = jnp.zeros(shape, jnp.bfloat16)
    for some in (down_blocks[:half], down_blocks[half:]):
        if not some:
            continue
        wide = jnp.concatenate([block for _, block in some], axis=1)
        part = jnp.dot(hidden, wide, preferred_element_type=jnp.float32).astype(jnp.bfloat16)
        piece = share_sum(part, shape[0])
        for slot, (offset, _) in enumerate(some):
            branch = lax.dynamic_update_slice_in_dim(
                branch, piece[:, slot * width : (slot + 1) * width], owner_of(offset) * width, 1
            )
    return branch


def per_device(
    queries,
    keys,
    values,
    gates,
    log_decay,
    norm_gain,
    out_weight,
    resid,
    post_mix_gain,
    pre_ffn_gain,
    w_gate,
    w_up,
    w_down,
    post_ffn_gain,
):
    ring = lax.axis_size("sp")
    fewer = (ring - 1) // 2
    more = ring - 1 - fewer
    short = ring <= LONGEST_RING
    if short:
        gate_blocks = ring_gather(w_gate, more, fewer)
        up_blocks = ring_gather(w_up, fewer, more)
        down_blocks = ring_gather(w_down, more, fewer)
    row_count = queries.shape[0]
    head_count = log_decay.shape[1]
    head_dim = queries.shape[1] // head_count
    block_count = row_count // BLOCK
    query_blocks = to_blocks(queries, BLOCK, head_count)
    key_blocks = to_blocks(keys, BLOCK, head_count)
    value_blocks = to_blocks(values, BLOCK, head_count)
    decay_blocks = log_decay.reshape(block_count, BLOCK, head_count).transpose(0, 2, 1)
    start_state = jnp.zeros((head_count, head_dim, head_dim), jnp.float32)
    local_state, outputs = lax.scan(
        block_step, start_state, (query_blocks, key_blocks, value_blocks, decay_blocks)
    )
    retention = outputs.transpose(0, 2, 1, 3).reshape(row_count, head_count, head_dim)
    cumulative = jnp.cumsum(log_decay, axis=0)
    local_decay = jnp.exp(cumulative[-1])
    incoming = (entering_by_hops if short else entering)(local_decay, local_state)
    query_rows = queries.reshape(row_count, head_count, head_dim).astype(jnp.float32)
    retention = (
        retention
        + jnp.einsum("thd,hde->the", query_rows, incoming, precision=lax.Precision.HIGHEST)
        * jnp.exp(cumulative)[:, :, None]
    )
    retained = finish_heads(retention, gates, norm_gain)
    quarter = resid.shape[0]
    regrouped = lax.all_to_all(retained, "tp", split_axis=0, concat_axis=1, tiled=True)
    group_rows = out_weight.shape[0]
    empty_mix = jnp.zeros((quarter, out_weight.shape[1]), jnp.float32)
    running = empty_mix
    shard_piece = lax.all_gather(out_weight, "tp", axis=0, tiled=True)
    for offset in range(shard_piece.shape[0] // group_rows):
        columns = lax.dynamic_slice_in_dim(regrouped, offset * group_rows, group_rows, 1)
        part = jnp.dot(
            columns,
            shard_piece[offset * group_rows : (offset + 1) * group_rows],
            preferred_element_type=jnp.float32,
        )
        running = running + part.astype(jnp.bfloat16).astype(jnp.float32)
    mixed = running
    mixed = mixed.astype(jnp.bfloat16)
    middle = (resid.astype(jnp.float32) + rms_norm(mixed, post_mix_gain)).astype(jnp.bfloat16)
    ffn_input = rms_norm(middle, pre_ffn_gain).astype(jnp.bfloat16)
    gathered = lax.all_gather(ffn_input, "tp", axis=0, tiled=True)
    if not short:
        gate_act = jnp.dot(
            gathered,
            lax.all_gather(w_gate, "sp", axis=0, tiled=True),
            preferred_element_type=jnp.float32,
        )
        up_act = jnp.dot(
            gathered,
            lax.all_gather(w_up, "sp", axis=0, tiled=True),
            preferred_element_type=jnp.float32,
        )
        hidden = (jax.nn.silu(gate_act) * up_act).astype(jnp.bfloat16)
        down_full = lax.all_gather(w_down, "sp", axis=1, tiled=True)
        partial = jnp.dot(hidden, down_full, preferred_element_type=jnp.float32)
        branch = lax.psum_scatter(
            partial.astype(jnp.bfloat16), "tp", scatter_dimension=0, tiled=True
        )
    else:
        branch = ring_feed_forward(gathered, gate_blocks, up_blocks, down_blocks, resid.shape)
    return (middle.astype(jnp.float32) + rms_norm(branch, post_ffn_gain)).astype(jnp.bfloat16)


MESH = pl.DeviceIdType.MESH
HEADER_ROWS = 16
F32 = jnp.float32
BF16 = jnp.bfloat16


def silu_of(v):
    return v / (1.0 + jnp.exp(-v))


def layer_kernel(
    q_in,
    k_in,
    v_in,
    gates_in,
    decay_in,
    norm_gain,
    ow_in,
    resid_in,
    mix_gain,
    pre_gain,
    wg_in,
    wu_in,
    wd_in,
    post_gain,
    out,
    q_ref,
    k_ref,
    v_ref,
    gates_ref,
    resid_ref,
    wg,
    wu,
    wd,
    ow,
    cum_row,
    cum_col,
    local_state,
    start_state,
    state_out,
    state_pair,
    total_out,
    total_in,
    retention,
    retained_out,
    retained_in,
    mixed,
    middle,
    rows,
    gate_acts,
    hidden,
    part_out,
    part_in,
    sum_out,
    sum_in,
    branch,
    local_sem,
    own_sem,
    z_send,
    z_recv,
    y_send,
    y_recv,
    c_send,
    c_recv,
    ow_send,
    ow_recv,
    pair_send,
    pair_recv,
    total_send,
    total_recv,
    ret_send,
    ret_recv,
    rows_send,
    rows_recv,
    part_send,
    part_recv,
    sum_send,
    sum_recv,
):
    sp, tp = lax.axis_index("sp"), lax.axis_index("tp")
    planes = lax.axis_size("sp") // 2
    z, y = sp // 2, sp % 2
    x, core = tp // 2, tp % 2
    parity = z % 2
    pair = z + 1 - 2 * parity
    far = (z + 2) % planes
    far_pair = (pair + 2) % planes
    other_x, other_y, other_core = 1 - x, 1 - y, 1 - core
    is_main = core == parity
    is_helper = core != parity
    sp_y = z * 2 + other_y
    sp_pair = pair * 2 + y
    tp_x = other_x * 2 + core
    tp_core = x * 2 + other_core
    tp_both = other_x * 2 + other_core

    row_count, _ = q_ref.shape
    heads = norm_gain.shape[0]
    dim = norm_gain.shape[1]
    block_count = row_count // BLOCK
    quarter = resid_in.shape[0]
    model = resid_in.shape[1]
    units = wg_in.shape[1]
    tps = ow.shape[0]
    scale = dim ** (-0.5)

    inputs = [
        (k_in, k_ref),
        (v_in, v_ref),
        (q_in, q_ref),
        (gates_in, gates_ref),
        (resid_in, resid_ref),
        (ow_in, ow.at[tp]),
    ]

    def local_copy(i):
        return pltpu.make_async_copy(inputs[i][0], inputs[i][1], local_sem.at[i])

    weights_in = (wg_in, wu_in, wd_in)
    weights = (wg, wu, wd)

    def own_copy(m):
        return pltpu.make_async_copy(weights_in[m], weights[m].at[sp], own_sem.at[m])

    for i in range(len(inputs)):
        local_copy(i).start()

    @pl.when(is_main)
    def _():
        for m in range(3):
            own_copy(m).start()

    def remote(src, dst, send, recv, device):
        return pltpu.make_async_remote_copy(
            src_ref=src,
            dst_ref=dst,
            send_sem=send,
            recv_sem=recv,
            device_id=device,
            device_id_type=MESH,
        )

    barrier = pltpu.get_barrier_semaphore()
    peers = [(((z + i) % planes) * 2 + y, tp) for i in range(1, 4)]
    peers += [(sp_y, tp), (sp, tp_x), (sp, tp_core), (sp, tp_both), (sp_pair, tp_x)]
    for peer in peers:
        pl.semaphore_signal(barrier, inc=1, device_id=peer, device_id_type=MESH)
    pl.semaphore_wait(barrier, len(peers))

    far_target = lax.select(is_main, far, far_pair)
    in_middle = jnp.logical_and(z > 0, z < planes - 1)
    at_end = jnp.logical_or(z == 0, z == planes - 1)

    def cut(ref, half):
        size = ref.shape[0] // 2
        return ref.at[half * size : (half + 1) * size]

    def source(m, half):
        return cut(weights_in[m], half)

    def slot(m, half, place):
        size = weights[m].shape[1] // 2
        return weights[m].at[place, half * size : (half + 1) * size]

    def z_near(m, half):
        piece = 2 * m + half
        return remote(
            source(m, half),
            slot(m, half, sp),
            z_send.at[piece, 0],
            z_recv.at[piece, z],
            (pair * 2 + y, tp),
        )

    def z_far(m, half):
        piece = 2 * m + half
        return remote(
            source(m, half),
            slot(m, half, sp),
            z_send.at[piece, 1],
            z_recv.at[piece, z],
            (far_target * 2 + y, tp),
        )

    def to_y(m, half, plane, src):
        piece, place = 2 * m + half, plane * 2 + y
        return remote(
            src,
            slot(m, half, place),
            y_send.at[piece, plane],
            y_recv.at[piece, plane],
            (sp_y, tp),
        )

    def to_core(m, half, place, src):
        piece = 2 * m + half
        return remote(
            src,
            slot(m, half, place),
            c_send.at[piece, place],
            c_recv.at[piece, place],
            (sp, tp_core),
        )

    def z_arrival(m, half, plane):
        piece, here = 2 * m + half, slot(m, half, plane * 2 + y)
        return remote(here, here, z_send.at[piece, 1], z_recv.at[piece, plane], (sp_y, tp))

    def y_arrival(m, half, plane):
        piece, here = 2 * m + half, slot(m, half, plane * 2 + other_y)
        return remote(here, here, y_send.at[piece, plane], y_recv.at[piece, plane], (sp_y, tp))

    def start_own(m):
        @pl.when(is_main)
        def _():
            for half in range(2):
                to_y(m, half, z, source(m, half)).start()
                to_core(m, half, sp, source(m, half)).start()

    def pass_plane(m, half, plane):
        z_arrival(m, half, plane).wait_recv()
        here = slot(m, half, plane * 2 + y)
        to_y(m, half, plane, here).start()
        to_core(m, half, plane * 2 + y, here).start()

    def pass_z(m, half, planes_list):
        @pl.when(is_main)
        def _():
            for plane in planes_list:
                pass_plane(m, half, plane)

    def pass_if(condition, m, half, plane):
        @pl.when(jnp.logical_and(condition, is_main))
        def _():
            pass_plane(m, half, plane)

    def pass_y(m, half, planes_list, condition=True):
        @pl.when(jnp.logical_and(condition, is_main))
        def _():
            for plane in planes_list:
                y_arrival(m, half, plane).wait_recv()
                place = plane * 2 + other_y
                to_core(m, half, place, slot(m, half, place)).start()

    def core_wait(m, planes_list):
        @pl.when(is_helper)
        def _():
            for plane in planes_list:
                for half in range(2):
                    for place in (plane * 2 + y, plane * 2 + other_y):
                        here = slot(m, half, place)
                        to_core(m, half, place, here).wait_recv()

    def own_wait(m):
        @pl.when(is_main)
        def _():
            own_copy(m).wait()

    near_up = parity == 0
    far_up = z < planes // 2
    near_down, far_down = parity == 1, z >= planes // 2
    one_hop = jnp.logical_and(in_middle, is_helper)
    more_hops = jnp.logical_or(at_end, is_main)
    both = jnp.logical_and

    def when_do(condition, do):
        @pl.when(condition)
        def _():
            do()

    def start_far(m, half, condition):
        when_do(condition, lambda: z_far(m, half).start())

    def start_near(m, half, condition):
        when_do(both(is_helper, condition), lambda: z_near(m, half).start())

    when_do(is_helper, lambda: z_near(0, 0).start())
    start_far(0, 0, jnp.logical_or(far_down, one_hop))
    when_do(is_helper, lambda: z_near(0, 1).start())
    start_far(0, 1, far_down)
    near_planes = [pair, far, far_pair]
    all_planes = [z] + near_planes

    ow_copies = [
        remote(ow_in, ow.at[tp], ow_send.at[0], ow_recv.at[tp], (sp, tp_x)),
        remote(ow_in, ow.at[tp], ow_send.at[1], ow_recv.at[tp], (sp, tp_core)),
        remote(ow.at[tp_x], ow.at[tp_x], ow_send.at[2], ow_recv.at[tp_x], (sp, tp_core)),
    ]
    ow_copies[0].start()
    ow_copies[1].start()

    for i in range(3):
        local_copy(i).wait()

    row_index = lax.broadcasted_iota(jnp.int32, (BLOCK, BLOCK), 0)
    col_index = lax.broadcasted_iota(jnp.int32, (BLOCK, BLOCK), 1)
    before = jnp.where(row_index <= col_index, 1.0, 0.0).astype(BF16)
    until = jnp.where(row_index >= col_index, 1.0, 0.0).astype(BF16)
    for b in range(block_count):
        decay = decay_in[:, b * BLOCK : (b + 1) * BLOCK]
        high = decay.astype(BF16)
        rest = decay - high.astype(F32)
        middle_term = rest.astype(BF16)
        low = (rest - middle_term.astype(F32)).astype(BF16)
        by_row, by_col = 0.0, 0.0
        for term in (low, middle_term, high):
            by_row = by_row + jnp.dot(term, before, preferred_element_type=F32)
            by_col = by_col + lax.dot_general(
                until, term, (((1,), (1,)), ((), ())), preferred_element_type=F32
            )
        cum_row[b] = by_row
        cum_col[b] = by_col

    def block_decay(b, h):
        return jnp.exp(cum_row[b, h : h + 1, BLOCK - 1 : BLOCK])

    for h in range(heads):
        lanes = slice(h * dim, (h + 1) * dim)
        for b in range(block_count):
            span = slice(b * BLOCK, (b + 1) * BLOCK)
            last = cum_row[b, h : h + 1, BLOCK - 1 : BLOCK]
            to_end = jnp.exp(last - cum_col[b, :, h : h + 1]) * scale
            scaled = (k_ref[span, lanes].astype(F32) * to_end).astype(BF16)
            local_state[b, h] = lax.dot_general(
                scaled, v_ref[span, lanes], (((0,), (0,)), ((), ())), preferred_element_type=F32
            )

    def local_total(h):
        total, decay = local_state[0, h], block_decay(0, h)
        for b in range(1, block_count):
            total = block_decay(b, h) * total + local_state[b, h]
            decay = decay * block_decay(b, h)
        return total, decay

    header_row = lax.broadcasted_iota(jnp.int32, (HEADER_ROWS, dim), 0)

    def pack(ref, h, total, decay):
        ref[h, :dim] = total.astype(BF16)
        wide = jnp.broadcast_to(decay, (HEADER_ROWS, dim))
        high = wide.astype(BF16).astype(F32)
        ref[h, dim:] = jnp.where(header_row < 8, high, wide - high).astype(BF16)

    def unpack(packed, h):
        block = packed[h].astype(F32)
        return block[:dim], block[dim : dim + 1] + block[dim + 8 : dim + 9]

    for h in range(heads):
        total, decay = local_total(h)
        pack(state_out, h, total, decay)
    pair_copy = remote(state_out, state_pair, pair_send.at[0], pair_recv.at[0], (sp_y, tp))
    pair_copy.start()
    start_own(0)

    def scores_of(b):
        for h in range(heads):
            lanes = slice(h * dim, (h + 1) * dim)
            span = slice(b * BLOCK, (b + 1) * BLOCK)
            tile = 128
            keys, vals = k_ref[span, lanes], v_ref[span, lanes]
            row_sums = cum_row[b, h : h + 1, :]

            def one(i, _):
                at = pl.multiple_of(i * tile, tile)
                here = pl.ds(b * BLOCK + at, tile)
                products = lax.dot_general(
                    q_ref[here, lanes], keys, (((1,), (1,)), ((), ())), preferred_element_type=F32
                )
                gap = cum_col[b, pl.ds(at, tile), h : h + 1] - row_sums
                t_index = at + lax.broadcasted_iota(jnp.int32, (tile, BLOCK), 0)
                s_index = lax.broadcasted_iota(jnp.int32, (tile, BLOCK), 1)
                weight = jnp.where(s_index <= t_index, jnp.exp(jnp.minimum(gap, 0.0)), 0.0)
                scores = (products * scale * weight).astype(BF16)
                retention[here, lanes] = jnp.dot(scores, vals, preferred_element_type=F32)
                return 0

            lax.fori_loop(0, BLOCK // tile, one, 0)

    scores_of(0)

    pair_copy.wait_recv()
    for h in range(heads):
        total, decay = local_total(h)
        their_total, their_decay = unpack(state_pair, h)
        last_factor = jnp.where(y == 1, decay, their_decay)
        first = jnp.where(y == 1, their_total, total)
        second = jnp.where(y == 1, total, their_total)
        pack(total_out, h, last_factor * first + second, decay * their_decay)

    def total_copy(plane):
        return remote(
            total_out,
            total_in.at[z],
            total_send.at[plane],
            total_recv.at[z],
            (plane * 2 + y, tp),
        )

    for plane in range(1, 4):

        @pl.when(z < plane)
        def _():
            total_copy(plane).start()


    for half in range(2):
        start_far(1, half, both(far_down, in_middle))
        start_near(1, half, near_down)
    for b in range(1, block_count):
        scores_of(b)

    ow_arrival = [
        remote(ow.at[t], ow.at[t], ow_send.at[0], ow_recv.at[t], (sp, tp_x))
        for t in (tp_x, tp_core, tp_both)
    ]

    for h in range(heads):
        start_state[0, h] = jnp.zeros((dim, dim), F32)
    for plane in range(3):

        @pl.when(plane < z)
        def _():
            remote(
                total_out,
                total_in.at[plane],
                total_send.at[plane],
                total_recv.at[plane],
                (sp_y, tp),
            ).wait_recv()
            for h in range(heads):
                total, decay = unpack(total_in.at[plane], h)
                start_state[0, h] = decay * start_state[0, h] + total

    for h in range(heads):
        their_total, their_decay = unpack(state_pair, h)
        state = start_state[0, h]
        state = jnp.where(y == 1, their_decay * state + their_total, state)
        start_state[0, h] = state
        for b in range(1, block_count):
            state = block_decay(b - 1, h) * state + local_state[b - 1, h]
            start_state[b, h] = state

    local_copy(3).wait()

    def retained_copy(j):
        return remote(
            retained_out.at[j],
            retained_in.at[tp],
            ret_send.at[j],
            ret_recv.at[tp],
            (sp, j),
        )

    per_block = BLOCK // quarter

    def finish(j, target):
        b = j // per_block
        at = pl.multiple_of((j % per_block) * quarter, quarter)
        here = pl.ds(pl.multiple_of(j * quarter, quarter), quarter)
        for h in range(heads):
            lanes = slice(h * dim, (h + 1) * dim)
            state = start_state[b, h]
            high = state.astype(BF16)
            low = (state - high.astype(F32)).astype(BF16)
            query = q_ref[here, lanes]
            carried = jnp.dot(query, high, preferred_element_type=F32) + jnp.dot(
                query, low, preferred_element_type=F32
            )
            kept = retention[here, lanes] + carried * jnp.exp(
                cum_col[b, pl.ds(at, quarter), h : h + 1]
            )
            centered = kept - jnp.mean(kept, axis=-1, keepdims=True)
            variance = jnp.mean(centered * centered, axis=-1, keepdims=True)
            normed = centered * lax.rsqrt(variance + EPSILON) * norm_gain[h : h + 1, :]
            target[:, lanes] = (silu_of(gates_ref[here, lanes].astype(F32)) * normed).astype(BF16)

    others = [(tp + i) % tps for i in range(1, tps)]
    start_far(0, 0, both(far_up, more_hops))
    start_far(0, 1, far_up)
    for half in range(2):
        start_far(1, half, both(far_up, in_middle))
        start_near(1, half, near_up)

    for j in others:
        finish(j, retained_out.at[j])
        retained_copy(j).start()
    finish(tp, retained_in.at[tp])

    pass_z(0, 0, near_planes[:1])
    start_own(1)
    ow_arrival[0].wait_recv()
    ow_copies[2].start()
    for arrival in ow_arrival[1:]:
        arrival.wait_recv()
    local_copy(5).wait()
    local_copy(4).wait()
    for j in others:
        remote(
            retained_out.at[j],
            retained_in.at[j],
            ret_send.at[j],
            ret_recv.at[j],
            (sp, j),
        ).wait_recv()

    mix_tile = 512

    def mix(i, _):
        here = pl.ds(pl.multiple_of(i * mix_tile, mix_tile), mix_tile)
        total = jnp.zeros((quarter, mix_tile), F32)
        for g in range(tps):
            part = jnp.dot(retained_in[g], ow[g, :, here], preferred_element_type=F32)
            total = total + part.astype(BF16).astype(F32)
        mixed[:, here] = total.astype(BF16)
        return 0

    lax.fori_loop(0, model // mix_tile, mix, 0)

    def rms_of(v):
        return v * lax.rsqrt(jnp.mean(v * v, axis=-1, keepdims=True) + EPSILON)

    mine = x * 2 + parity
    norm_tile = 32

    def into_rows(i, _):
        here = pl.ds(pl.multiple_of(i * norm_tile, norm_tile), norm_tile)
        value = rms_of(mixed[here, :].astype(F32)) * mix_gain[...]
        value = (resid_ref[here, :].astype(F32) + value).astype(BF16)
        middle[here, :] = value
        rows[mine, here, :] = (rms_of(value.astype(F32)) * pre_gain[...]).astype(BF16)
        return 0

    from_pair = x * 2 + 1 - parity
    from_x = other_x * 2 + parity
    from_both = other_x * 2 + 1 - parity
    row_parts = 4
    part_rows = quarter // row_parts

    def rows_copy(i, half, place, device):
        here = rows.at[place, half * part_rows : (half + 1) * part_rows]
        return remote(here, here, rows_send.at[i, half], rows_recv.at[place, half], device)

    for half in range(row_parts):
        steps = part_rows // norm_tile
        lax.fori_loop(half * steps, (half + 1) * steps, into_rows, 0)
        rows_copy(0, half, mine, (sp_pair, tp)).start()
        rows_copy(1, half, mine, (sp, tp_x)).start()

    pass_z(0, 1, near_planes[:1])
    pass_z(0, 0, near_planes[1:])
    pass_z(0, 1, near_planes[1:])
    for half in range(2):
        pass_z(1, half, near_planes[:1])
    early_far = both(at_end, both(is_main, far_down))
    for half in range(2):
        start_far(1, half, early_far)
    for half in range(row_parts // 2):
        rows_copy(0, half, from_pair, (sp_pair, tp)).wait_recv()
        rows_copy(2, half, from_pair, (sp, tp_x)).start()
    for half in range(2):
        start_far(1, half, both(at_end, jnp.logical_not(early_far)))
    start_own(2)
    for half in range(2):
        pass_if(at_end, 1, half, far)
        pass_if(in_middle, 1, half, far_pair)
    for half in range(row_parts // 2, row_parts):
        rows_copy(0, half, from_pair, (sp_pair, tp)).wait_recv()
        rows_copy(2, half, from_pair, (sp, tp_x)).start()
    for half in range(2):
        when_do(is_helper, lambda: z_near(2, half).start())
        start_far(2, half, in_middle)
    for half in range(2):
        pass_y(0, half, all_planes)
    own_wait(0)
    core_wait(0, all_planes)

    unit_tile = 256
    unit_steps = units // unit_tile

    def acts_of(weight, first, at, size):
        here = pl.ds(at, size)
        return jnp.dot(
            rows[pl.ds(first, 2)].reshape(2 * quarter, model),
            weight[:, :, here].reshape(model, size),
            preferred_element_type=F32,
        ).reshape(2, quarter, size)

    def over_units(one, begin=0, end=unit_steps + 1):
        def step(i, _):
            one(pl.multiple_of(i * unit_tile, unit_tile), unit_tile)
            return 0

        lax.fori_loop(begin, min(end, unit_steps), step, 0)
        if end > unit_steps and units % unit_tile:
            one(unit_steps * unit_tile, units % unit_tile)

    def gate_of(first):
        def one(at, size):
            gate_acts[pl.ds(first, 2), :, pl.ds(at, size)] = acts_of(wg, first, at, size)

        over_units(one)

    def up_of(first, begin=0, end=unit_steps + 1):
        def one(at, size):
            here = pl.ds(at, size)
            gate = gate_acts[pl.ds(first, 2), :, here]
            value = silu_of(gate) * acts_of(wu, first, at, size)
            hidden[pl.ds(first, 2), :, here] = value.astype(BF16)

        over_units(one, begin, end)

    gate_of(x * 2)
    for half in range(2):
        start_far(2, half, at_end)
    pass_if(at_end, 1, 0, far_pair)
    pass_if(in_middle, 1, 0, far)
    pass_if(at_end, 1, 1, far_pair)
    pass_if(in_middle, 1, 1, far)
    for half in range(2):
        pass_y(1, half, [z, pair])
        pass_y(1, half, [far], at_end)
        pass_y(1, half, [far_pair], in_middle)
    pass_z(2, 0, near_planes[:1])
    for half in range(row_parts):
        rows_copy(1, half, from_x, (sp, tp_x)).wait_recv()
        rows_copy(2, half, from_both, (sp, tp_x)).wait_recv()
    gate_of(other_x * 2)
    for half in range(2):
        pass_y(1, half, [far_pair], at_end)
        pass_y(1, half, [far], in_middle)
    for half in range(2):
        pass_y(2, half, [z])
    pass_z(2, 1, near_planes[:1])
    own_wait(1)
    core_wait(1, all_planes)

    columns = wd_in.shape[1]

    def down(place, first, second):
        left = jnp.concatenate([hidden[first], hidden[second]], axis=0)
        product = jnp.dot(left, wd[place], preferred_element_type=F32)
        return product.astype(BF16).reshape(2, quarter, columns)

    def place_of(plane, over_x):
        even = plane % 2 == 0
        return plane * 2 + (lax.select(even, y, other_y) if over_x else lax.select(even, other_y, y))

    def block_of(plane, own):
        place = plane * 2 + (y if own else other_y)
        return place, (plane % 2 == 0) if own else (plane % 2 == 1)

    def part_copy(place, over_x):
        if isinstance(over_x, bool):
            device = (sp, tp_x) if over_x else (sp_pair, tp)
        else:
            device = (lax.select(over_x, sp, sp_pair), lax.select(over_x, tp_x, tp))
        return remote(
            part_out.at[place], part_in.at[place], part_send.at[place], part_recv.at[place], device
        )

    def sum_copy(place, over_x):
        device = (sp_pair, tp) if over_x else (sp, tp_x)
        return remote(
            sum_out.at[place], sum_in.at[place], sum_send.at[place], sum_recv.at[place], device
        )

    def place_wait(place):
        @pl.when(is_helper)
        def _():
            for half in range(2):
                to_core(2, half, place, slot(2, half, place)).wait_recv()

    def send_part(plane, own):
        place, over_x = block_of(plane, own)
        if not own and plane is not z:
            for half in range(2):
                pass_y(2, half, [plane])
        place_wait(place)
        part_out[place] = down(
            place,
            lax.select(over_x, other_x * 2, 1 - parity),
            lax.select(over_x, other_x * 2 + 1, 3 - parity),
        )
        part_copy(place, over_x).start()

    def own_product(plane, over_x):
        place = place_of(plane, over_x)
        product = down(place, mine, from_pair if over_x else from_x)
        branch[place] = product[0].astype(F32)
        sum_out[place] = product[1]

    def own_part(plane, over_x):
        place = place_of(plane, over_x)
        mine_at, other_at = (parity, 1 - parity) if over_x else (x, other_x)
        part_copy(place, over_x).wait_recv()
        sum_out[place] = (
            sum_out[place].astype(F32) + part_in[place, other_at].astype(F32)
        ).astype(BF16)
        sum_copy(place, over_x).start()
        branch[place] = branch[place] + part_in[place, mine_at].astype(F32)

    def pass_late(half):
        pass_if(at_end, 2, half, far)
        pass_if(at_end, 2, half, far_pair)
        pass_if(in_middle, 2, half, far_pair)
        pass_if(in_middle, 2, half, far)

    up_of(other_x * 2)
    own_wait(2)
    when_do(parity == 0, lambda: send_part(z, True))
    when_do(parity == 1, lambda: send_part(z, False))
    up_of(x * 2, 0, unit_steps // 2)
    pass_late(0)
    up_of(x * 2, unit_steps // 2)
    when_do(parity == 0, lambda: send_part(z, False))
    when_do(parity == 1, lambda: send_part(z, True))
    pass_late(1)
    send_part(pair, True)
    own_product(z, True)
    own_product(z, False)
    own_part(z, True)
    send_part(pair, False)
    send_part(far, True)
    own_product(pair, True)
    own_product(pair, False)
    own_part(pair, False)
    send_part(far, False)
    send_part(far_pair, True)
    send_part(far_pair, False)
    own_part(z, False)
    own_part(pair, True)
    own_product(far, True)
    own_part(far, True)
    own_product(far_pair, False)
    own_part(far_pair, False)
    own_product(far_pair, True)
    own_part(far_pair, True)
    own_product(far, False)
    own_part(far, False)

    for plane in all_planes:
        for over_x in (True, False):
            sum_copy(place_of(plane, over_x), over_x).wait_recv()

    def final(i, _):
        here = pl.ds(pl.multiple_of(i * norm_tile, norm_tile), norm_tile)
        value = jnp.concatenate(
            [branch[n, here, :] + sum_in[n, here, :].astype(F32) for n in range(2 * planes)],
            axis=1,
        )
        value = rms_of(value.astype(BF16).astype(F32)) * post_gain[...]
        out[here, :] = (middle[here, :].astype(F32) + value).astype(BF16)
        return 0

    lax.fori_loop(0, quarter // norm_tile, final, 0)

    for m in range(3):
        for half in range(2):
            z_far(m, half).wait_send()
            when_do(is_helper, lambda: z_near(m, half).wait_send())

            @pl.when(is_main)
            def _():
                for plane in all_planes:
                    place = plane * 2 + y
                    src = source(m, half) if plane is z else slot(m, half, place)
                    to_y(m, half, plane, src).wait_send()
                    to_core(m, half, place, src).wait_send()
                    place = plane * 2 + other_y
                    to_core(m, half, place, slot(m, half, place)).wait_send()

    for copy in ow_copies:
        copy.wait_send()
    pair_copy.wait_send()
    for plane in range(1, 4):

        @pl.when(z < plane)
        def _():
            total_copy(plane).wait_send()

    for j in others:
        retained_copy(j).wait_send()
    for half in range(row_parts):
        rows_copy(0, half, mine, (sp_pair, tp)).wait_send()
        rows_copy(1, half, mine, (sp, tp_x)).wait_send()
        rows_copy(2, half, from_pair, (sp, tp_x)).wait_send()
    for plane in range(planes):
        for over_x in (True, False):
            place = plane * 2 + int(over_x)
            part_copy(place, over_x).wait_send()
            sum_copy(place, over_x).wait_send()


def whole_layer(
    queries,
    keys,
    values,
    gates,
    log_decay,
    norm_gain,
    out_weight,
    resid,
    post_mix_gain,
    pre_ffn_gain,
    w_gate,
    w_up,
    w_down,
    post_ffn_gain,
):
    places, tps = lax.axis_size("sp"), lax.axis_size("tp")
    planes = places // 2
    row_count, width = queries.shape
    heads, dim = norm_gain.shape
    block_count = row_count // BLOCK
    quarter, model = resid.shape
    depth, units = w_gate.shape
    columns = w_down.shape[1]
    decay_rows = log_decay.T
    anywhere = pl.BlockSpec(memory_space=pl.ANY)
    onchip = pl.BlockSpec(memory_space=pltpu.VMEM)
    dma = pltpu.SemaphoreType.DMA
    packed = (heads, dim + HEADER_ROWS, dim)
    scratch = [
        pltpu.VMEM((row_count, width), BF16),
        pltpu.VMEM((row_count, width), BF16),
        pltpu.VMEM((row_count, width), BF16),
        pltpu.VMEM((row_count, width), BF16),
        pltpu.VMEM((quarter, model), BF16),
        pltpu.VMEM((places, depth, units), BF16),
        pltpu.VMEM((places, depth, units), BF16),
        pltpu.VMEM((places, units, columns), BF16),
        pltpu.VMEM((tps, width, model), BF16),
        pltpu.VMEM((block_count, heads, BLOCK), F32),
        pltpu.VMEM((block_count, BLOCK, heads), F32),
        pltpu.VMEM((block_count, heads, dim, dim), F32),
        pltpu.VMEM((block_count, heads, dim, dim), F32),
        pltpu.VMEM(packed, BF16),
        pltpu.VMEM(packed, BF16),
        pltpu.VMEM(packed, BF16),
        pltpu.VMEM((planes,) + packed, BF16),
        pltpu.VMEM((row_count, width), F32),
        pltpu.VMEM((tps, quarter, width), BF16),
        pltpu.VMEM((tps, quarter, width), BF16),
        pltpu.VMEM((quarter, model), BF16),
        pltpu.VMEM((quarter, model), BF16),
        pltpu.VMEM((4, quarter, model), BF16),
        pltpu.VMEM((4, quarter, units), F32),
        pltpu.VMEM((4, quarter, units), BF16),
        pltpu.VMEM((places, 2, quarter, columns), BF16),
        pltpu.VMEM((places, 2, quarter, columns), BF16),
        pltpu.VMEM((places, quarter, columns), BF16),
        pltpu.VMEM((places, quarter, columns), BF16),
        pltpu.VMEM((places, quarter, columns), F32),
        dma((6,)),
        dma((3,)),
        dma((6, 2)),
        dma((6, planes)),
        dma((6, planes)),
        dma((6, planes)),
        dma((6, places)),
        dma((6, places)),
        dma((3,)),
        dma((tps,)),
        dma((1,)),
        dma((1,)),
        dma((planes,)),
        dma((planes,)),
        dma((tps,)),
        dma((tps,)),
        dma((3, 4)),
        dma((4, 4)),
        dma((places,)),
        dma((places,)),
        dma((places,)),
        dma((places,)),
    ]
    return pl.pallas_call(
        layer_kernel,
        out_shape=jax.ShapeDtypeStruct((quarter, model), BF16),
        in_specs=[anywhere] * 4
        + [onchip, onchip, anywhere, anywhere, onchip, onchip]
        + [anywhere] * 3
        + [onchip],
        out_specs=onchip,
        scratch_shapes=scratch,
        compiler_params=pltpu.CompilerParams(
            collective_id=0, has_side_effects=True, vmem_limit_bytes=62 * 1024 * 1024
        ),
    )(
        queries,
        keys,
        values,
        gates,
        decay_rows,
        norm_gain,
        out_weight,
        resid,
        post_mix_gain[None],
        pre_ffn_gain[None],
        w_gate,
        w_up,
        w_down,
        post_ffn_gain[None],
    )


def solution(mesh):
    in_specs = (
        P("sp", "tp"),
        P("sp", "tp"),
        P("sp", "tp"),
        P("sp", "tp"),
        P("sp", "tp"),
        P("tp", None),
        P("tp", None),
        P(("sp", "tp"), None),
        P(),
        P(),
        P("sp", "tp"),
        P("sp", "tp"),
        P("tp", "sp"),
        P(),
    )
    out_specs = P(("sp", "tp"), None)
    if mesh.shape["sp"] == LONGEST_RING and mesh.shape["tp"] == 4:
        return jax.shard_map(
            whole_layer, mesh=mesh, in_specs=in_specs, out_specs=out_specs, check_vma=False
        )

    return jax.shard_map(
        per_device, mesh=mesh, in_specs=in_specs, out_specs=out_specs, check_vma=False
    )
```
